128 devices in a mesh: rep: 2 (over z_hi), fs: 32 (over z_lo, y, x), tp: 2 (over core).
Axes of the slice: x: 4, y: 4, z: 4 (z_hi: 2, z_lo: 2; z = z_hi * 2 + z_lo), core: 2. Of those that a mesh axis runs over, the one named last changes fastest.
Arguments:
- inputs: bfloat16 [32768, 1024], P(('rep', 'fs', 'tp')), may hold values from -6 to 6
- up_proj: bfloat16 [1024, 4096], P('fs', 'tp'), may hold values from -0.1875 to 0.1875
- down_proj: bfloat16 [4096, 1024], P('tp', 'fs'), may hold values from -0.09375 to 0.09375
- out_cotangent: bfloat16 [32768, 1024], P(('rep', 'fs', 'tp')), may hold values from -24 to 24
Outputs:
- grad_inputs: bfloat16 [32768, 1024], P(('rep', 'fs', 'tp'))
- grad_up: float32 [1024, 4096], P('fs', 'tp')
- grad_down: float32 [4096, 1024], P('tp', 'fs')
- energy_up: float32 [1024], P('fs')
- energy_down: float32 [4096], P('tp')
The draws below stay inside these ranges and needn't reach their ends.
All inputs are finite; a program needn't handle non-finite values.
Results may differ from the reference program's by a relative error of at most 0.001.
Values may be sent and summed in bfloat16 or wider, within the bound.
A program may use at most 128 MiB of HBM per device.

```python
import jax
import jax.numpy as jnp
from jax import lax

D = 1024
FF = 4096
TOKENS = 32768


def raised(entries, key, source, target, parts, factor):
    owner, partner = [(jnp.arange(entries.shape[position]) // (entries.shape[position] // parts)).reshape([-1 if axis == position else 1 for axis in range(entries.ndim)]) for position in (source, target)]
    chosen = jax.random.permutation(key, parts)[partner]
    strong = (owner == chosen) | (owner == (partner + parts // 2) % parts)
    return jnp.where(strong, factor * entries, entries)


def level_of(rng, extent, shards, smallest, top_value):
    factor_of = 1.0
    for dim, blocks in shards:
        heights = jax.random.uniform(jax.random.fold_in(jax.random.fold_in(rng, 6), dim), (blocks,), jnp.float32, smallest / len(shards), top_value / len(shards))
        factor_of = factor_of * jnp.repeat(jnp.exp(heights), extent[dim] // blocks).reshape((-1,) + (1,) * (len(extent) - 1 - dim))
    return factor_of


def gaussian(rng, dims, width, bound, cuts=(), dtype=jnp.bfloat16):
    array = width * jax.random.normal(rng, dims, jnp.float32)
    if cuts:
        array = array * level_of(rng, dims, cuts, -0.22, 0.18)
    return jnp.clip(array, -bound, bound).astype(dtype)


def heavy_noise(key, shape, deviation, reach, split, heavy, held_as=jnp.bfloat16):
    entries = deviation * jax.random.normal(key, shape, jnp.float32)
    if split:
        entries = entries * level_of(key, shape, split, -0.22, 0.18)
    return jnp.clip(raised(entries, jax.random.fold_in(key, 3), *heavy), -reach, reach).astype(held_as)


def setup_inputs(seed: int = 0) -> dict:
    streams_of = jax.random.split(jax.random.key(seed), 5)
    return {
        "inputs": gaussian(streams_of[0], (TOKENS, D), 1.0, 6.0, ((0, 128),)),
        "up_proj": gaussian(streams_of[1], (D, FF), D ** -0.5, 0.1875, ((0, 32), (1, 2))),
        "down_proj": gaussian(streams_of[2], (FF, D), FF ** -0.5, 0.09375, ((0, 2), (1, 32))),
        "out_cotangent": heavy_noise(streams_of[3], (TOKENS, D), 1.0, 24.0, ((0, 128),), (0, 1, 128, 5.5)),
    }


def contract(left, right, left_dim, right_dim):
    return lax.dot_general(left, right, (((left_dim,), (right_dim,)), ((), ())), preferred_element_type=jnp.float32)


def reference(inputs, up_proj, down_proj, out_cotangent):
    factor = float(TOKENS) ** -0.5
    pre = jnp.dot(inputs, up_proj, preferred_element_type=jnp.float32)
    active = jnp.square(jax.nn.relu(pre)).astype(jnp.bfloat16)
    back = contract(out_cotangent, down_proj, 1, 1)
    grad_pre = (2.0 * jax.nn.relu(pre) * back).astype(jnp.bfloat16)
    grad_inputs = contract(grad_pre, up_proj, 1, 1).astype(jnp.bfloat16)
    grad_up = contract(inputs, grad_pre, 0, 0) * factor
    grad_down = contract(active, out_cotangent, 0, 0) * factor
    energy_up = jnp.sum(grad_up * grad_up, axis=1) / FF
    energy_down = jnp.sum(grad_down * grad_down, axis=1) / D
    return grad_inputs, grad_up, grad_down, energy_up, energy_down
```

```python
import functools

import jax
import jax.numpy as jnp
from jax import lax
from jax.experimental import pallas as pl
from jax.experimental.pallas import tpu as pltpu
from jax.sharding import PartitionSpec as P

MESH = pl.DeviceIdType.MESH
ORDERS = (
    (0, 4, 1, 2, 3),
    (2, 3, 4, 0, 1),
    (1, 0, 3, 4, 2),
    (3, 2, 1, 4, 0),
    (3, 0, 2, 4, 1),
    (2, 1, 0, 4, 3),
    (0, 1, 4, 3, 2),
    (3, 2, 1, 4, 0),
)
STEPS = 5
PARTS = len(ORDERS)


def bits_of(fs):
    z, y, x = fs // 16, (fs // 4) % 4, fs % 4
    return (z, (y % 2 + y // 2) % 2, y // 2, (x % 2 + x // 2) % 2, x // 2)


def partners_of(fs):
    z, y, x = fs // 16, (fs // 4) % 4, fs % 4
    return (
        fs + 16 - 32 * z,
        fs + 4 - 8 * (y % 2),
        fs + 12 - 8 * y,
        fs + 1 - 2 * (x % 2),
        fs + 3 - 2 * x,
    )


def remote(src, dst, send, recv, device):
    return pltpu.make_async_remote_copy(
        src_ref=src, dst_ref=dst, send_sem=send, recv_sem=recv, device_id=device, device_id_type=MESH
    )


def contract(left, right, left_dim, right_dim):
    return lax.dot_general(
        left, right, (((left_dim,), (right_dim,)), ((), ())), preferred_element_type=jnp.float32
    )


def kernel(
    factor,
    x_ref,
    c_ref,
    u_ref,
    d_ref,
    gin_ref,
    gup_ref,
    gdn_ref,
    eup_ref,
    edn_ref,
    tok,
    tokt,
    wg,
    wn,
    pre,
    act,
    gpre,
    gbuf,
    rbuf,
    part_in,
    pair_in,
    last_in,
    outs,
    ebuf,
    esum,
    eup_own,
    eup_in,
    tok_s,
    tok_r,
    fwd_s,
    fwd_r,
    sib_s,
    sib_r,
    g_s,
    g_r,
    r_s,
    r_r,
    rep_s,
    rep_r,
    pi_s,
    pi_r,
    li_s,
    li_r,
    e_s,
    e_r,
    eu_s,
    eu_r,
):
    rep, fs, tp = lax.axis_index("rep"), lax.axis_index("fs"), lax.axis_index("tp")
    mine = bits_of(fs)
    near = [{"fs": other} for other in partners_of(fs)]
    sibling = {"tp": 1 - tp}
    pair = {"rep": 1 - rep, "fs": partners_of(fs)[0]}
    twin = {"rep": 1 - rep}
    rows, width = x_ref.shape
    shard = u_ref.shape[0]
    hidden = u_ref.shape[1] // 2
    cols = hidden // PARTS
    base = rep * hidden
    weights = (u_ref, d_ref)
    tokens = (x_ref, c_ref)
    pieces = 2
    chunk = rows // pieces

    barrier = pltpu.get_barrier_semaphore()
    for device in near + [sibling, pair, twin]:
        pl.semaphore_signal(barrier, inc=1, device_id=device, device_id_type=MESH)

    for m in range(2):
        tok[m, 0] = tokens[m][...]
        for p in range(PARTS):
            wg[m, p, 0] = weights[m][:, pl.ds(pl.multiple_of(base + p * cols, cols), cols)]

    pl.semaphore_wait(barrier, STEPS + 3)

    pending = []

    def start(copy):
        copy.start()
        pending.append(copy)
        return copy

    def token_copy(m, q):
        return remote(
            tokens[m].at[pl.ds(q * chunk, chunk)],
            tok.at[m, 2, pl.ds(q * chunk, chunk)],
            tok_s.at[m, q],
            tok_r.at[m, q],
            pair,
        )

    def forward_copy(m, q):
        return remote(
            tok.at[m, 2, pl.ds(q * chunk, chunk)],
            tok.at[m, 3, pl.ds(q * chunk, chunk)],
            fwd_s.at[m, q],
            fwd_r.at[m, q],
            sibling,
        )

    def sibling_copy(m):
        return remote(tokens[m], tok.at[m, 1], sib_s.at[m], sib_r.at[m], sibling)

    def gather_copy(m, p, k):
        if k == 0:
            src = weights[m].at[:, pl.ds(pl.multiple_of(base + p * cols, cols), cols)]
            dst = wg.at[m, p, 1]
        else:
            src = wg.at[m, p, pl.ds(0, 2**k)]
            dst = wg.at[m, p, pl.ds(2**k, 2**k)]
        return remote(src, dst, g_s.at[m * PARTS + p, k], g_r.at[m * PARTS + p, k], near[ORDERS[p][k]])

    def gather_step(m, k):
        for p in range(PARTS):
            if k > 0:
                gather_copy(m, p, k - 1).wait_recv()
            start(gather_copy(m, p, k))

    def forward(m, q):
        token_copy(m, q).wait_recv()
        start(forward_copy(m, q))

    for m in range(2):
        gather_step(m, 0)
        for q in range(pieces):
            start(token_copy(m, q))
    for m in range(2):
        start(sibling_copy(m))

    def transpose(m, g):
        tokt[m, :, g * rows : (g + 1) * rows] = tok[m, g].T

    gather_step(0, 1)
    gather_step(1, 1)
    gather_step(0, 2)
    gather_step(1, 2)
    for m in range(2):
        transpose(m, 0)
        sibling_copy(m).wait_recv()
        transpose(m, 1)
    forward(0, 0)
    gather_step(0, 3)
    gather_step(1, 3)
    forward(0, 1)
    gather_step(0, 4)
    gather_step(1, 4)

    def slot(bits, p):
        total = 0
        for k in range(STEPS):
            total = total + bits[ORDERS[p][k]] * 2**k
        return total

    def relative(shard_index):
        return [(a + b) % 2 for a, b in zip(mine, bits_of(shard_index))]

    def unpack(m, p):
        gather_copy(m, p, STEPS - 1).wait_recv()

        def some(i, carry):
            for t in range(8):
                s = i * 8 + t
                wn[m, pl.ds(pl.multiple_of(s * shard, shard), shard), p * cols : (p + 1) * cols] = wg[
                    m, p, slot(relative(s), p)
                ]
            return carry

        lax.fori_loop(0, 4, some, 0)

    for q in range(pieces):
        forward_copy(0, q).wait_recv()
    transpose(0, 2)
    transpose(0, 3)
    blocks = PARTS // 2
    bw = 2 * cols

    def part_cols(j):
        return slice(j * bw, (j + 1) * bw)

    for j in range(blocks):
        unpack(0, 2 * j)
        unpack(0, 2 * j + 1)

        def tokens_pre(g, carry, j=j):
            pre[g, :, part_cols(j)] = jnp.maximum(
                jnp.dot(tok[0, g], wn[0, :, part_cols(j)], preferred_element_type=jnp.float32), 0.0
            )
            return carry

        lax.fori_loop(0, 4, tokens_pre, 0)

    for q in range(pieces):
        forward(1, q)
    for j in range(blocks):
        unpack(1, 2 * j)
        unpack(1, 2 * j + 1)
    for q in range(pieces):
        forward_copy(1, q).wait_recv()
    transpose(1, 2)
    transpose(1, 3)

    offset = (0, 16, 24, 28, 30)
    half = (16, 8, 4, 2, 1)

    def reduce_copy(r, k):
        return remote(
            gbuf.at[r, pl.ds(half[k], half[k])],
            rbuf.at[r, pl.ds(offset[k], half[k])],
            r_s.at[r, k],
            r_r.at[r, k],
            near[ORDERS[r % PARTS][STEPS - 1 - k]],
        )

    def reduce_step(r, k):
        reduce_copy(r, k).wait_recv()
        h, o = half[k], offset[k]
        if k < STEPS - 1:
            n = h // 2
            gbuf[r, n:h] = gbuf[r, n:h] + rbuf[r, o + n : o + h]
            start(reduce_copy(r, k + 1))
            gbuf[r, 0:n] = gbuf[r, 0:n] + rbuf[r, o : o + n]

    def weight_grad(m, j, right):
        per = width // 4 // shard

        def some(i, carry):
            out = jnp.dot(
                tokt[m, pl.ds(pl.multiple_of(i * (width // 4), width // 4), width // 4), :],
                right(),
                preferred_element_type=jnp.float32,
            )
            for t in range(per):
                rel = relative(i * per + t)
                for e in range(2):
                    p = 2 * j + e
                    gbuf[(1 - m) * PARTS + p, slot(rel, p)] = out[
                        t * shard : (t + 1) * shard, e * cols : (e + 1) * cols
                    ]
            return carry

        lax.fori_loop(0, 4, some, 0)

    total = 4 * rows
    for j in range(blocks):

        def activate(g, carry, j=j):
            kept = pre[g, :, part_cols(j)]
            act[pl.ds(pl.multiple_of(g * rows, rows), rows), :] = (kept * kept).astype(jnp.bfloat16)
            return carry

        lax.fori_loop(0, 4, activate, 0)
        weight_grad(1, j, lambda: act[...])
        start(reduce_copy(2 * j, 0))
        start(reduce_copy(2 * j + 1, 0))

    for j in range(blocks):

        def back(g, carry, j=j):
            value = jnp.dot(tok[1, g], wn[1, :, part_cols(j)], preferred_element_type=jnp.float32)
            gpre[pl.ds(pl.multiple_of(g * rows, rows), rows), part_cols(j)] = (
                2.0 * pre[g, :, part_cols(j)] * value
            ).astype(jnp.bfloat16)
            return carry

        lax.fori_loop(0, 4, back, 0)
        weight_grad(0, j, lambda j=j: gpre[:, part_cols(j)])
        start(reduce_copy(PARTS + 2 * j, 0))
        start(reduce_copy(PARTS + 2 * j + 1, 0))
        reduce_step(2 * j, 0)
        reduce_step(2 * j + 1, 0)

    def inputs_grad(n, carry):
        columns = pl.ds(pl.multiple_of(n * bw, bw), bw)
        w = wn[0, pl.ds(pl.multiple_of(n * bw, bw), bw), :]
        for g in range(4):
            pre[g, :, columns] = contract(gpre[g * rows : (g + 1) * rows, :], w, 1, 1)
        return carry

    lax.fori_loop(0, width // bw, inputs_grad, 0)

    def share_copy(i):
        return remote(pre.at[1 + 2 * i], part_in.at[i], pi_s.at[i], pi_r.at[i], sibling)

    def pair_copy(q):
        return remote(
            pair_in.at[0, pl.ds(q * chunk, chunk)],
            pair_in.at[1, pl.ds(q * chunk, chunk)],
            li_s.at[q],
            li_r.at[q],
            pair,
        )

    start(share_copy(1))
    start(share_copy(0))
    for p in range(PARTS):
        reduce_step(p, 1)
    share_copy(1).wait_recv()
    for q in range(pieces):
        s = slice(q * chunk, (q + 1) * chunk)
        pair_in[0, s] = pre[2, s] + part_in[1, s]
        start(pair_copy(q))
    share_copy(0).wait_recv()
    pre[0] = pre[0] + part_in[0]
    for p in range(PARTS):
        reduce_step(PARTS + p, 0)
    for p in range(PARTS):
        reduce_step(p, 2)
    for p in range(PARTS):
        reduce_step(PARTS + p, 1)
    for p in range(PARTS):
        reduce_step(p, 3)

    def twin_copy(r):
        place = outs.at[r // PARTS, :, pl.ds(pl.multiple_of(base + (r % PARTS) * cols, cols), cols)]
        return remote(place, place, rep_s.at[r], rep_r.at[r], twin)

    def finish(r):
        reduce_step(r, STEPS - 1)
        value = (gbuf[r, 0] + rbuf[r, 30]) * factor
        outs[r // PARTS, :, pl.ds(pl.multiple_of(base + (r % PARTS) * cols, cols), cols)] = value
        start(twin_copy(r))
        return value

    for p in range(PARTS):
        value = finish(p)
        ebuf[0, p : p + 1, :] = jnp.sum(value * value, axis=0, keepdims=True)

    def energy_copy(k):
        if k < STEPS:
            return remote(ebuf.at[k], esum.at[k], e_s.at[k], e_r.at[k], near[k])
        return remote(ebuf.at[k], esum.at[k], e_s.at[k], e_r.at[k], twin)

    def energy_step(k):
        energy_copy(k).wait_recv()
        ebuf[k + 1] = ebuf[k] + esum[k]
        start(energy_copy(k + 1))

    start(energy_copy(0))
    for p in range(PARTS):
        reduce_step(PARTS + p, 2)
    energy_step(0)
    for p in range(PARTS):
        reduce_step(PARTS + p, 3)
    energy_step(1)
    for p in range(PARTS):
        finish(PARTS + p)
    energy_step(2)
    energy_step(3)
    energy_step(4)
    for q in range(pieces):
        pair_copy(q).wait_recv()
    gin_ref[...] = (pre[0] + pair_in[1]).astype(jnp.bfloat16)
    for p in range(PARTS):
        twin_copy(p).wait_recv()
    gdn_ref[...] = outs[0]
    for p in range(PARTS):
        twin_copy(PARTS + p).wait_recv()
    gup = outs[1]
    gup_ref[...] = gup
    own = jnp.sum(gup * gup, axis=1, keepdims=True)
    eup_own[...] = jnp.broadcast_to(own, eup_own.shape)
    up_copy = remote(eup_own, eup_in, eu_s, eu_r, sibling)
    start(up_copy)
    energy_copy(STEPS).wait_recv()
    edn_ref[rep] = ebuf[STEPS] * (1.0 / width)
    edn_ref[1 - rep] = esum[STEPS] * (1.0 / width)
    up_copy.wait_recv()
    eup_ref[...] = (eup_own[...] + eup_in[...]) * (1.0 / (hidden * 4))
    for copy in pending:
        copy.wait_send()


def body(inputs, up_proj, down_proj, out_cotangent):
    rows, width = inputs.shape
    shard, both = up_proj.shape
    hidden = both // 2
    cols = hidden // PARTS
    factor = float(rows * lax.axis_size("rep") * lax.axis_size("fs") * lax.axis_size("tp")) ** (-0.5)
    f32, bf16 = jnp.float32, jnp.bfloat16
    shape = jax.ShapeDtypeStruct
    vmem = pl.BlockSpec(memory_space=pltpu.VMEM)
    dma = pltpu.SemaphoreType.DMA
    gin, gup, gdn, eup, edn = pl.pallas_call(
        functools.partial(kernel, factor),
        out_shape=(
            shape((rows, width), bf16),
            shape((shard, both), f32),
            shape((shard, both), f32),
            shape((shard, 128), f32),
            shape((2, PARTS, cols), f32),
        ),
        in_specs=[vmem] * 4,
        out_specs=(vmem,) * 5,
        scratch_shapes=[
            pltpu.VMEM((2, 4, rows, width), bf16),
            pltpu.VMEM((2, width, 4 * rows), bf16),
            pltpu.VMEM((2, PARTS, 32, shard, cols), bf16),
            pltpu.VMEM((2, width, hidden), bf16),
            pltpu.VMEM((4, rows, max(hidden, width)), f32),
            pltpu.VMEM((4 * rows, 2 * cols), bf16),
            pltpu.VMEM((4 * rows, hidden), bf16),
            pltpu.VMEM((2 * PARTS, 32, shard, cols), f32),
            pltpu.VMEM((2 * PARTS, 31, shard, cols), f32),
            pltpu.VMEM((2, rows, width), f32),
            pltpu.VMEM((2, rows, width), f32),
            pltpu.VMEM((8, 128), f32),
            pltpu.VMEM((2, shard, both), f32),
            pltpu.VMEM((STEPS + 1, PARTS, cols), f32),
            pltpu.VMEM((STEPS + 1, PARTS, cols), f32),
            pltpu.VMEM((shard, 128), f32),
            pltpu.VMEM((shard, 128), f32),
            dma((2, 2)),
            dma((2, 2)),
            dma((2, 2)),
            dma((2, 2)),
            dma((2,)),
            dma((2,)),
            dma((2 * PARTS, STEPS)),
            dma((2 * PARTS, STEPS)),
            dma((2 * PARTS, STEPS)),
            dma((2 * PARTS, STEPS)),
            dma((2 * PARTS,)),
            dma((2 * PARTS,)),
            dma((2,)),
            dma((2,)),
            dma((2,)),
            dma((2,)),
            dma((STEPS + 1,)),
            dma((STEPS + 1,)),
            dma,
            dma,
        ],
        compiler_params=pltpu.CompilerParams(
            collective_id=0, has_side_effects=True, vmem_limit_bytes=60 * 2**20
        ),
        name="step",
    )(inputs, out_cotangent, up_proj, down_proj.T)
    return gin, gup, gdn.T, eup[:, 0], edn.reshape((both,))


def solution(mesh):
    return jax.shard_map(
        body,
        mesh=mesh,
        in_specs=(
            P(("rep", "fs", "tp"), None),
            P("fs", "tp"),
            P("tp", "fs"),
            P(("rep", "fs", "tp"), None),
        ),
        out_specs=(P(("rep", "fs", "tp"), None), P("fs", "tp"), P("tp", "fs"), P("fs"), P("tp")),
        check_vma=False,
    )
```

```python
import functools

import jax
import jax.numpy as jnp
from jax import lax
from jax.experimental import pallas as pl
from jax.experimental.pallas import tpu as pltpu
from jax.sharding import PartitionSpec as P

MESH = pl.DeviceIdType.MESH
ORDERS = (
    (0, 4, 1, 2, 3),
    (2, 3, 4, 0, 1),
    (1, 0, 3, 4, 2),
    (3, 2, 1, 4, 0),
    (3, 0, 2, 4, 1),
    (2, 1, 0, 4, 3),
    (0, 1, 4, 3, 2),
    (3, 2, 1, 4, 0),
)
STEPS = 5
SPLIT = 2
PARTS = len(ORDERS)


def bits_of(fs):
    z, y, x = fs // 16, (fs // 4) % 4, fs % 4
    return (z, (y % 2 + y // 2) % 2, y // 2, (x % 2 + x // 2) % 2, x // 2)


def partners_of(fs):
    z, y, x = fs // 16, (fs // 4) % 4, fs % 4
    return (
        fs + 16 - 32 * z,
        fs + 4 - 8 * (y % 2),
        fs + 12 - 8 * y,
        fs + 1 - 2 * (x % 2),
        fs + 3 - 2 * x,
    )


def remote(src, dst, send, recv, device):
    return pltpu.make_async_remote_copy(
        src_ref=src, dst_ref=dst, send_sem=send, recv_sem=recv, device_id=device, device_id_type=MESH
    )


def contract(left, right, left_dim, right_dim):
    return lax.dot_general(
        left, right, (((left_dim,), (right_dim,)), ((), ())), preferred_element_type=jnp.float32
    )


def kernel(
    factor,
    x_ref,
    c_ref,
    u_ref,
    d_ref,
    gin_ref,
    gup_ref,
    gdn_ref,
    eup_ref,
    edn_ref,
    tok,
    tokt,
    wg,
    wn,
    pre,
    act,
    gpre,
    gbuf,
    rbuf,
    part_in,
    pair_in,
    outs,
    ebuf,
    esum,
    eup_own,
    eup_in,
    tok_s,
    tok_r,
    fwd_s,
    fwd_r,
    sib_s,
    sib_r,
    g_s,
    g_r,
    r_s,
    r_r,
    rep_s,
    rep_r,
    pi_s,
    pi_r,
    li_s,
    li_r,
    e_s,
    e_r,
    eu_s,
    eu_r,
):
    rep, fs, tp = lax.axis_index("rep"), lax.axis_index("fs"), lax.axis_index("tp")
    mine = bits_of(fs)
    near = [{"fs": other} for other in partners_of(fs)]
    sibling = {"tp": 1 - tp}
    pair = {"rep": 1 - rep, "fs": partners_of(fs)[0]}
    twin = {"rep": 1 - rep}
    rows, width = x_ref.shape
    shard = u_ref.shape[0]
    hidden = u_ref.shape[1] // 2
    cols = hidden // PARTS
    base = rep * hidden
    weights = (u_ref, d_ref)
    tokens = (x_ref, c_ref)
    pieces = 2
    chunk = rows // pieces

    barrier = pltpu.get_barrier_semaphore()
    for device in near + [sibling, pair, twin]:
        pl.semaphore_signal(barrier, inc=1, device_id=device, device_id_type=MESH)

    for m in range(2):
        tok[m, 0:rows] = tokens[m][...]
        for p in range(PARTS):
            wg[m, p, 0] = weights[m][:, pl.ds(pl.multiple_of(base + p * cols, cols), cols)]

    pl.semaphore_wait(barrier, STEPS + 3)

    pending = []

    def start(copy):
        copy.start()
        pending.append(copy)
        return copy

    def token_copy(m, q):
        return remote(
            tokens[m].at[pl.ds(q * chunk, chunk)],
            tok.at[m, pl.ds(2 * rows + q * chunk, chunk)],
            tok_s.at[m, q],
            tok_r.at[m, q],
            pair,
        )

    def forward_copy(m, q):
        return remote(
            tok.at[m, pl.ds(2 * rows + q * chunk, chunk)],
            tok.at[m, pl.ds(3 * rows + q * chunk, chunk)],
            fwd_s.at[m, q],
            fwd_r.at[m, q],
            sibling,
        )

    def sibling_copy(m):
        return remote(tokens[m], tok.at[m, pl.ds(rows, rows)], sib_s.at[m], sib_r.at[m], sibling)

    def gather_copy(m, p, k):
        if k == 0:
            src = weights[m].at[:, pl.ds(pl.multiple_of(base + p * cols, cols), cols)]
            dst = wg.at[m, p, 1]
        else:
            src = wg.at[m, p, pl.ds(0, 2**k)]
            dst = wg.at[m, p, pl.ds(2**k, 2**k)]
        return remote(src, dst, g_s.at[m * PARTS + p, k], g_r.at[m * PARTS + p, k], near[ORDERS[p][k]])

    def gather_step(m, k):
        for p in range(PARTS):
            if k > 0:
                gather_copy(m, p, k - 1).wait_recv()
            start(gather_copy(m, p, k))

    def forward(m, q):
        token_copy(m, q).wait_recv()
        start(forward_copy(m, q))

    for m in range(2):
        gather_step(m, 0)
        for q in range(pieces):
            start(token_copy(m, q))
    for m in range(2):
        start(sibling_copy(m))

    def transpose(m, g):
        tokt[m, :, g * rows : (g + 1) * rows] = tok[m, g * rows : (g + 1) * rows].T

    gather_step(0, 1)
    gather_step(1, 1)
    gather_step(0, 2)
    gather_step(1, 2)
    for m in range(2):
        transpose(m, 0)
        sibling_copy(m).wait_recv()
        transpose(m, 1)
    forward(0, 0)
    gather_step(0, 3)
    gather_step(1, 3)
    forward(0, 1)
    gather_step(0, 4)
    gather_step(1, 4)

    flip = [(bit, 1 - bit) for bit in mine]
    tables = {}

    def slot(s, p):
        order = ORDERS[p]
        if order not in tables:
            place = {d: 2**k for k, d in enumerate(order)}
            high, low = [], []
            for v in range(8):
                bits = bits_of(4 * v)
                high.append(sum(flip[d][bits[d]] * place[d] for d in (0, 1, 2)))
            for v in range(4):
                bits = bits_of(v)
                low.append(sum(flip[d][bits[d]] * place[d] for d in (3, 4)))
            tables[order] = high, low
        high, low = tables[order]
        return high[s // 4] + low[s % 4]

    def unpack(m, p):
        gather_copy(m, p, STEPS - 1).wait_recv()
        for s in range(32):
            wn[m, s * shard : (s + 1) * shard, p * cols : (p + 1) * cols] = wg[m, p, slot(s, p)]

    for q in range(pieces):
        forward_copy(0, q).wait_recv()
    transpose(0, 2)
    transpose(0, 3)
    blocks = PARTS // 2
    bw = 2 * cols
    total = 4 * rows
    big = total // SPLIT

    def part_cols(j):
        return slice(j * bw, (j + 1) * bw)

    for j in range(blocks):
        unpack(0, 2 * j)
        unpack(0, 2 * j + 1)

        for i in range(total // big):
            pre[i * big : (i + 1) * big, part_cols(j)] = jnp.maximum(
                jnp.dot(
                    tok[0, i * big : (i + 1) * big],
                    wn[0, :, part_cols(j)],
                    preferred_element_type=jnp.float32,
                ),
                0.0,
            )

    for q in range(pieces):
        forward(1, q)
    for j in range(blocks):
        unpack(1, 2 * j)
        unpack(1, 2 * j + 1)
    for q in range(pieces):
        forward_copy(1, q).wait_recv()
    transpose(1, 2)
    transpose(1, 3)

    offset = (0, 16, 24, 28, 30)
    half = (16, 8, 4, 2, 1)

    def reduce_copy(r, k):
        return remote(
            gbuf.at[r, pl.ds(half[k], half[k])],
            rbuf.at[r, pl.ds(offset[k], half[k])],
            r_s.at[r, k],
            r_r.at[r, k],
            near[ORDERS[r % PARTS][STEPS - 1 - k]],
        )

    def reduce_step(r, k):
        reduce_copy(r, k).wait_recv()
        h, o = half[k], offset[k]
        if k < STEPS - 1:
            n = h // 2
            gbuf[r, n:h] = gbuf[r, n:h] + rbuf[r, o + n : o + h]
            start(reduce_copy(r, k + 1))
            gbuf[r, 0:n] = gbuf[r, 0:n] + rbuf[r, o : o + n]

    def weight_grad(m, j, right):
        tall = width // SPLIT
        per = tall // shard
        for i in range(SPLIT):
            out = jnp.dot(
                tokt[m, i * tall : (i + 1) * tall, :], right(), preferred_element_type=jnp.float32
            )
            for t in range(per):
                for e in range(2):
                    p = 2 * j + e
                    gbuf[(1 - m) * PARTS + p, slot(i * per + t, p)] = out[
                        t * shard : (t + 1) * shard, e * cols : (e + 1) * cols
                    ]

    for j in range(blocks):
        kept = pre[:, part_cols(j)]
        act[...] = (kept * kept).astype(jnp.bfloat16)
        weight_grad(1, j, lambda: act[...])
        start(reduce_copy(2 * j, 0))
        start(reduce_copy(2 * j + 1, 0))

    for j in range(blocks):
        for i in range(SPLIT):
            part = slice(i * big, (i + 1) * big)
            value = jnp.dot(tok[1, part], wn[1, :, part_cols(j)], preferred_element_type=jnp.float32)
            gpre[part, part_cols(j)] = (2.0 * pre[part, part_cols(j)] * value).astype(jnp.bfloat16)
        weight_grad(0, j, lambda j=j: gpre[:, part_cols(j)])
        start(reduce_copy(PARTS + 2 * j, 0))
        start(reduce_copy(PARTS + 2 * j + 1, 0))
        reduce_step(2 * j, 0)
        reduce_step(2 * j + 1, 0)

    for n in range(width // bw):
        w = wn[0, n * bw : (n + 1) * bw, :]
        for i in range(SPLIT):
            part = slice(i * big, (i + 1) * big)
            pre[part, n * bw : (n + 1) * bw] = contract(gpre[part, :], w, 1, 1)

    def share_copy(i):
        return remote(pre.at[pl.ds((1 + 2 * i) * rows, rows)], part_in.at[i], pi_s.at[i], pi_r.at[i], sibling)

    def pair_copy(q):
        return remote(
            pair_in.at[0, pl.ds(q * chunk, chunk)],
            pair_in.at[1, pl.ds(q * chunk, chunk)],
            li_s.at[q],
            li_r.at[q],
            pair,
        )

    start(share_copy(1))
    start(share_copy(0))
    for p in range(PARTS):
        reduce_step(p, 1)
    share_copy(1).wait_recv()
    for q in range(pieces):
        s = slice(q * chunk, (q + 1) * chunk)
        pair_in[0, s] = pre[2 * rows + q * chunk : 2 * rows + (q + 1) * chunk] + part_in[1, s]
        start(pair_copy(q))
    share_copy(0).wait_recv()
    pre[0:rows] = pre[0:rows] + part_in[0]
    for p in range(PARTS):
        reduce_step(PARTS + p, 0)
    for p in range(PARTS):
        reduce_step(p, 2)
    for p in range(PARTS):
        reduce_step(PARTS + p, 1)
    for p in range(PARTS):
        reduce_step(p, 3)

    def twin_copy(r):
        place = outs.at[r // PARTS, :, pl.ds(pl.multiple_of(base + (r % PARTS) * cols, cols), cols)]
        return remote(place, place, rep_s.at[r], rep_r.at[r], twin)

    def finish(r):
        reduce_step(r, STEPS - 1)
        value = (gbuf[r, 0] + rbuf[r, 30]) * factor
        outs[r // PARTS, :, pl.ds(pl.multiple_of(base + (r % PARTS) * cols, cols), cols)] = value
        start(twin_copy(r))
        return value

    for p in range(PARTS):
        value = finish(p)
        ebuf[0, p : p + 1, :] = jnp.sum(value * value, axis=0, keepdims=True)

    def energy_copy(k):
        if k < STEPS:
            return remote(ebuf.at[k], esum.at[k], e_s.at[k], e_r.at[k], near[k])
        return remote(ebuf.at[k], esum.at[k], e_s.at[k], e_r.at[k], twin)

    def energy_step(k):
        energy_copy(k).wait_recv()
        ebuf[k + 1] = ebuf[k] + esum[k]
        start(energy_copy(k + 1))

    start(energy_copy(0))
    for p in range(PARTS):
        reduce_step(PARTS + p, 2)
    energy_step(0)
    for p in range(PARTS):
        reduce_step(PARTS + p, 3)
    energy_step(1)
    for p in range(PARTS):
        finish(PARTS + p)
    energy_step(2)
    energy_step(3)
    energy_step(4)
    for q in range(pieces):
        pair_copy(q).wait_recv()
    gin_ref[...] = (pre[0:rows] + pair_in[1]).astype(jnp.bfloat16)
    for p in range(PARTS):
        twin_copy(p).wait_recv()
    gdn_ref[...] = outs[0]
    for p in range(PARTS):
        twin_copy(PARTS + p).wait_recv()
    gup = outs[1]
    gup_ref[...] = gup
    own = jnp.sum(gup * gup, axis=1, keepdims=True)
    eup_own[...] = jnp.broadcast_to(own, eup_own.shape)
    up_copy = remote(eup_own, eup_in, eu_s, eu_r, sibling)
    start(up_copy)
    energy_copy(STEPS).wait_recv()
    edn_ref[rep] = ebuf[STEPS] * (1.0 / width)
    edn_ref[1 - rep] = esum[STEPS] * (1.0 / width)
    up_copy.wait_recv()
    eup_ref[...] = (eup_own[...] + eup_in[...]) * (1.0 / (hidden * 4))
    for copy in pending:
        copy.wait_send()


def body(inputs, up_proj, down_proj, out_cotangent):
    rows, width = inputs.shape
    shard, both = up_proj.shape
    hidden = both // 2
    cols = hidden // PARTS
    factor = float(rows * lax.axis_size("rep") * lax.axis_size("fs") * lax.axis_size("tp")) ** (-0.5)
    f32, bf16 = jnp.float32, jnp.bfloat16
    shape = jax.ShapeDtypeStruct
    vmem = pl.BlockSpec(memory_space=pltpu.VMEM)
    dma = pltpu.SemaphoreType.DMA
    gin, gup, gdn, eup, edn = pl.pallas_call(
        functools.partial(kernel, factor),
        out_shape=(
            shape((rows, width), bf16),
            shape((shard, both), f32),
            shape((shard, both), f32),
            shape((shard, 128), f32),
            shape((2, PARTS, cols), f32),
        ),
        in_specs=[vmem] * 4,
        out_specs=(vmem,) * 5,
        scratch_shapes=[
            pltpu.VMEM((2, 4 * rows, width), bf16),
            pltpu.VMEM((2, width, 4 * rows), bf16),
            pltpu.VMEM((2, PARTS, 32, shard, cols), bf16),
            pltpu.VMEM((2, width, hidden), bf16),
            pltpu.VMEM((4 * rows, max(hidden, width)), f32),
            pltpu.VMEM((4 * rows, 2 * cols), bf16),
            pltpu.VMEM((4 * rows, hidden), bf16),
            pltpu.VMEM((2 * PARTS, 32, shard, cols), f32),
            pltpu.VMEM((2 * PARTS, 31, shard, cols), f32),
            pltpu.VMEM((2, rows, width), f32),
            pltpu.VMEM((2, rows, width), f32),
            pltpu.VMEM((2, shard, both), f32),
            pltpu.VMEM((STEPS + 1, PARTS, cols), f32),
            pltpu.VMEM((STEPS + 1, PARTS, cols), f32),
            pltpu.VMEM((shard, 128), f32),
            pltpu.VMEM((shard, 128), f32),
            dma((2, 2)),
            dma((2, 2)),
            dma((2, 2)),
            dma((2, 2)),
            dma((2,)),
            dma((2,)),
            dma((2 * PARTS, STEPS)),
            dma((2 * PARTS, STEPS)),
            dma((2 * PARTS, STEPS)),
            dma((2 * PARTS, STEPS)),
            dma((2 * PARTS,)),
            dma((2 * PARTS,)),
            dma((2,)),
            dma((2,)),
            dma((2,)),
            dma((2,)),
            dma((STEPS + 1,)),
            dma((STEPS + 1,)),
            dma,
            dma,
        ],
        compiler_params=pltpu.CompilerParams(
            collective_id=0, has_side_effects=True, vmem_limit_bytes=60 * 2**20
        ),
        name="step",
    )(inputs, out_cotangent, up_proj, down_proj.T)
    return gin, gup, gdn.T, eup[:, 0], edn.reshape((both,))


def solution(mesh):
    return jax.shard_map(
        body,
        mesh=mesh,
        in_specs=(
            P(("rep", "fs", "tp"), None),
            P("fs", "tp"),
            P("tp", "fs"),
            P(("rep", "fs", "tp"), None),
        ),
        out_specs=(P(("rep", "fs", "tp"), None), P("fs", "tp"), P("tp", "fs"), P("fs"), P("tp")),
        check_vma=False,
    )
```

```python
import functools

import jax
import jax.numpy as jnp
from jax import lax
from jax.experimental import pallas as pl
from jax.experimental.pallas import tpu as pltpu
from jax.sharding import PartitionSpec as P

MESH = pl.DeviceIdType.MESH
SIZES = ((3, 3, 3, 3, 4), (4, 3, 3, 3, 3))
STARTS = tuple(tuple(sum(size[:i]) for i in range(5)) for size in SIZES)
STEPS = 5
PARTS = 5
SPLIT = 2
ORDERS = tuple(tuple((i + 1 + k) % 5 for k in range(STEPS)) for i in range(PARTS))
UNITS = 16
BLOCKS = 8
HALF = (16, 8, 4, 2, 1)
SPAN = 240.0
SHIFT = 120.0


def encode(value, scale):
    code = jnp.exp2(jnp.abs(value) * (SPAN / scale) - SHIFT)
    return jnp.where(value < 0.0, -code, code).astype(jnp.bfloat16)


def decode(code, scale):
    code = code.astype(jnp.float32)
    size = (jnp.log2(jnp.abs(code)) + SHIFT) * (scale * (1.0 / SPAN))
    return jnp.where(code < 0.0, -size, size)


def scale_of(top):
    return (top * 1.01 + 1e-35).astype(jnp.bfloat16)


def bits_of(fs):
    z, y, x = fs // 16, (fs // 4) % 4, fs % 4
    return (z, (y % 2 + y // 2) % 2, y // 2, (x % 2 + x // 2) % 2, x // 2)


def partners_of(fs):
    z, y, x = fs // 16, (fs // 4) % 4, fs % 4
    return (
        fs + 16 - 32 * z,
        fs + 4 - 8 * (y % 2),
        fs + 12 - 8 * y,
        fs + 1 - 2 * (x % 2),
        fs + 3 - 2 * x,
    )


def remote(src, dst, send, recv, device):
    return pltpu.make_async_remote_copy(
        src_ref=src, dst_ref=dst, send_sem=send, recv_sem=recv, device_id=device, device_id_type=MESH
    )


def contract(left, right, left_dim, right_dim):
    return lax.dot_general(
        left, right, (((left_dim,), (right_dim,)), ((), ())), preferred_element_type=jnp.float32
    )


def kernel(
    factor,
    x_ref,
    c_ref,
    u_ref,
    d_ref,
    gin_ref,
    gup_ref,
    gdn_ref,
    eup_ref,
    edn_ref,
    tok,
    tokt,
    wg,
    wn,
    pre,
    act,
    gpre,
    gbuf,
    sbuf,
    rbuf,
    part_in,
    pair_out,
    pair_in,
    outs,
    ebuf,
    esum,
    eup_own,
    eup_in,
    tok_s,
    tok_r,
    fwd_s,
    fwd_r,
    sib_s,
    sib_r,
    g_s,
    g_r,
    r_s,
    r_r,
    rep_s,
    rep_r,
    pi_s,
    pi_r,
    li_s,
    li_r,
    e_s,
    e_r,
    eu_s,
    eu_r,
):
    rep, fs, tp = lax.axis_index("rep"), lax.axis_index("fs"), lax.axis_index("tp")
    mine = bits_of(fs)
    near = [{"fs": other} for other in partners_of(fs)]
    sibling = {"tp": 1 - tp}
    pair = {"rep": 1 - rep, "fs": partners_of(fs)[0]}
    twin = {"rep": 1 - rep}
    rows, width = x_ref.shape
    shard = u_ref.shape[0]
    hidden = u_ref.shape[1] // 2
    base = rep * hidden
    weights = (u_ref, d_ref)
    tokens = (x_ref, c_ref)
    pieces = 2
    chunk = rows // pieces
    half_rows = 2 * rows
    bw = 256
    blocks = hidden // bw
    all_parts = range(PARTS)
    f32, bf16 = jnp.float32, jnp.bfloat16

    flip = [(bit, 1 - bit) for bit in mine]
    tables = {}

    def unit(m, s, u):
        p = max(i for i in all_parts if STARTS[m][i] <= u)
        size = SIZES[m][p]
        if (p, size) not in tables:
            place = {d: size * 2**k for k, d in enumerate(ORDERS[p])}
            high, low = [], []
            for v in range(8):
                bits = bits_of(4 * v)
                high.append(sum(flip[d][bits[d]] * place[d] for d in (0, 1, 2)))
            for v in range(4):
                bits = bits_of(v)
                low.append(sum(flip[d][bits[d]] * place[d] for d in (3, 4)))
            tables[p, size] = high, low
        high, low = tables[p, size]
        return high[s // 4] + low[s % 4] + (m * UNITS * 32 + STARTS[m][p] * 32 + u - STARTS[m][p])

    def home(m, p):
        return m * UNITS * 32 + STARTS[m][p] * 32

    barrier = pltpu.get_barrier_semaphore()
    for device in near + [sibling, pair, twin]:
        pl.semaphore_signal(barrier, inc=1, device_id=device, device_id_type=MESH)

    for m in range(2):
        tok[m, 0:rows] = tokens[m][...]
        for p in all_parts:
            for i in range(SIZES[m][p]):
                block, row = divmod(STARTS[m][p] + i, 2)
                wg[home(m, p) + i] = weights[m][
                    row * 16 : row * 16 + 16, pl.ds(pl.multiple_of(base + block * 128, 128), 128)
                ]

    pl.semaphore_wait(barrier, STEPS + 3)

    pending = []

    def start(copy):
        copy.start()
        pending.append(copy)
        return copy

    def token_copy(m, q):
        return remote(
            tokens[m].at[pl.ds(q * chunk, chunk)],
            tok.at[m, pl.ds(2 * rows + q * chunk, chunk)],
            tok_s.at[m, q],
            tok_r.at[m, q],
            pair,
        )

    def forward_copy(m, q):
        return remote(
            tok.at[m, pl.ds(2 * rows + q * chunk, chunk)],
            tok.at[m, pl.ds(3 * rows + q * chunk, chunk)],
            fwd_s.at[m, q],
            fwd_r.at[m, q],
            sibling,
        )

    def sibling_copy(m):
        return remote(tokens[m], tok.at[m, pl.ds(rows, rows)], sib_s.at[m], sib_r.at[m], sibling)

    def gather_copy(m, p, k):
        n = SIZES[m][p] * 2**k
        return remote(
            wg.at[pl.ds(home(m, p), n)],
            wg.at[pl.ds(home(m, p) + n, n)],
            g_s.at[m, p, k],
            g_r.at[m, p, k],
            near[ORDERS[p][k]],
        )

    def gather_step(m, k):
        for p in all_parts:
            if k > 0:
                gather_copy(m, p, k - 1).wait_recv()
            start(gather_copy(m, p, k))

    def forward(m, q):
        token_copy(m, q).wait_recv()
        start(forward_copy(m, q))

    def transpose(m, g):
        tokt[m, :, g * rows : (g + 1) * rows] = tok[m, g * rows : (g + 1) * rows].T

    def unpack(m):
        for p in all_parts:
            gather_copy(m, p, STEPS - 1).wait_recv()
            for u in range(STARTS[m][p], STARTS[m][p] + SIZES[m][p]):
                block, row = divmod(u, 2)
                for s in range(32):
                    top = s * shard + row * 16
                    wn[m, top : top + 16, block * 128 : block * 128 + 128] = wg[unit(m, s, u)]

    def part_cols(j):
        return slice(j * bw, (j + 1) * bw)

    def forward_half(h):
        part = slice(h * half_rows, (h + 1) * half_rows)
        for j in range(blocks):
            kept = jnp.maximum(
                jnp.dot(tok[0, part], wn[0, :, part_cols(j)], preferred_element_type=f32), 0.0
            )
            pre[part, part_cols(j)] = kept
            act[part, part_cols(j)] = (kept * kept).astype(bf16)

    def back_half(h):
        part = slice(h * half_rows, (h + 1) * half_rows)
        for j in range(blocks):
            value = jnp.dot(tok[1, part], wn[1, :, part_cols(j)], preferred_element_type=f32)
            gpre[part, part_cols(j)] = (2.0 * pre[part, part_cols(j)] * value).astype(bf16)

    def room(m, p, k):
        before = sum(1 + HALF[i] * SIZES[m][p] for i in range(k))
        return m * (31 * UNITS + 25) + 31 * STARTS[m][p] + 5 * p + before

    def reduce_copy(m, p, k):
        n = 1 + HALF[k] * SIZES[m][p]
        place = pl.ds(room(m, p, k), n)
        return remote(
            sbuf.at[place], rbuf.at[place], r_s.at[m, p, k], r_r.at[m, p, k], near[ORDERS[p][STEPS - 1 - k]]
        )

    def chunks(count, size):
        step = min(count, 4) * size
        return count * size // step, step

    def highest(m, p, k):
        n = SIZES[m][p]
        loops, step = chunks(HALF[k], n)
        at = home(m, p) + HALF[k] * n

        def some(i, top):
            return jnp.maximum(top, jnp.max(jnp.abs(gbuf[pl.ds(at + i * step, step)]), axis=0))

        return lax.fori_loop(0, loops, some, jnp.zeros((16, 128), f32))

    def send_sums(m, p, k, top):
        n = SIZES[m][p]
        loops, step = chunks(HALF[k], n)
        at, to = home(m, p) + HALF[k] * n, room(m, p, k)
        coded = scale_of(top)
        sbuf[to] = coded
        scale = coded.astype(f32)

        def some(i, carry):
            sbuf[pl.ds(to + 1 + i * step, step)] = encode(gbuf[pl.ds(at + i * step, step)], scale)
            return carry

        lax.fori_loop(0, loops, some, 0)
        start(reduce_copy(m, p, k))

    def begin(m, p):
        send_sums(m, p, 0, highest(m, p, 0))

    def add_sums(m, p, k, first, count):
        n = SIZES[m][p]
        loops, step = chunks(count, n)
        at, got = home(m, p) + first * n, room(m, p, k) + 1 + first * n
        scale = rbuf[room(m, p, k)].astype(f32)

        def some(i, top):
            place = pl.ds(at + i * step, step)
            value = gbuf[place] + decode(rbuf[pl.ds(got + i * step, step)], scale)
            gbuf[place] = value
            return jnp.maximum(top, jnp.max(jnp.abs(value), axis=0))

        return lax.fori_loop(0, loops, some, jnp.zeros((16, 128), f32))

    def reduce_step(m, k):
        for p in all_parts:
            reduce_copy(m, p, k).wait_recv()
            n = HALF[k + 1]
            top = add_sums(m, p, k, n, n)
            send_sums(m, p, k + 1, top)
            add_sums(m, p, k, 0, n)

    def weight_grad(m, right):
        tall = width // SPLIT
        done = 0
        for j in range(blocks):
            for i in range(SPLIT):
                out = jnp.dot(
                    tokt[m, i * tall : (i + 1) * tall, :], right[:, part_cols(j)], preferred_element_type=f32
                )
                for t in range(tall // shard):
                    for u in range(4):
                        block, row = divmod(u, 2)
                        gbuf[unit(m, i * (tall // shard) + t, 4 * j + u)] = out[
                            t * shard + row * 16 : t * shard + row * 16 + 16, block * 128 : block * 128 + 128
                        ]
            while done < PARTS and STARTS[m][done] + SIZES[m][done] <= 4 * (j + 1):
                begin(m, done)
                done += 1

    def share_copy(i):
        return remote(
            pre.at[pl.ds((1 + 2 * i) * rows, rows)], part_in.at[i], pi_s.at[i], pi_r.at[i], sibling
        )

    def pair_copy(q):
        return remote(pair_out.at[q], pair_in.at[q], li_s.at[q], li_r.at[q], pair)

    for m in range(2):
        gather_step(m, 0)
        for q in range(pieces):
            start(token_copy(m, q))
    for m in range(2):
        start(sibling_copy(m))
    for k in (1, 2):
        for m in range(2):
            gather_step(m, k)
    for m in range(2):
        transpose(m, 0)
        sibling_copy(m).wait_recv()
        transpose(m, 1)
    gather_step(0, 3)
    gather_step(1, 3)
    forward(0, 0)
    gather_step(0, 4)
    forward(0, 1)
    gather_step(1, 4)
    unpack(0)
    forward_half(0)
    for q in range(pieces):
        forward_copy(0, q).wait_recv()
    forward_half(1)
    transpose(0, 2)
    transpose(0, 3)
    unpack(1)
    forward(1, 0)
    back_half(0)
    forward(1, 1)
    transpose(1, 2)
    for q in range(pieces):
        forward_copy(1, q).wait_recv()
    transpose(1, 3)

    weight_grad(1, act)
    back_half(1)
    weight_grad(0, gpre)
    reduce_step(1, 0)

    for i in (1, 0):
        part = slice(i * half_rows, (i + 1) * half_rows)
        for n in range(width // bw):
            pre[part, n * bw : (n + 1) * bw] = contract(
                gpre[part, :], wn[0, n * bw : (n + 1) * bw, :], 1, 1
            )
        start(share_copy(i))

    reduce_step(0, 0)
    share_copy(1).wait_recv()
    for q in range(pieces):
        s = slice(q * chunk, (q + 1) * chunk)
        value = pre[2 * rows + q * chunk : 2 * rows + (q + 1) * chunk] + part_in[1, s]
        coded = scale_of(jnp.max(jnp.abs(value), axis=0, keepdims=True))
        pair_out[q, 0:16] = jnp.broadcast_to(coded, (16, width))
        pair_out[q, 16 : 16 + chunk] = encode(value, coded.astype(f32))
        start(pair_copy(q))
    share_copy(0).wait_recv()
    pre[0:rows] = pre[0:rows] + part_in[0]
    reduce_step(1, 1)
    reduce_step(0, 1)
    reduce_step(1, 2)
    reduce_step(0, 2)
    reduce_step(1, 3)

    def twin_copy(m, p):
        place = outs.at[m, rep, pl.ds(STARTS[m][p], SIZES[m][p])]
        return remote(place, place, rep_s.at[m, p], rep_r.at[m, p], twin)

    def finish(m, p):
        n = SIZES[m][p]
        reduce_copy(m, p, STEPS - 1).wait_recv()
        scale = rbuf[room(m, p, STEPS - 1)].astype(f32)
        got = decode(rbuf[pl.ds(room(m, p, STEPS - 1) + 1, n)], scale)
        value = (gbuf[pl.ds(home(m, p), n)] + got) * factor
        outs[m, rep, pl.ds(STARTS[m][p], n)] = value
        start(twin_copy(m, p))
        return value

    sums = []
    for p in all_parts:
        value = finish(1, p)
        for i in range(SIZES[1][p]):
            sums.append(jnp.sum(value[i] * value[i], axis=0, keepdims=True))
    for i in range(BLOCKS):
        ebuf[0, i : i + 1, :] = sums[2 * i] + sums[2 * i + 1]

    def energy_copy(k):
        device = near[k] if k < STEPS else twin
        return remote(ebuf.at[k], esum.at[k], e_s.at[k], e_r.at[k], device)

    def energy_step(k):
        energy_copy(k).wait_recv()
        ebuf[k + 1] = ebuf[k] + esum[k]
        start(energy_copy(k + 1))

    start(energy_copy(0))
    reduce_step(0, 3)
    energy_step(0)
    for p in all_parts:
        finish(0, p)
    energy_step(1)
    for q in range(pieces):
        pair_copy(q).wait_recv()
        s = slice(q * chunk, (q + 1) * chunk)
        scale = pair_in[q, 0:16].astype(f32)[0:1]
        gin_ref[s] = (pre[s] + decode(pair_in[q, 16 : 16 + chunk], scale)).astype(bf16)
    energy_step(2)

    def write(m, ref):
        for p in all_parts:
            twin_copy(m, p).wait_recv()
        for r in range(2):
            for u in range(UNITS):
                block, row = divmod(u, 2)
                left = r * hidden + block * 128
                ref[row * 16 : row * 16 + 16, left : left + 128] = outs[m, r, u]

    write(1, gdn_ref)
    energy_step(3)
    energy_step(4)
    write(0, gup_ref)
    for row in range(2):
        squares = jnp.zeros((16, 128), f32)
        for r in range(2):
            for block in range(BLOCKS):
                value = outs[0, r, 2 * block + row]
                squares = squares + value * value
        eup_own[row * 16 : row * 16 + 16, :] = jnp.broadcast_to(
            jnp.sum(squares, axis=1, keepdims=True), (16, 128)
        )
    up_copy = start(remote(eup_own, eup_in, eu_s, eu_r, sibling))
    energy_copy(STEPS).wait_recv()
    edn_ref[rep] = ebuf[STEPS] * (1.0 / width)
    edn_ref[1 - rep] = esum[STEPS] * (1.0 / width)
    up_copy.wait_recv()
    eup_ref[...] = (eup_own[...] + eup_in[...]) * (1.0 / (hidden * 4))
    for copy in pending:
        copy.wait_send()


def body(inputs, up_proj, down_proj, out_cotangent):
    rows, width = inputs.shape
    shard, both = up_proj.shape
    hidden = both // 2
    factor = float(rows * lax.axis_size("rep") * lax.axis_size("fs") * lax.axis_size("tp")) ** (-0.5)
    f32, bf16 = jnp.float32, jnp.bfloat16
    shape = jax.ShapeDtypeStruct
    vmem = pl.BlockSpec(memory_space=pltpu.VMEM)
    dma = pltpu.SemaphoreType.DMA
    messages = 2 * (31 * UNITS + 25)
    gin, gup, gdn, eup, edn = pl.pallas_call(
        functools.partial(kernel, factor),
        out_shape=(
            shape((rows, width), bf16),
            shape((shard, both), f32),
            shape((shard, both), f32),
            shape((shard, 128), f32),
            shape((2, BLOCKS, 128), f32),
        ),
        in_specs=[vmem] * 4,
        out_specs=(vmem,) * 5,
        scratch_shapes=[
            pltpu.VMEM((2, 4 * rows, width), bf16),
            pltpu.VMEM((2, width, 4 * rows), bf16),
            pltpu.VMEM((2 * 32 * UNITS, 16, 128), bf16),
            pltpu.VMEM((2, width, hidden), bf16),
            pltpu.VMEM((4 * rows, max(hidden, width)), f32),
            pltpu.VMEM((4 * rows, hidden), bf16),
            pltpu.VMEM((4 * rows, hidden), bf16),
            pltpu.VMEM((2 * 32 * UNITS, 16, 128), f32),
            pltpu.VMEM((messages, 16, 128), bf16),
            pltpu.VMEM((messages, 16, 128), bf16),
            pltpu.VMEM((2, rows, width), f32),
            pltpu.VMEM((2, 16 + rows // 2, width), bf16),
            pltpu.VMEM((2, 16 + rows // 2, width), bf16),
            pltpu.VMEM((2, 2, UNITS, 16, 128), f32),
            pltpu.VMEM((STEPS + 1, BLOCKS, 128), f32),
            pltpu.VMEM((STEPS + 1, BLOCKS, 128), f32),
            pltpu.VMEM((shard, 128), f32),
            pltpu.VMEM((shard, 128), f32),
            dma((2, 2)),
            dma((2, 2)),
            dma((2, 2)),
            dma((2, 2)),
            dma((2,)),
            dma((2,)),
            dma((2, PARTS, STEPS)),
            dma((2, PARTS, STEPS)),
            dma((2, PARTS, STEPS)),
            dma((2, PARTS, STEPS)),
            dma((2, PARTS)),
            dma((2, PARTS)),
            dma((2,)),
            dma((2,)),
            dma((2,)),
            dma((2,)),
            dma((STEPS + 1,)),
            dma((STEPS + 1,)),
            dma,
            dma,
        ],
        compiler_params=pltpu.CompilerParams(
            collective_id=0, has_side_effects=True, vmem_limit_bytes=60 * 2**20
        ),
        name="step",
    )(inputs, out_cotangent, up_proj, down_proj.T)
    return gin, gup, gdn.T, eup[:, 0], edn.reshape((both,))


def solution(mesh):
    return jax.shard_map(
        body,
        mesh=mesh,
        in_specs=(
            P(("rep", "fs", "tp"), None),
            P("fs", "tp"),
            P("tp", "fs"),
            P(("rep", "fs", "tp"), None),
        ),
        out_specs=(P(("rep", "fs", "tp"), None), P("fs", "tp"), P("tp", "fs"), P("fs"), P("tp")),
        check_vma=False,
    )
```

```python
import functools

import jax
import jax.numpy as jnp
from jax import lax
from jax.experimental import pallas as pl
from jax.experimental.pallas import tpu as pltpu
from jax.sharding import PartitionSpec as P

MESH = pl.DeviceIdType.MESH
SIZES = ((3, 3, 3, 3, 4), (4, 3, 3, 3, 3))
STARTS = tuple(tuple(sum(size[:i]) for i in range(5)) for size in SIZES)
STEPS = 5
PARTS = 5
SPLIT = 2
ORDERS = tuple(tuple((i + 1 + k) % 5 for k in range(STEPS)) for i in range(PARTS))
UNITS = 16
BLOCKS = 8
HALF = (16, 8, 4, 2, 1)
SPAN = 240.0
SHIFT = 120.0


def encode(value, scale):
    code = jnp.exp2(jnp.abs(value) * (SPAN / scale) - SHIFT)
    return jnp.where(value < 0.0, -code, code).astype(jnp.bfloat16)


def decode(code, scale):
    code = code.astype(jnp.float32)
    size = (jnp.log2(jnp.abs(code)) + SHIFT) * (scale * (1.0 / SPAN))
    return jnp.where(code < 0.0, -size, size)


def scale_of(top):
    return (top * 1.01 + 1e-35).astype(jnp.bfloat16)


def bits_of(fs):
    z, y, x = fs // 16, (fs // 4) % 4, fs % 4
    return (z, (y % 2 + y // 2) % 2, y // 2, (x % 2 + x // 2) % 2, x // 2)


def partners_of(fs):
    z, y, x = fs // 16, (fs // 4) % 4, fs % 4
    return (
        fs + 16 - 32 * z,
        fs + 4 - 8 * (y % 2),
        fs + 12 - 8 * y,
        fs + 1 - 2 * (x % 2),
        fs + 3 - 2 * x,
    )


def remote(src, dst, send, recv, device):
    return pltpu.make_async_remote_copy(
        src_ref=src, dst_ref=dst, send_sem=send, recv_sem=recv, device_id=device, device_id_type=MESH
    )


def contract(left, right, left_dim, right_dim):
    return lax.dot_general(
        left, right, (((left_dim,), (right_dim,)), ((), ())), preferred_element_type=jnp.float32
    )


def kernel(
    factor,
    x_ref,
    c_ref,
    u_ref,
    d_ref,
    gin_ref,
    grad_ref,
    eup_ref,
    edn_ref,
    tok,
    tokt,
    wg,
    wn,
    pre,
    act,
    gpre,
    gbuf,
    sbuf,
    rbuf,
    part_in,
    pair_out,
    pair_in,
    outs,
    gin,
    ebuf,
    eup,
    tok_s,
    tok_r,
    fwd_s,
    fwd_r,
    sib_s,
    sib_r,
    g_s,
    g_r,
    r_s,
    r_r,
    rep_s,
    rep_r,
    pi_s,
    pi_r,
    li_s,
    li_r,
    e_s,
    e_r,
    eu_s,
    eu_r,
    out_s,
):
    rep, fs, tp = lax.axis_index("rep"), lax.axis_index("fs"), lax.axis_index("tp")
    mine = bits_of(fs)
    near = [{"fs": other} for other in partners_of(fs)]
    sibling = {"tp": 1 - tp}
    pair = {"rep": 1 - rep, "fs": partners_of(fs)[0]}
    twin = {"rep": 1 - rep}
    cross = {"rep": 1 - rep, "tp": 1 - tp}
    z, y, x = fs // 16, (fs // 4) % 4, fs % 4
    far_x = {"fs": fs + (x + 2) % 4 - x}
    far_y = {"fs": fs + 4 * ((y + 2) % 4 - y)}
    rows, width = x_ref.shape
    shard = u_ref.shape[0]
    hidden = u_ref.shape[1] // 2
    base = rep * hidden
    weights = (u_ref, d_ref)
    tokens = (x_ref, c_ref)
    pieces = 2
    chunk = rows // pieces
    half_rows = 2 * rows
    bw = 256
    blocks = hidden // bw
    all_parts = range(PARTS)
    f32, bf16 = jnp.float32, jnp.bfloat16

    flip = [(bit, 1 - bit) for bit in mine]
    tables = {}

    def unit(m, s, u):
        p = max(i for i in all_parts if STARTS[m][i] <= u)
        size = SIZES[m][p]
        if (p, size) not in tables:
            place = {d: size * 2**k for k, d in enumerate(ORDERS[p])}
            high, low = [], []
            for v in range(8):
                bits = bits_of(4 * v)
                high.append(sum(flip[d][bits[d]] * place[d] for d in (0, 1, 2)))
            for v in range(4):
                bits = bits_of(v)
                low.append(sum(flip[d][bits[d]] * place[d] for d in (3, 4)))
            tables[p, size] = high, low
        high, low = tables[p, size]
        return high[s // 4] + low[s % 4] + (m * UNITS * 32 + STARTS[m][p] * 32 + u - STARTS[m][p])

    def home(m, p):
        return m * UNITS * 32 + STARTS[m][p] * 32

    barrier = pltpu.get_barrier_semaphore()
    for device in near + [sibling, pair, twin, cross, far_x, far_y]:
        pl.semaphore_signal(barrier, inc=1, device_id=device, device_id_type=MESH)

    for m in range(2):
        tok[m, 0:rows] = tokens[m][...]
        for p in all_parts:
            for i in range(SIZES[m][p]):
                block, row = divmod(STARTS[m][p] + i, 2)
                wg[home(m, p) + i] = weights[m][
                    row * 16 : row * 16 + 16, pl.ds(pl.multiple_of(base + block * 128, 128), 128)
                ]

    pl.semaphore_wait(barrier, STEPS + 6)

    pending = []

    def start(copy):
        copy.start()
        pending.append(copy)
        return copy

    def token_copy(m, q):
        return remote(
            tokens[m].at[pl.ds(q * chunk, chunk)],
            tok.at[m, pl.ds(2 * rows + q * chunk, chunk)],
            tok_s.at[m, q],
            tok_r.at[m, q],
            pair,
        )

    def forward_copy(m, q):
        return remote(
            tok.at[m, pl.ds(2 * rows + q * chunk, chunk)],
            tok.at[m, pl.ds(3 * rows + q * chunk, chunk)],
            fwd_s.at[m, q],
            fwd_r.at[m, q],
            sibling,
        )

    def sibling_copy(m):
        return remote(tokens[m], tok.at[m, pl.ds(rows, rows)], sib_s.at[m], sib_r.at[m], sibling)

    def gather_copy(m, p, k):
        n = SIZES[m][p] * 2**k
        return remote(
            wg.at[pl.ds(home(m, p), n)],
            wg.at[pl.ds(home(m, p) + n, n)],
            g_s.at[m, p, k],
            g_r.at[m, p, k],
            near[ORDERS[p][k]],
        )

    def gather_step(m, k):
        for p in all_parts:
            if k > 0:
                gather_copy(m, p, k - 1).wait_recv()
            start(gather_copy(m, p, k))

    def forward(m, q):
        token_copy(m, q).wait_recv()
        start(forward_copy(m, q))

    def transpose(m, g):
        tokt[m, :, g * rows : (g + 1) * rows] = tok[m, g * rows : (g + 1) * rows].T

    def unpack(m):
        for p in all_parts:
            gather_copy(m, p, STEPS - 1).wait_recv()
            for u in range(STARTS[m][p], STARTS[m][p] + SIZES[m][p]):
                block, row = divmod(u, 2)
                for s in range(32):
                    top = s * shard + row * 16
                    wn[m, top : top + 16, block * 128 : block * 128 + 128] = wg[unit(m, s, u)]

    def part_cols(j):
        return slice(j * bw, (j + 1) * bw)

    def forward_half(h):
        part = slice(h * half_rows, (h + 1) * half_rows)
        for j in range(blocks):
            kept = jnp.maximum(
                jnp.dot(tok[0, part], wn[0, :, part_cols(j)], preferred_element_type=f32), 0.0
            )
            pre[part, part_cols(j)] = kept
            act[part, part_cols(j)] = (kept * kept).astype(bf16)

    def back_half(h):
        part = slice(h * half_rows, (h + 1) * half_rows)
        for j in range(blocks):
            value = jnp.dot(tok[1, part], wn[1, :, part_cols(j)], preferred_element_type=f32)
            gpre[part, part_cols(j)] = (2.0 * pre[part, part_cols(j)] * value).astype(bf16)

    def room(m, p, k):
        before = sum(1 + HALF[i] * SIZES[m][p] for i in range(k))
        return m * (31 * UNITS + 25) + 31 * STARTS[m][p] + 5 * p + before

    def reduce_copy(m, p, k):
        n = 1 + HALF[k] * SIZES[m][p]
        place = pl.ds(room(m, p, k), n)
        return remote(
            sbuf.at[place], rbuf.at[place], r_s.at[m, p, k], r_r.at[m, p, k], near[ORDERS[p][STEPS - 1 - k]]
        )

    def chunks(count, size):
        step = min(count, 2) * size
        return count * size // step, step

    def highest(m, p, k):
        n = SIZES[m][p]
        loops, step = chunks(HALF[k], n)
        at = home(m, p) + HALF[k] * n

        def some(i, top):
            return jnp.maximum(top, jnp.max(jnp.abs(gbuf[pl.ds(at + i * step, step)]), axis=0))

        return lax.fori_loop(0, loops, some, jnp.zeros((16, 128), f32))

    def send_sums(m, p, k, top):
        n = SIZES[m][p]
        loops, step = chunks(HALF[k], n)
        at, to = home(m, p) + HALF[k] * n, room(m, p, k)
        coded = scale_of(top)
        sbuf[to] = coded
        scale = coded.astype(f32)

        def some(i, carry):
            sbuf[pl.ds(to + 1 + i * step, step)] = encode(gbuf[pl.ds(at + i * step, step)], scale)
            return carry

        lax.fori_loop(0, loops, some, 0)
        start(reduce_copy(m, p, k))

    def begin(m, p):
        send_sums(m, p, 0, highest(m, p, 0))

    def add_sums(m, p, k, first, count):
        n = SIZES[m][p]
        loops, step = chunks(count, n)
        at, got = home(m, p) + first * n, room(m, p, k) + 1 + first * n
        scale = rbuf[room(m, p, k)].astype(f32)

        def some(i, top):
            place = pl.ds(at + i * step, step)
            value = gbuf[place] + decode(rbuf[pl.ds(got + i * step, step)], scale)
            gbuf[place] = value
            return jnp.maximum(top, jnp.max(jnp.abs(value), axis=0))

        return lax.fori_loop(0, loops, some, jnp.zeros((16, 128), f32))

    def reduce_step(m, k):
        for p in all_parts:
            reduce_copy(m, p, k).wait_recv()
            n = HALF[k + 1]
            top = add_sums(m, p, k, n, n)
            send_sums(m, p, k + 1, top)
            add_sums(m, p, k, 0, n)

    def weight_grad(m, right):
        tall = width // SPLIT
        done = 0
        for j in range(blocks):
            for i in range(SPLIT):
                out = jnp.dot(
                    tokt[m, i * tall : (i + 1) * tall, :], right[:, part_cols(j)], preferred_element_type=f32
                )
                for t in range(tall // shard):
                    for u in range(4):
                        block, row = divmod(u, 2)
                        gbuf[unit(m, i * (tall // shard) + t, 4 * j + u)] = out[
                            t * shard + row * 16 : t * shard + row * 16 + 16, block * 128 : block * 128 + 128
                        ]
            while done < PARTS and STARTS[m][done] + SIZES[m][done] <= 4 * (j + 1):
                begin(m, done)
                done += 1

    def share_copy(i):
        return remote(
            pre.at[pl.ds((1 + 2 * i) * rows, rows)], part_in.at[i], pi_s.at[i], pi_r.at[i], sibling
        )

    def pair_copy(q):
        return remote(pair_out.at[q], pair_in.at[q], li_s.at[q], li_r.at[q], pair)

    for m in range(2):
        gather_step(m, 0)
        for q in range(pieces):
            start(token_copy(m, q))
    for m in range(2):
        start(sibling_copy(m))
    for k in (1, 2):
        for m in range(2):
            gather_step(m, k)
    for m in range(2):
        transpose(m, 0)
        sibling_copy(m).wait_recv()
        transpose(m, 1)
    gather_step(0, 3)
    gather_step(1, 3)
    forward(0, 0)
    gather_step(0, 4)
    forward(0, 1)
    gather_step(1, 4)
    unpack(0)
    forward_half(0)
    for q in range(pieces):
        forward_copy(0, q).wait_recv()
    forward_half(1)
    transpose(0, 2)
    transpose(0, 3)
    unpack(1)
    forward(1, 0)
    back_half(0)
    forward(1, 1)
    transpose(1, 2)
    for q in range(pieces):
        forward_copy(1, q).wait_recv()
    transpose(1, 3)

    weight_grad(1, act)
    back_half(1)
    weight_grad(0, gpre)
    reduce_step(1, 0)

    for i in (1, 0):
        part = slice(i * half_rows, (i + 1) * half_rows)
        for n in range(width // bw):
            pre[part, n * bw : (n + 1) * bw] = contract(
                gpre[part, :], wn[0, n * bw : (n + 1) * bw, :], 1, 1
            )
        start(share_copy(i))

    reduce_step(0, 0)
    share_copy(1).wait_recv()
    for q in range(pieces):
        s = slice(q * chunk, (q + 1) * chunk)
        value = pre[2 * rows + q * chunk : 2 * rows + (q + 1) * chunk] + part_in[1, s]
        coded = scale_of(jnp.max(jnp.abs(value), axis=0, keepdims=True))
        pair_out[q, 0:16] = jnp.broadcast_to(coded, (16, width))
        pair_out[q, 16 : 16 + chunk] = encode(value, coded.astype(f32))
        start(pair_copy(q))
    share_copy(0).wait_recv()
    pre[0:rows] = pre[0:rows] + part_in[0]
    reduce_step(1, 1)
    reduce_step(0, 1)
    reduce_step(1, 2)
    reduce_step(0, 2)
    reduce_step(1, 3)

    def twin_copy(m, p):
        place = outs.at[m, rep, pl.ds(STARTS[m][p], SIZES[m][p])]
        return remote(place, place, rep_s.at[m, p], rep_r.at[m, p], twin)

    def finish(m, p):
        n = SIZES[m][p]
        reduce_copy(m, p, STEPS - 1).wait_recv()
        scale = rbuf[room(m, p, STEPS - 1)].astype(f32)
        got = decode(rbuf[pl.ds(room(m, p, STEPS - 1) + 1, n)], scale)
        value = (gbuf[pl.ds(home(m, p), n)] + got) * factor
        outs[m, rep, pl.ds(STARTS[m][p], n)] = value
        start(twin_copy(m, p))
        return value

    def output(i, src, dst):
        copy = pltpu.make_async_copy(src, dst, out_s.at[i])
        copy.start()
        return copy

    sums = []
    for p in all_parts:
        value = finish(1, p)
        for i in range(SIZES[1][p]):
            sums.append(jnp.sum(value[i] * value[i], axis=0, keepdims=True))
    for i in range(BLOCKS):
        ebuf[0, 0, i : i + 1, :] = sums[2 * i] + sums[2 * i + 1]

    rounds = ((near[3], near[4], far_x), (near[1], near[2], far_y), (near[0], twin, pair))

    def energy_copy(k, i):
        return remote(ebuf.at[k, 0], ebuf.at[k, 1 + i], e_s.at[k, i], e_r.at[k, i], rounds[k][i])

    def energy_begin(k):
        for i in range(3):
            start(energy_copy(k, i))

    def energy_step(k):
        for i in range(3):
            energy_copy(k, i).wait_recv()
        ebuf[k + 1, 0] = (ebuf[k, 0] + ebuf[k, 1]) + (ebuf[k, 2] + ebuf[k, 3])
        energy_begin(k + 1)

    energy_begin(0)
    reduce_step(0, 3)
    energy_step(0)
    squares = [jnp.zeros((16, 128), f32), jnp.zeros((16, 128), f32)]
    for p in all_parts:
        value = finish(0, p)
        for i in range(SIZES[0][p]):
            row = (STARTS[0][p] + i) % 2
            squares[row] = squares[row] + value[i] * value[i]
    for row in range(2):
        eup[0, row * 16 : row * 16 + 16] = squares[row]
    row_copies = [
        start(remote(eup.at[0], eup.at[1 + i], eu_s.at[i], eu_r.at[i], device))
        for i, device in enumerate((sibling, twin, cross))
    ]
    energy_step(1)
    for q in range(pieces):
        pair_copy(q).wait_recv()
        s = slice(q * chunk, (q + 1) * chunk)
        scale = pair_in[q, 0:16].astype(f32)[0:1]
        gin[s] = (pre[s] + decode(pair_in[q, 16 : 16 + chunk], scale)).astype(bf16)
    outputs = [output(0, gin, gin_ref)]
    for p in all_parts:
        twin_copy(1, p).wait_recv()
    outputs.append(output(1, outs.at[1], grad_ref.at[1]))
    for i in range(3):
        energy_copy(2, i).wait_recv()
    ebuf[3, 0] = (ebuf[2, 0] + ebuf[2, 1]) * (1.0 / width)
    ebuf[3, 1] = (ebuf[2, 2] + ebuf[2, 3]) * (1.0 / width)
    outputs.append(output(2, ebuf.at[3, 0], edn_ref.at[rep]))
    outputs.append(output(3, ebuf.at[3, 1], edn_ref.at[1 - rep]))
    for p in all_parts:
        twin_copy(0, p).wait_recv()
    outputs.append(output(4, outs.at[0], grad_ref.at[0]))
    for copy in row_copies:
        copy.wait_recv()
    outputs.append(output(5, eup, eup_ref))
    for copy in pending:
        copy.wait_send()
    for copy in outputs:
        copy.wait()


def layout(
    gin_ref, grad_ref, eup_ref, edn_ref, gin_out, gup_out, gdn_out, eup_out, edn_out,
    gin, grad, eup, edn, both, row, in_s, out_s,
):
    pairs = ((gin_ref, gin), (grad_ref.at[1], grad.at[1]), (grad_ref.at[0], grad.at[0]), (eup_ref, eup), (edn_ref, edn))
    loads = [pltpu.make_async_copy(a, b, in_s.at[i]) for i, (a, b) in enumerate(pairs)]
    for copy in loads:
        copy.start()
    stores = []

    def store(i, src, dst):
        copy = pltpu.make_async_copy(src, dst, out_s.at[i])
        copy.start()
        stores.append(copy)

    half = gup_out.shape[1] // 2
    loads[3].wait()
    total = (eup[0] + eup[1]) + (eup[2] + eup[3])
    row[...] = jnp.sum(total.T, axis=0) * (1.0 / (4 * half))
    loads[4].wait()
    store(3, row, eup_out)
    store(4, edn, edn_out)
    loads[0].wait()
    store(0, gin, gin_out)
    for m, load, out in ((1, 1, gdn_out), (0, 2, gup_out)):
        loads[load].wait()
        for r in range(2):
            for u in range(UNITS):
                block, top = divmod(u, 2)
                left = r * half + block * 128
                both[m, top * 16 : top * 16 + 16, left : left + 128] = grad[m, r, u]
        store(load, both.at[m], out)
    for copy in stores:
        copy.wait()


def body(inputs, up_proj, down_proj, out_cotangent):
    rows, width = inputs.shape
    shard, both = up_proj.shape
    hidden = both // 2
    factor = float(rows * lax.axis_size("rep") * lax.axis_size("fs") * lax.axis_size("tp")) ** (-0.5)
    f32, bf16 = jnp.float32, jnp.bfloat16
    shape = jax.ShapeDtypeStruct
    vmem = pl.BlockSpec(memory_space=pltpu.VMEM)
    dma = pltpu.SemaphoreType.DMA
    messages = 2 * (31 * UNITS + 25)
    anywhere = pl.BlockSpec(memory_space=pl.ANY)
    raw = pl.pallas_call(
        functools.partial(kernel, factor),
        out_shape=(
            shape((rows, width), bf16),
            shape((2, 2, UNITS, 16, 128), f32),
            shape((4, shard, 128), f32),
            shape((2, BLOCKS, 128), f32),
        ),
        in_specs=[vmem] * 4,
        out_specs=(anywhere,) * 4,
        scratch_shapes=[
            pltpu.VMEM((2, 4 * rows, width), bf16),
            pltpu.VMEM((2, width, 4 * rows), bf16),
            pltpu.VMEM((2 * 32 * UNITS, 16, 128), bf16),
            pltpu.VMEM((2, width, hidden), bf16),
            pltpu.VMEM((4 * rows, max(hidden, width)), f32),
            pltpu.VMEM((4 * rows, hidden), bf16),
            pltpu.VMEM((4 * rows, hidden), bf16),
            pltpu.VMEM((2 * 32 * UNITS, 16, 128), f32),
            pltpu.VMEM((messages, 16, 128), bf16),
            pltpu.VMEM((messages, 16, 128), bf16),
            pltpu.VMEM((2, rows, width), f32),
            pltpu.VMEM((2, 16 + rows // 2, width), bf16),
            pltpu.VMEM((2, 16 + rows // 2, width), bf16),
            pltpu.VMEM((2, 2, UNITS, 16, 128), f32),
            pltpu.VMEM((rows, width), bf16),
            pltpu.VMEM((4, 4, BLOCKS, 128), f32),
            pltpu.VMEM((4, shard, 128), f32),
            dma((2, 2)),
            dma((2, 2)),
            dma((2, 2)),
            dma((2, 2)),
            dma((2,)),
            dma((2,)),
            dma((2, PARTS, STEPS)),
            dma((2, PARTS, STEPS)),
            dma((2, PARTS, STEPS)),
            dma((2, PARTS, STEPS)),
            dma((2, PARTS)),
            dma((2, PARTS)),
            dma((2,)),
            dma((2,)),
            dma((2,)),
            dma((2,)),
            dma((3, 3)),
            dma((3, 3)),
            dma((3,)),
            dma((3,)),
            dma((6,)),
        ],
        compiler_params=pltpu.CompilerParams(
            collective_id=0, has_side_effects=True, vmem_limit_bytes=60 * 2**20
        ),
        name="step",
    )(inputs, out_cotangent, up_proj, down_proj.T)
    gin, gup, gdn, eup, edn = pl.pallas_call(
        layout,
        out_shape=(
            shape((rows, width), bf16),
            shape((shard, both), f32),
            shape((shard, both), f32),
            shape((shard,), f32),
            shape((2, BLOCKS, 128), f32),
        ),
        in_specs=[anywhere] * 4,
        out_specs=(anywhere,) * 5,
        scratch_shapes=[
            pltpu.VMEM((rows, width), bf16),
            pltpu.VMEM((2, 2, UNITS, 16, 128), f32),
            pltpu.VMEM((4, shard, 128), f32),
            pltpu.VMEM((2, BLOCKS, 128), f32),
            pltpu.VMEM((2, shard, both), f32),
            pltpu.VMEM((shard,), f32),
            dma((5,)),
            dma((5,)),
        ],
        name="layout",
    )(*raw)
    return gin, gup, gdn.T, eup, edn.reshape((both,))


def solution(mesh):
    return jax.shard_map(
        body,
        mesh=mesh,
        in_specs=(
            P(("rep", "fs", "tp"), None),
            P("fs", "tp"),
            P("tp", "fs"),
            P(("rep", "fs", "tp"), None),
        ),
        out_specs=(P(("rep", "fs", "tp"), None), P("fs", "tp"), P("tp", "fs"), P("fs"), P("tp")),
        check_vma=False,
    )
```

```python
import functools

import jax
import jax.numpy as jnp
from jax import lax
from jax.experimental import pallas as pl
from jax.experimental.pallas import tpu as pltpu
from jax.sharding import PartitionSpec as P

MESH = pl.DeviceIdType.MESH
GATHER = (
    (
        (2, 4, 0, 1, 3),
        (0, 3, 1, 2, 4),
        (1, 4, 0, 2, 3),
        (2, 3, 1, 0, 4),
        (4, 0, 2, 3, 1),
        (4, 3, 0, 1, 2),
        (1, 2, 3, 4, 0),
        (3, 1, 4, 0, 2),
    ),
    (
        (0, 4, 1, 3, 2),
        (3, 2, 0, 1, 4),
        (2, 4, 3, 1, 0),
        (1, 3, 2, 0, 4),
        (0, 1, 2, 4, 3),
        (2, 4, 3, 1, 0),
        (2, 1, 4, 0, 3),
        (3, 0, 4, 2, 1),
    ),
)
REDUCE = (
    (
        (4, 3, 0, 1, 2),
        (0, 1, 2, 4, 3),
        (2, 4, 3, 0, 1),
        (3, 1, 2, 0, 4),
        (4, 0, 1, 3, 2),
        (1, 2, 0, 4, 3),
        (3, 4, 2, 1, 0),
        (0, 3, 1, 2, 4),
    ),
    (
        (2, 1, 3, 4, 0),
        (4, 0, 2, 1, 3),
        (0, 4, 2, 1, 3),
        (4, 3, 1, 0, 2),
        (1, 4, 2, 3, 0),
        (4, 2, 3, 0, 1),
        (0, 3, 1, 4, 2),
        (2, 3, 1, 0, 4),
    ),
)
FIRST = (
    0, 10, 20, 40, 70, 30, 50, 60, 100, 110, 120, 130, 140, 170, 150, 160,
    1, 11, 41, 71, 61, 21, 31, 51, 101, 111, 141, 161, 171, 121, 131,
    151, 2, 12, 42, 72, 62, 22, 32, 52, 102, 122, 142, 132, -2, 162, 172,
    152, 112, 3, 13, 43, 63, 73, 53, 23, 33, 103, 143, 123, 173, 133, -3, -1,
    153, 163, 4, 14, 113, 74, 64, 24, 34, 44, 54,
)
THEN = (
    1010, 1011, 1012, 1013, 1100, 1000, 1101, 100, 110, 1001, 130, 150, 1102, 140, 120, 170,
    1002, 160, 101, 111, 1103, 10, 131, 1003, 0, 141, 151, 30, 20, 1201, 171, 161,
    121, 132, 40, 50, 11, 112, 1200, 102, 142, 1, 152, 60, 1301, 133, 172, 122,
    70, 162, 12, 31, 41, 51, 103, 1300, 153, 143, 21, 113, 134, 173, 123, 61,
    163, 2, 13, 71, 42, 154, 144, 52, 32, 114, 104, 22, 174, 124, 164, 3,
    14, 62, 43, 72, 53, 33, 23, 4, 1400, 63, 44, 1500, 54, 73, 34, 24,
    64, 1401, 74, 1402, 1310, 1311,
)
STEPS = 5
PARTS = 8
SPLIT = 2
SIZE = 2
UNITS = 16
BLOCKS = 8
HALF = (16, 8, 4, 2, 1)
SPAN = 240.0
SHIFT = 120.0


def encode(value, scale):
    code = jnp.exp2(jnp.abs(value) * (SPAN / scale) - SHIFT)
    return jnp.where(value < 0.0, -code, code).astype(jnp.bfloat16)


def decode(code, scale):
    code = code.astype(jnp.float32)
    size = (jnp.log2(jnp.abs(code)) + SHIFT) * (scale * (1.0 / SPAN))
    return jnp.where(code < 0.0, -size, size)


def scale_of(top):
    return (top * 1.01 + 1e-35).astype(jnp.bfloat16)


def bits_of(fs):
    z, y, x = fs // 16, (fs // 4) % 4, fs % 4
    return (z, (y % 2 + y // 2) % 2, y // 2, (x % 2 + x // 2) % 2, x // 2)


def partners_of(fs):
    z, y, x = fs // 16, (fs // 4) % 4, fs % 4
    return (
        fs + 16 - 32 * z,
        fs + 4 - 8 * (y % 2),
        fs + 12 - 8 * y,
        fs + 1 - 2 * (x % 2),
        fs + 3 - 2 * x,
    )


def remote(src, dst, send, recv, device):
    return pltpu.make_async_remote_copy(
        src_ref=src, dst_ref=dst, send_sem=send, recv_sem=recv, device_id=device, device_id_type=MESH
    )


def contract(left, right, left_dim, right_dim):
    return lax.dot_general(
        left, right, (((left_dim,), (right_dim,)), ((), ())), preferred_element_type=jnp.float32
    )


def kernel(
    factor,
    x_ref,
    c_ref,
    u_ref,
    d_ref,
    gin_ref,
    grad_ref,
    eup_ref,
    edn_ref,
    tok,
    tokt,
    wg,
    wn,
    pre,
    act,
    gpre,
    gbuf,
    sbuf,
    rbuf,
    part_in,
    pair_out,
    pair_in,
    outs,
    gin,
    ebuf,
    eup,
    load_s,
    tok_s,
    tok_r,
    fwd_s,
    fwd_r,
    sib_s,
    sib_r,
    g_s,
    g_r,
    r_s,
    r_r,
    rep_s,
    rep_r,
    pi_s,
    pi_r,
    li_s,
    li_r,
    e_s,
    e_r,
    eu_s,
    eu_r,
    out_s,
):
    rep, fs, tp = lax.axis_index("rep"), lax.axis_index("fs"), lax.axis_index("tp")
    mine = bits_of(fs)
    near = [{"fs": other} for other in partners_of(fs)]
    sibling = {"tp": 1 - tp}
    pair = {"rep": 1 - rep, "fs": partners_of(fs)[0]}
    twin = {"rep": 1 - rep}
    cross = {"rep": 1 - rep, "tp": 1 - tp}
    z, y, x = fs // 16, (fs // 4) % 4, fs % 4
    far_x = {"fs": fs + (x + 2) % 4 - x}
    far_y = {"fs": fs + 4 * ((y + 2) % 4 - y)}
    rows, width = x_ref.shape
    shard = u_ref.shape[0]
    hidden = u_ref.shape[1] // 2
    base = rep * hidden
    weights = (u_ref, d_ref)
    tokens = (x_ref, c_ref)
    pieces = 2
    chunk = rows // pieces
    half_rows = 2 * rows
    bw = 256
    blocks = hidden // bw
    all_parts = range(PARTS)
    f32, bf16 = jnp.float32, jnp.bfloat16

    flip = [(bit, 1 - bit) for bit in mine]
    tables = {}

    def slot(order, s):
        if order not in tables:
            place = {d: 2**k for k, d in enumerate(order)}
            high, low = [], []
            for v in range(8):
                bits = bits_of(4 * v)
                high.append(sum(flip[d][bits[d]] * place[d] for d in (0, 1, 2)))
            for v in range(4):
                bits = bits_of(v)
                low.append(sum(flip[d][bits[d]] * place[d] for d in (3, 4)))
            tables[order] = high, low
        high, low = tables[order]
        return high[s // 4] + low[s % 4]

    def home(m, p):
        return (m * PARTS + p) * 32 * SIZE

    def place_of(m, p):
        return (m * PARTS + p) * 32

    barrier = pltpu.get_barrier_semaphore()
    for device in near + [sibling, pair, twin, cross, far_x, far_y]:
        pl.semaphore_signal(barrier, inc=1, device_id=device, device_id_type=MESH)

    loads = []
    for m in range(2):
        loads.append(pltpu.make_async_copy(tokens[m], tok.at[m, pl.ds(0, rows)], load_s.at[16 + m]))
        for p in all_parts:
            columns = pl.ds(pl.multiple_of(base + p * 128, 128), 128)
            loads.append(
                pltpu.make_async_copy(
                    weights[m].at[:, columns], wg.at[place_of(m, p)], load_s.at[m * PARTS + p]
                )
            )
    for copy in loads:
        copy.start()
    for copy in loads:
        copy.wait()

    pl.semaphore_wait(barrier, STEPS + 6)

    pending = []

    def start(copy):
        copy.start()
        pending.append(copy)
        return copy

    def token_copy(m, q):
        return remote(
            tok.at[m, pl.ds(q * chunk, chunk)],
            tok.at[m, pl.ds(2 * rows + q * chunk, chunk)],
            tok_s.at[m, q],
            tok_r.at[m, q],
            pair,
        )

    def forward_copy(m, q):
        return remote(
            tok.at[m, pl.ds(2 * rows + q * chunk, chunk)],
            tok.at[m, pl.ds(3 * rows + q * chunk, chunk)],
            fwd_s.at[m, q],
            fwd_r.at[m, q],
            sibling,
        )

    def sibling_copy(m):
        return remote(tok.at[m, pl.ds(0, rows)], tok.at[m, pl.ds(rows, rows)], sib_s.at[m], sib_r.at[m], sibling)

    def gather_copy(m, p, k):
        n = 2**k
        return remote(
            wg.at[pl.ds(place_of(m, p), n)],
            wg.at[pl.ds(place_of(m, p) + n, n)],
            g_s.at[m * PARTS + p, k],
            g_r.at[m * PARTS + p, k],
            near[GATHER[m][p][k]],
        )

    def forward(m, q):
        token_copy(m, q).wait_recv()
        start(forward_copy(m, q))

    def transpose(m, g):
        tokt[m, :, g * rows : (g + 1) * rows] = tok[m, g * rows : (g + 1) * rows].T

    def unpack(m, p):
        for s in range(32):
            wn[m, s * shard : (s + 1) * shard, p * 128 : (p + 1) * 128] = wg[
                place_of(m, p) + slot(GATHER[m][p], s)
            ]

    def part_cols(j):
        return slice(j * bw, (j + 1) * bw)

    def forward_block(j):
        for h in range(2):
            part = slice(h * half_rows, (h + 1) * half_rows)
            kept = jnp.maximum(
                jnp.dot(tok[0, part], wn[0, :, part_cols(j)], preferred_element_type=f32), 0.0
            )
            pre[part, part_cols(j)] = kept
            act[part, part_cols(j)] = (kept * kept).astype(bf16)

    def back_block(j):
        for p in (2 * j, 2 * j + 1):
            gather_copy(1, p, STEPS - 1).wait_recv()
            unpack(1, p)
        for h in range(2):
            part = slice(h * half_rows, (h + 1) * half_rows)
            value = jnp.dot(tok[1, part], wn[1, :, part_cols(j)], preferred_element_type=f32)
            gpre[part, part_cols(j)] = (2.0 * pre[part, part_cols(j)] * value).astype(bf16)

    def room(m, p, k):
        before = sum(1 + HALF[i] * SIZE for i in range(k))
        return (m * PARTS + p) * (31 * SIZE + 5) + before

    def reduce_copy(m, p, k):
        place = pl.ds(room(m, p, k), 1 + HALF[k] * SIZE)
        return remote(
            sbuf.at[place],
            rbuf.at[place],
            r_s.at[m * PARTS + p, k],
            r_r.at[m * PARTS + p, k],
            near[REDUCE[m][p][STEPS - 1 - k]],
        )

    def chunks(count, size):
        step = min(count, 4) * size
        return count * size // step, step

    def highest(m, p, k):
        n = SIZE
        loops, step = chunks(HALF[k], n)
        at = home(m, p) + HALF[k] * n

        def some(i, top):
            return jnp.maximum(top, jnp.max(jnp.abs(gbuf[pl.ds(at + i * step, step)]), axis=0))

        return lax.fori_loop(0, loops, some, jnp.zeros((16, 128), f32))

    def send_sums(m, p, k, top):
        n = SIZE
        loops, step = chunks(HALF[k], n)
        at, to = home(m, p) + HALF[k] * n, room(m, p, k)
        coded = scale_of(top)
        sbuf[to] = coded
        scale = coded.astype(f32)

        def some(i, carry):
            sbuf[pl.ds(to + 1 + i * step, step)] = encode(gbuf[pl.ds(at + i * step, step)], scale)
            return carry

        lax.fori_loop(0, loops, some, 0)
        start(reduce_copy(m, p, k))

    def begin(m, p):
        send_sums(m, p, 0, highest(m, p, 0))

    def add_sums(m, p, k, first, count):
        n = SIZE
        loops, step = chunks(count, n)
        at, got = home(m, p) + first * n, room(m, p, k) + 1 + first * n
        scale = rbuf[room(m, p, k)].astype(f32)

        def some(i, top):
            place = pl.ds(at + i * step, step)
            value = gbuf[place] + decode(rbuf[pl.ds(got + i * step, step)], scale)
            gbuf[place] = value
            return jnp.maximum(top, jnp.max(jnp.abs(value), axis=0))

        return lax.fori_loop(0, loops, some, jnp.zeros((16, 128), f32))

    def reduce_step(m, p, k):
        reduce_copy(m, p, k).wait_recv()
        n = HALF[k + 1]
        top = add_sums(m, p, k, n, n)
        send_sums(m, p, k + 1, top)
        add_sums(m, p, k, 0, n)

    def weight_grad(m, right, j):
        tall = width // SPLIT
        for i in range(SPLIT):
            out = jnp.dot(
                tokt[m, i * tall : (i + 1) * tall, :], right[:, part_cols(j)], preferred_element_type=f32
            )
            for t in range(tall // shard):
                for e in range(2):
                    p = 2 * j + e
                    at = home(m, p) + slot(REDUCE[m][p], i * (tall // shard) + t) * SIZE
                    value = out[t * shard : (t + 1) * shard, e * 128 : (e + 1) * 128]
                    gbuf[pl.ds(at, SIZE)] = value.reshape(SIZE, 16, 128)
        begin(m, 2 * j)
        begin(m, 2 * j + 1)

    def share_copy(i):
        return remote(
            pre.at[pl.ds((1 + 2 * i) * rows, rows)], part_in.at[i], pi_s.at[i], pi_r.at[i], sibling
        )

    def pair_copy(q):
        return remote(pair_out.at[q], pair_in.at[q], li_s.at[q], li_r.at[q], pair)

    for m in range(2):
        for p in all_parts:
            start(gather_copy(m, p, 0))
        for q in range(pieces):
            start(token_copy(m, q))
    for m in range(2):
        start(sibling_copy(m))

    unpacked = []
    for a in FIRST:
        if a == -1:
            for m in range(2):
                transpose(m, 0)
                sibling_copy(m).wait_recv()
                transpose(m, 1)
        elif a < 0:
            forward((-2 - a) // 2, (-2 - a) % 2)
        else:
            m, p, k = a // 100, a // 10 % 10, a % 10
            gather_copy(m, p, k).wait_recv()
            if k < STEPS - 1:
                start(gather_copy(m, p, k + 1))
                continue
            unpack(m, p)
            if not unpacked:
                for q in range(pieces):
                    forward_copy(0, q).wait_recv()
                transpose(0, 2)
                transpose(0, 3)
            unpacked.append(p)
            if p ^ 1 in unpacked:
                forward_block(p // 2)

    if -4 not in FIRST:
        forward(1, 0)
    forward(1, 1)
    transpose(1, 2)
    for q in range(pieces):
        forward_copy(1, q).wait_recv()
    transpose(1, 3)

    def twin_copy(m, p):
        place = outs.at[m, rep, pl.ds(p * SIZE, SIZE)]
        return remote(place, place, rep_s.at[m * PARTS + p], rep_r.at[m * PARTS + p], twin)

    def finish(m, p):
        n = SIZE
        reduce_copy(m, p, STEPS - 1).wait_recv()
        scale = rbuf[room(m, p, STEPS - 1)].astype(f32)
        got = decode(rbuf[pl.ds(room(m, p, STEPS - 1) + 1, n)], scale)
        value = (gbuf[pl.ds(home(m, p), n)] + got) * factor
        outs[m, rep, pl.ds(p * SIZE, n)] = value
        start(twin_copy(m, p))
        return value

    def output(i, src, dst):
        copy = pltpu.make_async_copy(src, dst, out_s.at[i])
        copy.start()
        return copy

    rounds = ((near[3], near[4], far_x), (near[1], near[2], far_y), (near[0], twin, pair))

    def energy_copy(k, i):
        return remote(ebuf.at[k, 0], ebuf.at[k, 1 + i], e_s.at[k, i], e_r.at[k, i], rounds[k][i])

    def energy_begin(k):
        for i in range(3):
            start(energy_copy(k, i))

    def energy_step(k):
        for i in range(3):
            energy_copy(k, i).wait_recv()
        ebuf[k + 1, 0] = (ebuf[k, 0] + ebuf[k, 1]) + (ebuf[k, 2] + ebuf[k, 3])
        energy_begin(k + 1)

    squares = [jnp.zeros((16, 128), f32), jnp.zeros((16, 128), f32)]
    left = [PARTS, PARTS]
    outputs = []
    row_copies = []

    def arrived(m, p, k):
        if k < STEPS - 1:
            reduce_step(m, p, k)
            return
        value = finish(m, p)
        left[m] -= 1
        if m == 1:
            total = value[0] * value[0] + value[1] * value[1]
            ebuf[0, 0, p : p + 1, :] = jnp.sum(total, axis=0, keepdims=True)
            if left[m] == 0:
                energy_begin(0)
            return
        for row in range(2):
            squares[row] = squares[row] + value[row] * value[row]
        if left[m] == 0:
            for row in range(2):
                eup[0, row * 16 : row * 16 + 16] = squares[row]
            for i, device in enumerate((sibling, twin, cross)):
                row_copies.append(start(remote(eup.at[0], eup.at[1 + i], eu_s.at[i], eu_r.at[i], device)))

    def inputs_grad(i):
        part = slice(i * half_rows, (i + 1) * half_rows)
        for n in range(width // bw):
            pre[part, n * bw : (n + 1) * bw] = contract(
                gpre[part, :], wn[0, n * bw : (n + 1) * bw, :], 1, 1
            )
        start(share_copy(i))

    def share_arrived(i):
        share_copy(i).wait_recv()
        if i == 0:
            pre[0:rows] = pre[0:rows] + part_in[0]
            return
        for q in range(pieces):
            s = slice(q * chunk, (q + 1) * chunk)
            value = pre[2 * rows + q * chunk : 2 * rows + (q + 1) * chunk] + part_in[1, s]
            coded = scale_of(jnp.max(jnp.abs(value), axis=0, keepdims=True))
            pair_out[q, 0:16] = jnp.broadcast_to(coded, (16, width))
            pair_out[q, 16 : 16 + chunk] = encode(value, coded.astype(f32))
            start(pair_copy(q))

    def pair_arrived(q):
        pair_copy(q).wait_recv()
        s = slice(q * chunk, (q + 1) * chunk)
        scale = pair_in[q, 0:16].astype(f32)[0:1]
        gin[s] = (pre[s] + decode(pair_in[q, 16 : 16 + chunk], scale)).astype(bf16)
        if q == pieces - 1:
            outputs.append(output(0, gin, gin_ref))

    def energy_end():
        for i in range(3):
            energy_copy(2, i).wait_recv()
        ebuf[3, 0] = (ebuf[2, 0] + ebuf[2, 1]) * (1.0 / width)
        ebuf[3, 1] = (ebuf[2, 2] + ebuf[2, 3]) * (1.0 / width)
        outputs.append(output(2, ebuf.at[3, 0], edn_ref.at[rep]))
        outputs.append(output(3, ebuf.at[3, 1], edn_ref.at[1 - rep]))

    def twins_arrived(m):
        for p in all_parts:
            twin_copy(m, p).wait_recv()
        outputs.append(output(4 if m == 0 else 1, outs.at[m], grad_ref.at[m]))

    def run(a):
        if a < 200:
            arrived(a // 100, a // 10 % 10, a % 10)
        elif a < 1100:
            m, j = (a - 1000) // 10, a % 10
            weight_grad(m, (gpre, act)[m], j)
        elif a < 1200:
            back_block(a - 1100)
        elif a < 1300:
            inputs_grad(a - 1200)
        elif a < 1310:
            share_arrived(a - 1300)
        elif a < 1400:
            pair_arrived(a - 1310)
        elif a < 1402:
            energy_step(a - 1400)
        elif a == 1402:
            energy_end()
        else:
            twins_arrived(1)

    for a in THEN[:-3]:
        run(a)
    twins_arrived(0)
    for a in THEN[-3:]:
        run(a)
    for copy in row_copies:
        copy.wait_recv()
    outputs.append(output(5, eup, eup_ref))
    for copy in pending:
        copy.wait_send()
    for copy in outputs:
        copy.wait()


def layout(
    gin_ref, grad_ref, eup_ref, edn_ref, gin_out, gup_out, gdn_out, eup_out, edn_out,
    gin, grad, eup, edn, both, row, in_s, out_s,
):
    pairs = ((gin_ref, gin), (grad_ref.at[1], grad.at[1]), (grad_ref.at[0], grad.at[0]), (eup_ref, eup), (edn_ref, edn))
    loads = [pltpu.make_async_copy(a, b, in_s.at[i]) for i, (a, b) in enumerate(pairs)]
    for copy in loads:
        copy.start()
    stores = []

    def store(i, src, dst):
        copy = pltpu.make_async_copy(src, dst, out_s.at[i])
        copy.start()
        stores.append(copy)

    half = gup_out.shape[1] // 2
    loads[3].wait()
    total = (eup[0] + eup[1]) + (eup[2] + eup[3])
    row[...] = jnp.sum(total.T, axis=0) * (1.0 / (4 * half))
    loads[4].wait()
    store(3, row, eup_out)
    store(4, edn, edn_out)
    loads[0].wait()
    store(0, gin, gin_out)
    for m, load, out in ((1, 1, gdn_out), (0, 2, gup_out)):
        loads[load].wait()
        for r in range(2):
            for u in range(UNITS):
                block, top = divmod(u, 2)
                left = r * half + block * 128
                both[m, top * 16 : top * 16 + 16, left : left + 128] = grad[m, r, u]
        store(load, both.at[m], out)
    for copy in stores:
        copy.wait()


def body(inputs, up_proj, down_proj, out_cotangent):
    rows, width = inputs.shape
    shard, both = up_proj.shape
    hidden = both // 2
    factor = float(rows * lax.axis_size("rep") * lax.axis_size("fs") * lax.axis_size("tp")) ** (-0.5)
    f32, bf16 = jnp.float32, jnp.bfloat16
    shape = jax.ShapeDtypeStruct
    dma = pltpu.SemaphoreType.DMA
    messages = 2 * PARTS * (31 * SIZE + 5)
    anywhere = pl.BlockSpec(memory_space=pl.ANY)
    raw = pl.pallas_call(
        functools.partial(kernel, factor),
        out_shape=(
            shape((rows, width), bf16),
            shape((2, 2, UNITS, 16, 128), f32),
            shape((4, shard, 128), f32),
            shape((2, BLOCKS, 128), f32),
        ),
        in_specs=[anywhere] * 4,
        out_specs=(anywhere,) * 4,
        scratch_shapes=[
            pltpu.VMEM((2, 4 * rows, width), bf16),
            pltpu.VMEM((2, width, 4 * rows), bf16),
            pltpu.VMEM((2 * PARTS * 32, shard, 128), bf16),
            pltpu.VMEM((2, width, hidden), bf16),
            pltpu.VMEM((4 * rows, max(hidden, width)), f32),
            pltpu.VMEM((4 * rows, hidden), bf16),
            pltpu.VMEM((4 * rows, hidden), bf16),
            pltpu.VMEM((2 * 32 * UNITS, 16, 128), f32),
            pltpu.VMEM((messages, 16, 128), bf16),
            pltpu.VMEM((messages, 16, 128), bf16),
            pltpu.VMEM((2, rows, width), f32),
            pltpu.VMEM((2, 16 + rows // 2, width), bf16),
            pltpu.VMEM((2, 16 + rows // 2, width), bf16),
            pltpu.VMEM((2, 2, UNITS, 16, 128), f32),
            pltpu.VMEM((rows, width), bf16),
            pltpu.VMEM((4, 4, BLOCKS, 128), f32),
            pltpu.VMEM((4, shard, 128), f32),
            dma((2 * PARTS + 2,)),
            dma((2, 2)),
            dma((2, 2)),
            dma((2, 2)),
            dma((2, 2)),
            dma((2,)),
            dma((2,)),
            dma((2 * PARTS, STEPS)),
            dma((2 * PARTS, STEPS)),
            dma((2 * PARTS, STEPS)),
            dma((2 * PARTS, STEPS)),
            dma((2 * PARTS,)),
            dma((2 * PARTS,)),
            dma((2,)),
            dma((2,)),
            dma((2,)),
            dma((2,)),
            dma((3, 3)),
            dma((3, 3)),
            dma((3,)),
            dma((3,)),
            dma((6,)),
        ],
        compiler_params=pltpu.CompilerParams(
            collective_id=0, has_side_effects=True, vmem_limit_bytes=60 * 2**20
        ),
        name="step",
    )(inputs, out_cotangent, up_proj, down_proj.T)
    gin, gup, gdn, eup, edn = pl.pallas_call(
        layout,
        out_shape=(
            shape((rows, width), bf16),
            shape((shard, both), f32),
            shape((shard, both), f32),
            shape((shard,), f32),
            shape((2, BLOCKS, 128), f32),
        ),
        in_specs=[anywhere] * 4,
        out_specs=(anywhere,) * 5,
        scratch_shapes=[
            pltpu.VMEM((rows, width), bf16),
            pltpu.VMEM((2, 2, UNITS, 16, 128), f32),
            pltpu.VMEM((4, shard, 128), f32),
            pltpu.VMEM((2, BLOCKS, 128), f32),
            pltpu.VMEM((2, shard, both), f32),
            pltpu.VMEM((shard,), f32),
            dma((5,)),
            dma((5,)),
        ],
        name="layout",
    )(*raw)
    return gin, gup, gdn.T, eup, edn.reshape((both,))


def solution(mesh):
    return jax.shard_map(
        body,
        mesh=mesh,
        in_specs=(
            P(("rep", "fs", "tp"), None),
            P("fs", "tp"),
            P("tp", "fs"),
            P(("rep", "fs", "tp"), None),
        ),
        out_specs=(P(("rep", "fs", "tp"), None), P("fs", "tp"), P("tp", "fs"), P("fs"), P("tp")),
        check_vma=False,
    )
```

```python
import functools

import jax
import jax.numpy as jnp
from jax import lax
from jax.experimental import pallas as pl
from jax.experimental.pallas import tpu as pltpu
from jax.sharding import PartitionSpec as P

MESH = pl.DeviceIdType.MESH
GATHER = (
    (
        (2, 4, 0, 1, 3),
        (0, 3, 1, 2, 4),
        (1, 4, 0, 2, 3),
        (2, 3, 1, 0, 4),
        (4, 0, 2, 3, 1),
        (4, 3, 0, 1, 2),
        (1, 2, 3, 4, 0),
        (3, 1, 4, 0, 2),
    ),
    (
        (0, 4, 1, 3, 2),
        (3, 2, 0, 1, 4),
        (2, 4, 3, 1, 0),
        (1, 3, 2, 0, 4),
        (0, 1, 2, 4, 3),
        (2, 4, 3, 1, 0),
        (2, 1, 4, 0, 3),
        (3, 0, 4, 2, 1),
    ),
)
REDUCE = (
    (
        (4, 3, 0, 1, 2),
        (0, 2, 1, 4, 3),
        (0, 1, 4, 3, 2),
        (2, 4, 3, 1, 0),
        (2, 3, 0, 4, 1),
        (1, 0, 3, 2, 4),
        (2, 4, 1, 0, 3),
        (4, 0, 3, 1, 2),
    ),
    (
        (3, 4, 0, 1, 2),
        (2, 0, 4, 1, 3),
        (0, 2, 3, 4, 1),
        (4, 2, 3, 1, 0),
        (2, 3, 0, 1, 4),
        (3, 1, 0, 4, 2),
        (2, 4, 0, 3, 1),
        (1, 3, 2, 4, 0),
    ),
)
FIRST = (
    0, 10, 20, 40, 70, 30, 50, 60, 100, 110, 120, 130, 140, 170, 150, 160,
    1, 11, 41, 71, 61, 21, 31, 51, 101, 111, 141, 161, 171, 121, 131,
    151, 2, 12, 42, 72, 62, 22, 32, 52, 102, 122, 142, 132, -2, 162, 172,
    152, 112, 3, 13, 43, 63, 73, 53, 23, 33, 103, 143, 123, 173, 133, -3, -1,
    153, 163, 4, 14, 113, 74, 64, 24, 34, 44, 54,
)
THEN = (
    1010, 1011, 1012, 1013, 1100, 1101, 1102, 100, 110, 1103, 120, 130, 1000, 140, 150, 1001,
    160, 170, 1201, 101, 121, 1002, 111, 151, 1003, 0, 10, 131, 171, 1301, 30, 161,
    141, 102, 122, 1200, 20, 152, 50, 40, 112, 162, 60, 70, 1, 142, 132, 172,
    11, 1300, 123, 103, 31, 21, 153, 113, 51, 41, 143, 163, 133, 173, 61, 104,
    71, 2, 12, 124, 114, 32, 154, 22, 144, 134, 52, 164, 42, 174, 62, 72,
    13, 3, 33, 23, 53, 43, 1400, 63, 73, 4, 1500, 14, 34, 24, 54, 44,
    64, 74, 1401, 1402, 1310, 1311,
)
STEPS = 5
PARTS = 8
SPLIT = 2
SIZE = 2
UNITS = 16
BLOCKS = 8
HALF = (16, 8, 4, 2, 1)
SPAN = 240.0
SHIFT = 120.0


def encode(value, scale):
    code = jnp.exp2(jnp.abs(value) * (SPAN / scale) - SHIFT)
    return jnp.where(value < 0.0, -code, code).astype(jnp.bfloat16)


def decode(code, scale):
    code = code.astype(jnp.float32)
    size = (jnp.log2(jnp.abs(code)) + SHIFT) * (scale * (1.0 / SPAN))
    return jnp.where(code < 0.0, -size, size)


def scale_of(top):
    return (top * 1.01 + 1e-35).astype(jnp.bfloat16)


def bits_of(fs):
    z, y, x = fs // 16, (fs // 4) % 4, fs % 4
    return (z, (y % 2 + y // 2) % 2, y // 2, (x % 2 + x // 2) % 2, x // 2)


def partners_of(fs):
    z, y, x = fs // 16, (fs // 4) % 4, fs % 4
    return (
        fs + 16 - 32 * z,
        fs + 4 - 8 * (y % 2),
        fs + 12 - 8 * y,
        fs + 1 - 2 * (x % 2),
        fs + 3 - 2 * x,
    )


def remote(src, dst, send, recv, device):
    return pltpu.make_async_remote_copy(
        src_ref=src, dst_ref=dst, send_sem=send, recv_sem=recv, device_id=device, device_id_type=MESH
    )


def contract(left, right, left_dim, right_dim):
    return lax.dot_general(
        left, right, (((left_dim,), (right_dim,)), ((), ())), preferred_element_type=jnp.float32
    )


def kernel(
    factor,
    x_ref,
    c_ref,
    u_ref,
    d_ref,
    gin_ref,
    grad_ref,
    eup_ref,
    edn_ref,
    tok,
    tokt,
    wg,
    wn,
    pre,
    act,
    gpre,
    gbuf,
    sbuf,
    rbuf,
    part_in,
    pair_out,
    pair_in,
    twin_out,
    twin_in,
    outs,
    gin,
    ebuf,
    eup,
    load_s,
    tok_r,
    fwd_r,
    sib_r,
    g_r,
    r_r,
    rep_r,
    pi_r,
    li_r,
    e_r,
    eu_r,
    sent,
    out_s,
):
    rep, fs, tp = lax.axis_index("rep"), lax.axis_index("fs"), lax.axis_index("tp")
    mine = bits_of(fs)
    near = [{"fs": other} for other in partners_of(fs)]
    sibling = {"tp": 1 - tp}
    pair = {"rep": 1 - rep, "fs": partners_of(fs)[0]}
    twin = {"rep": 1 - rep}
    cross = {"rep": 1 - rep, "tp": 1 - tp}
    z, y, x = fs // 16, (fs // 4) % 4, fs % 4
    far_x = {"fs": fs + (x + 2) % 4 - x}
    far_y = {"fs": fs + 4 * ((y + 2) % 4 - y)}
    rows, width = x_ref.shape
    shard = u_ref.shape[0]
    hidden = u_ref.shape[1] // 2
    base = rep * hidden
    weights = (u_ref, d_ref)
    tokens = (x_ref, c_ref)
    pieces = 2
    chunk = rows // pieces
    half_rows = 2 * rows
    bw = 256
    blocks = hidden // bw
    all_parts = range(PARTS)
    f32, bf16 = jnp.float32, jnp.bfloat16

    flip = [(bit, 1 - bit) for bit in mine]
    tables = {}

    def slot(order, s):
        if order not in tables:
            place = {d: 2**k for k, d in enumerate(order)}
            high, low = [], []
            for v in range(8):
                bits = bits_of(4 * v)
                high.append(sum(flip[d][bits[d]] * place[d] for d in (0, 1, 2)))
            for v in range(4):
                bits = bits_of(v)
                low.append(sum(flip[d][bits[d]] * place[d] for d in (3, 4)))
            tables[order] = high, low
        high, low = tables[order]
        return high[s // 4] + low[s % 4]

    def home(m, p):
        return (m * PARTS + p) * 32 * SIZE

    def place_of(m, p):
        return (m * PARTS + p) * 32

    barrier = pltpu.get_barrier_semaphore()
    for device in near + [sibling, pair, twin, cross, far_x, far_y]:
        pl.semaphore_signal(barrier, inc=1, device_id=device, device_id_type=MESH)

    for m in range(2):
        pltpu.make_async_copy(tokens[m], tok.at[m, pl.ds(0, rows)], load_s.at[m]).start()
        for p in all_parts:
            columns = pl.ds(pl.multiple_of(base + p * 128, 128), 128)
            pltpu.make_async_copy(weights[m].at[:, columns], wg.at[place_of(m, p)], load_s.at[2 + m]).start()

    def wait_bytes(ref, sem):
        pltpu.make_async_copy(ref, ref, sem).wait()

    for m in range(2):
        wait_bytes(tok.at[m, pl.ds(0, rows)], load_s.at[m])
        wait_bytes(wg.at[pl.ds(0, PARTS)], load_s.at[2 + m])

    pl.semaphore_wait(barrier, STEPS + 6)

    def start(copy):
        copy.start()
        return copy

    def token_copy(m, q):
        return remote(
            tok.at[m, pl.ds(q * chunk, chunk)],
            tok.at[m, pl.ds(2 * rows + q * chunk, chunk)],
            sent.at[0],
            tok_r.at[m, q],
            pair,
        )

    def forward_copy(m, q):
        return remote(
            tok.at[m, pl.ds(2 * rows + q * chunk, chunk)],
            tok.at[m, pl.ds(3 * rows + q * chunk, chunk)],
            sent.at[1],
            fwd_r.at[m, q],
            sibling,
        )

    def sibling_copy(m):
        return remote(tok.at[m, pl.ds(0, rows)], tok.at[m, pl.ds(rows, rows)], sent.at[2], sib_r.at[m], sibling)

    def gather_copy(m, p, k):
        n = 2**k
        return remote(
            wg.at[pl.ds(place_of(m, p), n)],
            wg.at[pl.ds(place_of(m, p) + n, n)],
            sent.at[3 + m],
            g_r.at[m * PARTS + p, k],
            near[GATHER[m][p][k]],
        )

    def forward(m, q):
        token_copy(m, q).wait_recv()
        start(forward_copy(m, q))

    def transpose(m, g):
        tokt[m, :, g * rows : (g + 1) * rows] = tok[m, g * rows : (g + 1) * rows].T

    def unpack(m, p):
        for s in range(32):
            wn[m, s * shard : (s + 1) * shard, p * 128 : (p + 1) * 128] = wg[
                place_of(m, p) + slot(GATHER[m][p], s)
            ]

    def part_cols(j):
        return slice(j * bw, (j + 1) * bw)

    def forward_block(j):
        for h in range(2):
            part = slice(h * half_rows, (h + 1) * half_rows)
            kept = jnp.maximum(
                jnp.dot(tok[0, part], wn[0, :, part_cols(j)], preferred_element_type=f32), 0.0
            )
            pre[part, part_cols(j)] = kept
            act[part, part_cols(j)] = (kept * kept).astype(bf16)

    def back_block(j):
        for p in (2 * j, 2 * j + 1):
            gather_copy(1, p, STEPS - 1).wait_recv()
            unpack(1, p)
        for h in range(2):
            part = slice(h * half_rows, (h + 1) * half_rows)
            value = jnp.dot(tok[1, part], wn[1, :, part_cols(j)], preferred_element_type=f32)
            gpre[part, part_cols(j)] = (2.0 * pre[part, part_cols(j)] * value).astype(bf16)

    def room(m, p, k):
        before = sum(1 + HALF[i] * SIZE for i in range(k))
        return (m * PARTS + p) * (31 * SIZE + 5) + before

    def reduce_copy(m, p, k):
        place = pl.ds(room(m, p, k), 1 + HALF[k] * SIZE)
        return remote(
            sbuf.at[place],
            rbuf.at[place],
            sent.at[5],
            r_r.at[m * PARTS + p, k],
            near[REDUCE[m][p][STEPS - 1 - k]],
        )

    def chunks(count, size):
        step = min(count, 4) * size
        return count * size // step, step

    def highest(m, p, k):
        n = SIZE
        loops, step = chunks(HALF[k], n)
        at = home(m, p) + HALF[k] * n

        def some(i, top):
            return jnp.maximum(top, jnp.max(jnp.abs(gbuf[pl.ds(at + i * step, step)]), axis=0))

        return lax.fori_loop(0, loops, some, jnp.zeros((16, 128), f32))

    def send_sums(m, p, k, top):
        n = SIZE
        loops, step = chunks(HALF[k], n)
        at, to = home(m, p) + HALF[k] * n, room(m, p, k)
        coded = scale_of(top)
        sbuf[to] = coded
        scale = coded.astype(f32)

        def some(i, carry):
            sbuf[pl.ds(to + 1 + i * step, step)] = encode(gbuf[pl.ds(at + i * step, step)], scale)
            return carry

        lax.fori_loop(0, loops, some, 0)
        start(reduce_copy(m, p, k))

    def begin(m, p):
        send_sums(m, p, 0, highest(m, p, 0))

    def add_sums(m, p, k, first, count):
        n = SIZE
        loops, step = chunks(count, n)
        at, got = home(m, p) + first * n, room(m, p, k) + 1 + first * n
        scale = rbuf[room(m, p, k)].astype(f32)

        def some(i, top):
            place = pl.ds(at + i * step, step)
            value = gbuf[place] + decode(rbuf[pl.ds(got + i * step, step)], scale)
            gbuf[place] = value
            return jnp.maximum(top, jnp.max(jnp.abs(value), axis=0))

        return lax.fori_loop(0, loops, some, jnp.zeros((16, 128), f32))

    def reduce_step(m, p, k):
        reduce_copy(m, p, k).wait_recv()
        n = HALF[k + 1]
        top = add_sums(m, p, k, n, n)
        send_sums(m, p, k + 1, top)
        add_sums(m, p, k, 0, n)

    def weight_grad(m, right, j):
        tall = width // SPLIT
        for i in range(SPLIT):
            out = jnp.dot(
                tokt[m, i * tall : (i + 1) * tall, :], right[:, part_cols(j)], preferred_element_type=f32
            )
            for t in range(tall // shard):
                for e in range(2):
                    p = 2 * j + e
                    at = home(m, p) + slot(REDUCE[m][p], i * (tall // shard) + t) * SIZE
                    value = out[t * shard : (t + 1) * shard, e * 128 : (e + 1) * 128]
                    gbuf[pl.ds(at, SIZE)] = value.reshape(SIZE, 16, 128)
        begin(m, 2 * j)
        begin(m, 2 * j + 1)

    def share_copy(i):
        return remote(
            pre.at[pl.ds((1 + 2 * i) * rows, rows)], part_in.at[i], sent.at[6], pi_r.at[i], sibling
        )

    def pair_copy(q):
        return remote(pair_out.at[q], pair_in.at[q], sent.at[7], li_r.at[q], pair)

    for m in range(2):
        for p in all_parts:
            start(gather_copy(m, p, 0))
        for q in range(pieces):
            start(token_copy(m, q))
    for m in range(2):
        start(sibling_copy(m))

    unpacked = []
    for a in FIRST:
        if a == -1:
            for m in range(2):
                transpose(m, 0)
                sibling_copy(m).wait_recv()
                transpose(m, 1)
        elif a < 0:
            forward((-2 - a) // 2, (-2 - a) % 2)
        else:
            m, p, k = a // 100, a // 10 % 10, a % 10
            gather_copy(m, p, k).wait_recv()
            if k < STEPS - 1:
                start(gather_copy(m, p, k + 1))
                continue
            unpack(m, p)
            if not unpacked:
                for q in range(pieces):
                    forward_copy(0, q).wait_recv()
                transpose(0, 2)
                transpose(0, 3)
            unpacked.append(p)
            if p ^ 1 in unpacked:
                forward_block(p // 2)

    if -4 not in FIRST:
        forward(1, 0)
    forward(1, 1)
    transpose(1, 2)
    for q in range(pieces):
        forward_copy(1, q).wait_recv()
    transpose(1, 3)

    order = [a // 10 % 10 for a in THEN if a < 100 and a % 10 == STEPS - 1]
    groups = (tuple(all_parts), tuple(order[:4]), tuple(order[4:]))
    spots = (0, 17, 26)

    def twin_copy(g):
        place = pl.ds(spots[g], 1 + len(groups[g]) * SIZE)
        return remote(twin_out.at[place], twin_in.at[place], sent.at[10], rep_r.at[g], twin)

    def twin_send(g):
        m = 1 if g == 0 else 0
        top = jnp.zeros((16, 128), f32)
        for p in groups[g]:
            for i in range(SIZE):
                top = jnp.maximum(top, jnp.abs(outs[m, rep, p * SIZE + i]))
        coded = scale_of(top)
        twin_out[spots[g]] = coded
        scale = coded.astype(f32)
        for n, p in enumerate(groups[g]):
            code = encode(outs[m, rep, pl.ds(p * SIZE, SIZE)], scale)
            twin_out[pl.ds(spots[g] + 1 + n * SIZE, SIZE)] = code
        start(twin_copy(g))
        for n, p in enumerate(groups[g]):
            code = twin_out[pl.ds(spots[g] + 1 + n * SIZE, SIZE)]
            outs[m, rep, pl.ds(p * SIZE, SIZE)] = decode(code, scale)

    def twin_receive(g):
        m = 1 if g == 0 else 0
        twin_copy(g).wait_recv()
        scale = twin_in[spots[g]].astype(f32)
        for n, p in enumerate(groups[g]):
            code = twin_in[pl.ds(spots[g] + 1 + n * SIZE, SIZE)]
            outs[m, 1 - rep, pl.ds(p * SIZE, SIZE)] = decode(code, scale)

    def finish(m, p):
        n = SIZE
        reduce_copy(m, p, STEPS - 1).wait_recv()
        scale = rbuf[room(m, p, STEPS - 1)].astype(f32)
        got = decode(rbuf[pl.ds(room(m, p, STEPS - 1) + 1, n)], scale)
        value = (gbuf[pl.ds(home(m, p), n)] + got) * factor
        outs[m, rep, pl.ds(p * SIZE, n)] = value
        return value

    def output(i, src, dst):
        copy = pltpu.make_async_copy(src, dst, out_s.at[i])
        copy.start()
        return copy

    rounds = ((near[3], near[4], far_x), (near[1], near[2], far_y), (near[0], twin, pair))

    def energy_copy(k, i):
        return remote(ebuf.at[k, 0], ebuf.at[k, 1 + i], sent.at[8], e_r.at[k, i], rounds[k][i])

    def energy_begin(k):
        for i in range(3):
            start(energy_copy(k, i))

    def energy_step(k):
        for i in range(3):
            energy_copy(k, i).wait_recv()
        ebuf[k + 1, 0] = (ebuf[k, 0] + ebuf[k, 1]) + (ebuf[k, 2] + ebuf[k, 3])
        energy_begin(k + 1)

    squares = [jnp.zeros((16, 128), f32), jnp.zeros((16, 128), f32)]
    left = [PARTS, PARTS]
    outputs = []
    row_copies = []

    def arrived(m, p, k):
        if k < STEPS - 1:
            reduce_step(m, p, k)
            return
        value = finish(m, p)
        left[m] -= 1
        if m == 1:
            total = value[0] * value[0] + value[1] * value[1]
            ebuf[0, 0, p : p + 1, :] = jnp.sum(total, axis=0, keepdims=True)
            if left[m] == 0:
                energy_begin(0)
                twin_send(0)
            return
        for row in range(2):
            squares[row] = squares[row] + value[row] * value[row]
        if left[m] == 4:
            twin_send(1)
        if left[m] == 0:
            twin_send(2)
            for row in range(2):
                eup[0, row * 16 : row * 16 + 16] = squares[row]
            for i, device in enumerate((sibling, twin, cross)):
                row_copies.append(start(remote(eup.at[0], eup.at[1 + i], sent.at[9], eu_r.at[i], device)))

    def inputs_grad(i):
        part = slice(i * half_rows, (i + 1) * half_rows)
        for n in range(width // bw):
            pre[part, n * bw : (n + 1) * bw] = contract(
                gpre[part, :], wn[0, n * bw : (n + 1) * bw, :], 1, 1
            )
        start(share_copy(i))

    def share_arrived(i):
        share_copy(i).wait_recv()
        if i == 0:
            pre[0:rows] = pre[0:rows] + part_in[0]
            return
        for q in range(pieces):
            s = slice(q * chunk, (q + 1) * chunk)
            value = pre[2 * rows + q * chunk : 2 * rows + (q + 1) * chunk] + part_in[1, s]
            coded = scale_of(jnp.max(jnp.abs(value), axis=0, keepdims=True))
            pair_out[q, 0:16] = jnp.broadcast_to(coded, (16, width))
            pair_out[q, 16 : 16 + chunk] = encode(value, coded.astype(f32))
            start(pair_copy(q))

    def pair_arrived(q):
        pair_copy(q).wait_recv()
        s = slice(q * chunk, (q + 1) * chunk)
        scale = pair_in[q, 0:16].astype(f32)[0:1]
        gin[s] = (pre[s] + decode(pair_in[q, 16 : 16 + chunk], scale)).astype(bf16)
        if q == pieces - 1:
            outputs.append(output(0, gin, gin_ref))

    def energy_end():
        for i in range(3):
            energy_copy(2, i).wait_recv()
        ebuf[3, 0] = (ebuf[2, 0] + ebuf[2, 1]) * (1.0 / width)
        ebuf[3, 1] = (ebuf[2, 2] + ebuf[2, 3]) * (1.0 / width)
        outputs.append(output(2, ebuf.at[3, 0], edn_ref.at[rep]))
        outputs.append(output(3, ebuf.at[3, 1], edn_ref.at[1 - rep]))

    def twins_arrived(m):
        for g in (0,) if m == 1 else (1, 2):
            twin_receive(g)
        outputs.append(output(4 if m == 0 else 1, outs.at[m], grad_ref.at[m]))

    def run(a):
        if a < 200:
            arrived(a // 100, a // 10 % 10, a % 10)
        elif a < 1100:
            m, j = (a - 1000) // 10, a % 10
            weight_grad(m, (gpre, act)[m], j)
        elif a < 1200:
            back_block(a - 1100)
        elif a < 1300:
            inputs_grad(a - 1200)
        elif a < 1310:
            share_arrived(a - 1300)
        elif a < 1400:
            pair_arrived(a - 1310)
        elif a < 1402:
            energy_step(a - 1400)
        elif a == 1402:
            energy_end()
        else:
            twins_arrived(1)

    for a in THEN[:-3]:
        run(a)
    twins_arrived(0)
    for a in THEN[-3:]:
        run(a)
    for copy in row_copies:
        copy.wait_recv()
    outputs.append(output(5, eup, eup_ref))
    wait_bytes(tok.at[:, pl.ds(0, rows)], sent.at[0])
    wait_bytes(tok.at[:, pl.ds(0, rows)], sent.at[1])
    wait_bytes(tok.at[:, pl.ds(0, rows)], sent.at[2])
    for m in range(2):
        wait_bytes(wg.at[pl.ds(0, 31 * PARTS)], sent.at[3 + m])
    wait_bytes(sbuf, sent.at[5])
    wait_bytes(part_in, sent.at[6])
    wait_bytes(pair_out, sent.at[7])
    wait_bytes(ebuf.at[pl.ds(0, 3), pl.ds(0, 3)], sent.at[8])
    wait_bytes(eup.at[pl.ds(0, 3)], sent.at[9])
    wait_bytes(twin_out, sent.at[10])
    for copy in outputs:
        copy.wait()


def layout(
    gin_ref, grad_ref, eup_ref, edn_ref, gin_out, gup_out, gdn_out, eup_out, edn_out,
    gin, grad, eup, edn, both, row, in_s, out_s,
):
    pairs = ((gin_ref, gin), (grad_ref.at[1], grad.at[1]), (grad_ref.at[0], grad.at[0]), (eup_ref, eup), (edn_ref, edn))
    loads = [pltpu.make_async_copy(a, b, in_s.at[i]) for i, (a, b) in enumerate(pairs)]
    for copy in loads:
        copy.start()
    stores = []

    def store(i, src, dst):
        copy = pltpu.make_async_copy(src, dst, out_s.at[i])
        copy.start()
        stores.append(copy)

    half = gup_out.shape[1] // 2
    loads[3].wait()
    total = (eup[0] + eup[1]) + (eup[2] + eup[3])
    row[...] = jnp.sum(total.T, axis=0) * (1.0 / (4 * half))
    loads[4].wait()
    store(3, row, eup_out)
    store(4, edn, edn_out)
    loads[0].wait()
    store(0, gin, gin_out)
    for m, load, out in ((1, 1, gdn_out), (0, 2, gup_out)):
        loads[load].wait()
        for r in range(2):
            for u in range(UNITS):
                block, top = divmod(u, 2)
                left = r * half + block * 128
                both[m, top * 16 : top * 16 + 16, left : left + 128] = grad[m, r, u]
        store(load, both.at[m], out)
    for copy in stores:
        copy.wait()


def body(inputs, up_proj, down_proj, out_cotangent):
    rows, width = inputs.shape
    shard, both = up_proj.shape
    hidden = both // 2
    factor = float(rows * lax.axis_size("rep") * lax.axis_size("fs") * lax.axis_size("tp")) ** (-0.5)
    f32, bf16 = jnp.float32, jnp.bfloat16
    shape = jax.ShapeDtypeStruct
    dma = pltpu.SemaphoreType.DMA
    messages = 2 * PARTS * (31 * SIZE + 5)
    anywhere = pl.BlockSpec(memory_space=pl.ANY)
    raw = pl.pallas_call(
        functools.partial(kernel, factor),
        out_shape=(
            shape((rows, width), bf16),
            shape((2, 2, UNITS, 16, 128), f32),
            shape((4, shard, 128), f32),
            shape((2, BLOCKS, 128), f32),
        ),
        in_specs=[anywhere] * 4,
        out_specs=(anywhere,) * 4,
        scratch_shapes=[
            pltpu.VMEM((2, 4 * rows, width), bf16),
            pltpu.VMEM((2, width, 4 * rows), bf16),
            pltpu.VMEM((2 * PARTS * 32, shard, 128), bf16),
            pltpu.VMEM((2, width, hidden), bf16),
            pltpu.VMEM((4 * rows, max(hidden, width)), f32),
            pltpu.VMEM((4 * rows, hidden), bf16),
            pltpu.VMEM((4 * rows, hidden), bf16),
            pltpu.VMEM((2 * 32 * UNITS, 16, 128), f32),
            pltpu.VMEM((messages, 16, 128), bf16),
            pltpu.VMEM((messages, 16, 128), bf16),
            pltpu.VMEM((2, rows, width), f32),
            pltpu.VMEM((2, 16 + rows // 2, width), bf16),
            pltpu.VMEM((2, 16 + rows // 2, width), bf16),
            pltpu.VMEM((35, 16, 128), bf16),
            pltpu.VMEM((35, 16, 128), bf16),
            pltpu.VMEM((2, 2, UNITS, 16, 128), f32),
            pltpu.VMEM((rows, width), bf16),
            pltpu.VMEM((4, 4, BLOCKS, 128), f32),
            pltpu.VMEM((4, shard, 128), f32),
            dma((4,)),
            dma((2, 2)),
            dma((2, 2)),
            dma((2,)),
            dma((2 * PARTS, STEPS)),
            dma((2 * PARTS, STEPS)),
            dma((3,)),
            dma((2,)),
            dma((2,)),
            dma((3, 3)),
            dma((3,)),
            dma((11,)),
            dma((6,)),
        ],
        compiler_params=pltpu.CompilerParams(
            collective_id=0, has_side_effects=True, vmem_limit_bytes=60 * 2**20
        ),
        name="step",
    )(inputs, out_cotangent, up_proj, down_proj.T)
    gin, gup, gdn, eup, edn = pl.pallas_call(
        layout,
        out_shape=(
            shape((rows, width), bf16),
            shape((shard, both), f32),
            shape((shard, both), f32),
            shape((shard,), f32),
            shape((2, BLOCKS, 128), f32),
        ),
        in_specs=[anywhere] * 4,
        out_specs=(anywhere,) * 5,
        scratch_shapes=[
            pltpu.VMEM((rows, width), bf16),
            pltpu.VMEM((2, 2, UNITS, 16, 128), f32),
            pltpu.VMEM((4, shard, 128), f32),
            pltpu.VMEM((2, BLOCKS, 128), f32),
            pltpu.VMEM((2, shard, both), f32),
            pltpu.VMEM((shard,), f32),
            dma((5,)),
            dma((5,)),
        ],
        name="layout",
    )(*raw)
    return gin, gup, gdn.T, eup, edn.reshape((both,))


def solution(mesh):
    return jax.shard_map(
        body,
        mesh=mesh,
        in_specs=(
            P(("rep", "fs", "tp"), None),
            P("fs", "tp"),
            P("tp", "fs"),
            P(("rep", "fs", "tp"), None),
        ),
        out_specs=(P(("rep", "fs", "tp"), None), P("fs", "tp"), P("tp", "fs"), P("fs"), P("tp")),
        check_vma=False,
    )
```

```python
import functools

import jax
import jax.numpy as jnp
from jax import lax
from jax.experimental import pallas as pl
from jax.experimental.pallas import tpu as pltpu
from jax.sharding import PartitionSpec as P

MESH = pl.DeviceIdType.MESH
GATHER = (
    (
        (2, 4, 0, 1, 3),
        (0, 3, 1, 2, 4),
        (1, 4, 0, 2, 3),
        (2, 3, 1, 0, 4),
        (4, 0, 2, 3, 1),
        (4, 3, 0, 1, 2),
        (1, 2, 3, 4, 0),
        (3, 1, 4, 0, 2),
    ),
    (
        (0, 4, 1, 3, 2),
        (3, 2, 0, 1, 4),
        (2, 4, 3, 1, 0),
        (1, 3, 2, 0, 4),
        (0, 1, 2, 4, 3),
        (2, 4, 3, 1, 0),
        (2, 1, 4, 0, 3),
        (3, 0, 4, 2, 1),
    ),
)
REDUCE = (
    (
        (4, 3, 0, 1, 2),
        (0, 2, 1, 4, 3),
        (0, 1, 4, 3, 2),
        (2, 4, 3, 1, 0),
        (2, 3, 0, 4, 1),
        (1, 0, 3, 2, 4),
        (2, 4, 1, 0, 3),
        (4, 0, 3, 1, 2),
    ),
    (
        (3, 4, 0, 1, 2),
        (2, 0, 4, 1, 3),
        (0, 2, 3, 4, 1),
        (4, 2, 3, 1, 0),
        (2, 3, 0, 1, 4),
        (3, 1, 0, 4, 2),
        (2, 4, 0, 3, 1),
        (1, 3, 2, 4, 0),
    ),
)
FIRST = (
    0, 10, 20, 40, 70, 30, 50, 60, 100, 110, 120, 130, 140, 170, 150, 160,
    1, 11, 41, 71, 61, 21, 31, 51, 101, 111, 141, 161, 171, 121, 131,
    151, 2, 12, 42, 72, 62, 22, 32, 52, 102, 122, 142, 132, -2, 162, 172,
    152, 112, 3, 13, 43, 63, 73, 53, 23, 33, 103, 143, 123, 173, 133, -3, -1,
    153, 163, 4, 14, 113, 74, 64, 24, 34, 44, 54,
)
THEN = (
    1010, 1011, 1012, 1013, 1100, 1101, 1102, 100, 110, 1103, 120, 130, 1000, 140, 150, 1001,
    160, 170, 101, 121, 1002, 111, 151, 1003, 1201, 0, 10, 131, 171, 1200, 30, 161,
    141, 1301, 102, 122, 20, 152, 1300, 50, 40, 112, 162, 60, 70, 1, 142, 132,
    172, 11, 123, 103, 31, 21, 153, 113, 51, 41, 143, 163, 133, 173, 61, 104,
    71, 2, 12, 124, 114, 32, 154, 22, 144, 134, 52, 164, 42, 174, 62, 72,
    13, 3, 33, 23, 53, 43, 1400, 63, 73, 4, 1500, 14, 34, 24, 54, 44,
    64, 74, 1401, 1402, 1310, 1311,
)
STEPS = 5
PARTS = 8
SPLIT = 2
SIZE = 2
UNITS = 16
BLOCKS = 8
HALF = (16, 8, 4, 2, 1)
SPAN = 240.0
SHIFT = 120.0


def encode(value, scale):
    code = jnp.exp2(jnp.abs(value) * (SPAN / scale) - SHIFT)
    return jnp.where(value < 0.0, -code, code).astype(jnp.bfloat16)


def decode(code, scale):
    code = code.astype(jnp.float32)
    size = (jnp.log2(jnp.abs(code)) + SHIFT) * (scale * (1.0 / SPAN))
    return jnp.where(code < 0.0, -size, size)


def scale_of(top):
    return (top * 1.01 + 1e-35).astype(jnp.bfloat16)


def bits_of(fs):
    z, y, x = fs // 16, (fs // 4) % 4, fs % 4
    return (z, (y % 2 + y // 2) % 2, y // 2, (x % 2 + x // 2) % 2, x // 2)


def partners_of(fs):
    z, y, x = fs // 16, (fs // 4) % 4, fs % 4
    return (
        fs + 16 - 32 * z,
        fs + 4 - 8 * (y % 2),
        fs + 12 - 8 * y,
        fs + 1 - 2 * (x % 2),
        fs + 3 - 2 * x,
    )


def remote(src, dst, send, recv, device):
    return pltpu.make_async_remote_copy(
        src_ref=src, dst_ref=dst, send_sem=send, recv_sem=recv, device_id=device, device_id_type=MESH
    )


def contract(left, right, left_dim, right_dim):
    return lax.dot_general(
        left, right, (((left_dim,), (right_dim,)), ((), ())), preferred_element_type=jnp.float32
    )


def kernel(
    factor,
    x_ref,
    c_ref,
    u_ref,
    d_ref,
    gin_ref,
    grad_ref,
    eup_ref,
    edn_ref,
    tok,
    tokt,
    wg,
    wn,
    pre,
    act,
    gpre,
    gbuf,
    sbuf,
    rbuf,
    part_in,
    pair_out,
    pair_in,
    twin_out,
    twin_in,
    outs,
    gin,
    ebuf,
    eup,
    load_s,
    tok_r,
    fwd_r,
    sib_r,
    g_r,
    r_r,
    rep_r,
    pi_r,
    li_r,
    e_r,
    eu_r,
    sent,
    out_s,
):
    rep, fs, tp = lax.axis_index("rep"), lax.axis_index("fs"), lax.axis_index("tp")
    mine = bits_of(fs)
    near = [{"fs": other} for other in partners_of(fs)]
    sibling = {"tp": 1 - tp}
    pair = {"rep": 1 - rep, "fs": partners_of(fs)[0]}
    twin = {"rep": 1 - rep}
    cross = {"rep": 1 - rep, "tp": 1 - tp}
    z, y, x = fs // 16, (fs // 4) % 4, fs % 4
    far_x = {"fs": fs + (x + 2) % 4 - x}
    far_y = {"fs": fs + 4 * ((y + 2) % 4 - y)}
    rows, width = x_ref.shape
    shard = u_ref.shape[0]
    hidden = u_ref.shape[1] // 2
    base = rep * hidden
    weights = (u_ref, d_ref)
    tokens = (x_ref, c_ref)
    pieces = 2
    chunk = rows // pieces
    cuts = (2, 4)
    half_rows = 2 * rows
    bw = 256
    blocks = hidden // bw
    all_parts = range(PARTS)
    f32, bf16 = jnp.float32, jnp.bfloat16

    flip = [(bit, 1 - bit) for bit in mine]
    tables = {}

    def slot(order, s):
        if order not in tables:
            place = {d: 2**k for k, d in enumerate(order)}
            high, low = [], []
            for v in range(8):
                bits = bits_of(4 * v)
                high.append(sum(flip[d][bits[d]] * place[d] for d in (0, 1, 2)))
            for v in range(4):
                bits = bits_of(v)
                low.append(sum(flip[d][bits[d]] * place[d] for d in (3, 4)))
            tables[order] = high, low
        high, low = tables[order]
        return high[s // 4] + low[s % 4]

    def home(m, p):
        return (m * PARTS + p) * 32 * SIZE

    def place_of(m, p):
        return (m * PARTS + p) * 32

    barrier = pltpu.get_barrier_semaphore()
    for device in near + [sibling, pair, twin, cross, far_x, far_y]:
        pl.semaphore_signal(barrier, inc=1, device_id=device, device_id_type=MESH)

    for m in range(2):
        pltpu.make_async_copy(tokens[m], tok.at[m, pl.ds(0, rows)], load_s.at[m]).start()
        for p in all_parts:
            columns = pl.ds(pl.multiple_of(base + p * 128, 128), 128)
            pltpu.make_async_copy(weights[m].at[:, columns], wg.at[place_of(m, p)], load_s.at[2 + m]).start()

    def wait_bytes(ref, sem):
        pltpu.make_async_copy(ref, ref, sem).wait()

    for m in range(2):
        wait_bytes(tok.at[m, pl.ds(0, rows)], load_s.at[m])
        wait_bytes(wg.at[pl.ds(0, PARTS)], load_s.at[2 + m])

    pl.semaphore_wait(barrier, STEPS + 6)

    def start(copy):
        copy.start()
        return copy

    def token_copy(m, q):
        return remote(
            tok.at[m, pl.ds(q * (rows // cuts[m]), rows // cuts[m])],
            tok.at[m, pl.ds(2 * rows + q * (rows // cuts[m]), rows // cuts[m])],
            sent.at[0],
            tok_r.at[m, q],
            pair,
        )

    def forward_copy(m, q):
        return remote(
            tok.at[m, pl.ds(2 * rows + q * (rows // cuts[m]), rows // cuts[m])],
            tok.at[m, pl.ds(3 * rows + q * (rows // cuts[m]), rows // cuts[m])],
            sent.at[1],
            fwd_r.at[m, q],
            sibling,
        )

    def sibling_copy(m):
        return remote(tok.at[m, pl.ds(0, rows)], tok.at[m, pl.ds(rows, rows)], sent.at[2], sib_r.at[m], sibling)

    def gather_copy(m, p, k):
        n = 2**k
        return remote(
            wg.at[pl.ds(place_of(m, p), n)],
            wg.at[pl.ds(place_of(m, p) + n, n)],
            sent.at[3 + m],
            g_r.at[m * PARTS + p, k],
            near[GATHER[m][p][k]],
        )

    def forward(m, q):
        token_copy(m, q).wait_recv()
        start(forward_copy(m, q))

    def transpose(m, g):
        tokt[m, :, g * rows : (g + 1) * rows] = tok[m, g * rows : (g + 1) * rows].T

    def unpack(m, p):
        for s in range(32):
            wn[m, s * shard : (s + 1) * shard, p * 128 : (p + 1) * 128] = wg[
                place_of(m, p) + slot(GATHER[m][p], s)
            ]

    def part_cols(j):
        return slice(j * bw, (j + 1) * bw)

    def forward_block(j):
        for h in range(2):
            part = slice(h * half_rows, (h + 1) * half_rows)
            kept = jnp.maximum(
                jnp.dot(tok[0, part], wn[0, :, part_cols(j)], preferred_element_type=f32), 0.0
            )
            pre[part, part_cols(j)] = kept
            act[part, part_cols(j)] = (kept * kept).astype(bf16)

    def back_block(j):
        for p in (2 * j, 2 * j + 1):
            gather_copy(1, p, STEPS - 1).wait_recv()
            unpack(1, p)
        for h in range(2):
            part = slice(h * half_rows, (h + 1) * half_rows)
            value = jnp.dot(tok[1, part], wn[1, :, part_cols(j)], preferred_element_type=f32)
            gpre[part, part_cols(j)] = (2.0 * pre[part, part_cols(j)] * value).astype(bf16)

    def room(m, p, k):
        before = sum(1 + HALF[i] * SIZE for i in range(k))
        return (m * PARTS + p) * (31 * SIZE + 5) + before

    def reduce_copy(m, p, k):
        place = pl.ds(room(m, p, k), 1 + HALF[k] * SIZE)
        return remote(
            sbuf.at[place],
            rbuf.at[place],
            sent.at[5],
            r_r.at[m * PARTS + p, k],
            near[REDUCE[m][p][STEPS - 1 - k]],
        )

    def chunks(count, size):
        step = min(count, 4) * size
        return count * size // step, step

    def highest(m, p, k):
        n = SIZE
        loops, step = chunks(HALF[k], n)
        at = home(m, p) + HALF[k] * n

        def some(i, top):
            return jnp.maximum(top, jnp.max(jnp.abs(gbuf[pl.ds(at + i * step, step)]), axis=0))

        return lax.fori_loop(0, loops, some, jnp.zeros((16, 128), f32))

    def send_sums(m, p, k, top):
        n = SIZE
        loops, step = chunks(HALF[k], n)
        at, to = home(m, p) + HALF[k] * n, room(m, p, k)
        coded = scale_of(top)
        sbuf[to] = coded
        scale = coded.astype(f32)

        def some(i, carry):
            sbuf[pl.ds(to + 1 + i * step, step)] = encode(gbuf[pl.ds(at + i * step, step)], scale)
            return carry

        lax.fori_loop(0, loops, some, 0)
        start(reduce_copy(m, p, k))

    def begin(m, p):
        send_sums(m, p, 0, highest(m, p, 0))

    def add_sums(m, p, k, first, count):
        n = SIZE
        loops, step = chunks(count, n)
        at, got = home(m, p) + first * n, room(m, p, k) + 1 + first * n
        scale = rbuf[room(m, p, k)].astype(f32)

        def some(i, top):
            place = pl.ds(at + i * step, step)
            value = gbuf[place] + decode(rbuf[pl.ds(got + i * step, step)], scale)
            gbuf[place] = value
            return jnp.maximum(top, jnp.max(jnp.abs(value), axis=0))

        return lax.fori_loop(0, loops, some, jnp.zeros((16, 128), f32))

    def reduce_step(m, p, k):
        reduce_copy(m, p, k).wait_recv()
        n = HALF[k + 1]
        top = add_sums(m, p, k, n, n)
        send_sums(m, p, k + 1, top)
        add_sums(m, p, k, 0, n)

    def weight_grad(m, right, j):
        tall = width // SPLIT
        for i in range(SPLIT):
            out = jnp.dot(
                tokt[m, i * tall : (i + 1) * tall, :], right[:, part_cols(j)], preferred_element_type=f32
            )
            for t in range(tall // shard):
                for e in range(2):
                    p = 2 * j + e
                    at = home(m, p) + slot(REDUCE[m][p], i * (tall // shard) + t) * SIZE
                    value = out[t * shard : (t + 1) * shard, e * 128 : (e + 1) * 128]
                    gbuf[pl.ds(at, SIZE)] = value.reshape(SIZE, 16, 128)
        begin(m, 2 * j)
        begin(m, 2 * j + 1)

    def share_copy(i):
        return remote(
            pre.at[pl.ds((1 + 2 * i) * rows, rows)], part_in.at[i], sent.at[6], pi_r.at[i], sibling
        )

    def pair_copy(q):
        return remote(pair_out.at[q], pair_in.at[q], sent.at[7], li_r.at[q], pair)

    for m in range(2):
        for p in all_parts:
            start(gather_copy(m, p, 0))
        for q in range(cuts[m]):
            start(token_copy(m, q))
    for m in range(2):
        start(sibling_copy(m))

    unpacked = []
    for a in FIRST:
        if a == -1:
            for m in range(2):
                transpose(m, 0)
                sibling_copy(m).wait_recv()
                transpose(m, 1)
        elif a < 0:
            forward((-2 - a) // 2, (-2 - a) % 2)
        else:
            m, p, k = a // 100, a // 10 % 10, a % 10
            gather_copy(m, p, k).wait_recv()
            if k < STEPS - 1:
                start(gather_copy(m, p, k + 1))
                continue
            unpack(m, p)
            if not unpacked:
                for q in range(pieces):
                    forward_copy(0, q).wait_recv()
                transpose(0, 2)
                transpose(0, 3)
            unpacked.append(p)
            if p ^ 1 in unpacked:
                forward_block(p // 2)

    for q in range(cuts[1]):
        forward(1, q)
    transpose(1, 2)
    for q in range(cuts[1]):
        forward_copy(1, q).wait_recv()
    transpose(1, 3)

    order = [a // 10 % 10 for a in THEN if a < 100 and a % 10 == STEPS - 1]
    groups = (tuple(all_parts), tuple(order[:6]), tuple(order[6:]))
    spots = (0, 17, 30)

    def twin_copy(g):
        place = pl.ds(spots[g], 1 + len(groups[g]) * SIZE)
        return remote(twin_out.at[place], twin_in.at[place], sent.at[10], rep_r.at[g], twin)

    def twin_send(g):
        m = 1 if g == 0 else 0
        top = jnp.zeros((16, 128), f32)
        for p in groups[g]:
            for i in range(SIZE):
                top = jnp.maximum(top, jnp.abs(outs[m, rep, p * SIZE + i]))
        coded = scale_of(top)
        twin_out[spots[g]] = coded
        scale = coded.astype(f32)
        for n, p in enumerate(groups[g]):
            code = encode(outs[m, rep, pl.ds(p * SIZE, SIZE)], scale)
            twin_out[pl.ds(spots[g] + 1 + n * SIZE, SIZE)] = code
        start(twin_copy(g))
        for n, p in enumerate(groups[g]):
            code = twin_out[pl.ds(spots[g] + 1 + n * SIZE, SIZE)]
            outs[m, rep, pl.ds(p * SIZE, SIZE)] = decode(code, scale)

    def twin_receive(g):
        m = 1 if g == 0 else 0
        twin_copy(g).wait_recv()
        scale = twin_in[spots[g]].astype(f32)
        for n, p in enumerate(groups[g]):
            code = twin_in[pl.ds(spots[g] + 1 + n * SIZE, SIZE)]
            outs[m, 1 - rep, pl.ds(p * SIZE, SIZE)] = decode(code, scale)

    def finish(m, p):
        n = SIZE
        reduce_copy(m, p, STEPS - 1).wait_recv()
        scale = rbuf[room(m, p, STEPS - 1)].astype(f32)
        got = decode(rbuf[pl.ds(room(m, p, STEPS - 1) + 1, n)], scale)
        value = (gbuf[pl.ds(home(m, p), n)] + got) * factor
        outs[m, rep, pl.ds(p * SIZE, n)] = value
        return value

    def output(i, src, dst):
        copy = pltpu.make_async_copy(src, dst, out_s.at[i])
        copy.start()
        return copy

    rounds = ((near[3], near[4], far_x), (near[1], near[2], far_y), (near[0], twin, pair))

    def energy_copy(k, i):
        return remote(ebuf.at[k, 0], ebuf.at[k, 1 + i], sent.at[8], e_r.at[k, i], rounds[k][i])

    def energy_begin(k):
        for i in range(3):
            start(energy_copy(k, i))

    def energy_step(k):
        for i in range(3):
            energy_copy(k, i).wait_recv()
        ebuf[k + 1, 0] = (ebuf[k, 0] + ebuf[k, 1]) + (ebuf[k, 2] + ebuf[k, 3])
        energy_begin(k + 1)

    squares = [jnp.zeros((16, 128), f32), jnp.zeros((16, 128), f32)]
    left = [PARTS, PARTS]
    outputs = []
    row_copies = []

    def arrived(m, p, k):
        if k < STEPS - 1:
            reduce_step(m, p, k)
            return
        value = finish(m, p)
        left[m] -= 1
        if m == 1:
            total = value[0] * value[0] + value[1] * value[1]
            ebuf[0, 0, p : p + 1, :] = jnp.sum(total, axis=0, keepdims=True)
            if left[m] == 0:
                energy_begin(0)
                twin_send(0)
            return
        for row in range(2):
            squares[row] = squares[row] + value[row] * value[row]
        if left[m] == 2:
            twin_send(1)
        if left[m] == 0:
            twin_send(2)
            for row in range(2):
                eup[0, row * 16 : row * 16 + 16] = squares[row]
            for i, device in enumerate((sibling, twin, cross)):
                row_copies.append(start(remote(eup.at[0], eup.at[1 + i], sent.at[9], eu_r.at[i], device)))

    def inputs_grad(i):
        part = slice(i * half_rows, (i + 1) * half_rows)
        for n in range(width // bw):
            pre[part, n * bw : (n + 1) * bw] = contract(
                gpre[part, :], wn[0, n * bw : (n + 1) * bw, :], 1, 1
            )
        start(share_copy(i))

    def share_arrived(i):
        share_copy(i).wait_recv()
        if i == 0:
            pre[0:rows] = pre[0:rows] + part_in[0]
            return
        for q in range(pieces):
            s = slice(q * chunk, (q + 1) * chunk)
            value = pre[2 * rows + q * chunk : 2 * rows + (q + 1) * chunk] + part_in[1, s]
            coded = scale_of(jnp.max(jnp.abs(value), axis=0, keepdims=True))
            pair_out[q, 0:16] = jnp.broadcast_to(coded, (16, width))
            pair_out[q, 16 : 16 + chunk] = encode(value, coded.astype(f32))
            start(pair_copy(q))

    def pair_arrived(q):
        pair_copy(q).wait_recv()
        s = slice(q * chunk, (q + 1) * chunk)
        scale = pair_in[q, 0:16].astype(f32)[0:1]
        gin[s] = (pre[s] + decode(pair_in[q, 16 : 16 + chunk], scale)).astype(bf16)
        if q == pieces - 1:
            outputs.append(output(0, gin, gin_ref))

    def energy_end():
        for i in range(3):
            energy_copy(2, i).wait_recv()
        ebuf[3, 0] = (ebuf[2, 0] + ebuf[2, 1]) * (1.0 / width)
        ebuf[3, 1] = (ebuf[2, 2] + ebuf[2, 3]) * (1.0 / width)
        outputs.append(output(2, ebuf.at[3, 0], edn_ref.at[rep]))
        outputs.append(output(3, ebuf.at[3, 1], edn_ref.at[1 - rep]))

    def twins_arrived(m):
        for g in (0,) if m == 1 else (1, 2):
            twin_receive(g)
        outputs.append(output(4 if m == 0 else 1, outs.at[m], grad_ref.at[m]))

    def run(a):
        if a < 200:
            arrived(a // 100, a // 10 % 10, a % 10)
        elif a < 1100:
            m, j = (a - 1000) // 10, a % 10
            weight_grad(m, (gpre, act)[m], j)
        elif a < 1200:
            back_block(a - 1100)
        elif a < 1300:
            inputs_grad(a - 1200)
        elif a < 1310:
            share_arrived(a - 1300)
        elif a < 1400:
            pair_arrived(a - 1310)
        elif a < 1402:
            energy_step(a - 1400)
        elif a == 1402:
            energy_end()
        else:
            twins_arrived(1)

    for a in THEN[:-3]:
        run(a)
    twins_arrived(0)
    for a in THEN[-3:]:
        run(a)
    for copy in row_copies:
        copy.wait_recv()
    outputs.append(output(5, eup, eup_ref))
    wait_bytes(tok.at[:, pl.ds(0, rows)], sent.at[0])
    wait_bytes(tok.at[:, pl.ds(0, rows)], sent.at[1])
    wait_bytes(tok.at[:, pl.ds(0, rows)], sent.at[2])
    for m in range(2):
        wait_bytes(wg.at[pl.ds(0, 31 * PARTS)], sent.at[3 + m])
    wait_bytes(sbuf, sent.at[5])
    wait_bytes(part_in, sent.at[6])
    wait_bytes(pair_out, sent.at[7])
    wait_bytes(ebuf.at[pl.ds(0, 3), pl.ds(0, 3)], sent.at[8])
    wait_bytes(eup.at[pl.ds(0, 3)], sent.at[9])
    wait_bytes(twin_out, sent.at[10])
    for copy in outputs:
        copy.wait()


def layout(
    gin_ref, grad_ref, eup_ref, edn_ref, gin_out, gup_out, gdn_out, eup_out, edn_out,
    gin, grad, eup, edn, both, row, in_s, out_s,
):
    pairs = ((gin_ref, gin), (grad_ref.at[1], grad.at[1]), (grad_ref.at[0], grad.at[0]), (eup_ref, eup), (edn_ref, edn))
    loads = [pltpu.make_async_copy(a, b, in_s.at[i]) for i, (a, b) in enumerate(pairs)]
    for copy in loads:
        copy.start()
    stores = []

    def store(i, src, dst):
        copy = pltpu.make_async_copy(src, dst, out_s.at[i])
        copy.start()
        stores.append(copy)

    half = gup_out.shape[1] // 2
    loads[3].wait()
    total = (eup[0] + eup[1]) + (eup[2] + eup[3])
    row[...] = jnp.sum(total.T, axis=0) * (1.0 / (4 * half))
    loads[4].wait()
    store(3, row, eup_out)
    store(4, edn, edn_out)
    loads[0].wait()
    store(0, gin, gin_out)
    for m, load, out in ((1, 1, gdn_out), (0, 2, gup_out)):
        loads[load].wait()
        for r in range(2):
            for u in range(UNITS):
                block, top = divmod(u, 2)
                left = r * half + block * 128
                both[m, top * 16 : top * 16 + 16, left : left + 128] = grad[m, r, u]
        store(load, both.at[m], out)
    for copy in stores:
        copy.wait()


def body(inputs, up_proj, down_proj, out_cotangent):
    rows, width = inputs.shape
    shard, both = up_proj.shape
    hidden = both // 2
    factor = float(rows * lax.axis_size("rep") * lax.axis_size("fs") * lax.axis_size("tp")) ** (-0.5)
    f32, bf16 = jnp.float32, jnp.bfloat16
    shape = jax.ShapeDtypeStruct
    dma = pltpu.SemaphoreType.DMA
    messages = 2 * PARTS * (31 * SIZE + 5)
    anywhere = pl.BlockSpec(memory_space=pl.ANY)
    raw = pl.pallas_call(
        functools.partial(kernel, factor),
        out_shape=(
            shape((rows, width), bf16),
            shape((2, 2, UNITS, 16, 128), f32),
            shape((4, shard, 128), f32),
            shape((2, BLOCKS, 128), f32),
        ),
        in_specs=[anywhere] * 4,
        out_specs=(anywhere,) * 4,
        scratch_shapes=[
            pltpu.VMEM((2, 4 * rows, width), bf16),
            pltpu.VMEM((2, width, 4 * rows), bf16),
            pltpu.VMEM((2 * PARTS * 32, shard, 128), bf16),
            pltpu.VMEM((2, width, hidden), bf16),
            pltpu.VMEM((4 * rows, max(hidden, width)), f32),
            pltpu.VMEM((4 * rows, hidden), bf16),
            pltpu.VMEM((4 * rows, hidden), bf16),
            pltpu.VMEM((2 * 32 * UNITS, 16, 128), f32),
            pltpu.VMEM((messages, 16, 128), bf16),
            pltpu.VMEM((messages, 16, 128), bf16),
            pltpu.VMEM((2, rows, width), f32),
            pltpu.VMEM((2, 16 + rows // 2, width), bf16),
            pltpu.VMEM((2, 16 + rows // 2, width), bf16),
            pltpu.VMEM((35, 16, 128), bf16),
            pltpu.VMEM((35, 16, 128), bf16),
            pltpu.VMEM((2, 2, UNITS, 16, 128), f32),
            pltpu.VMEM((rows, width), bf16),
            pltpu.VMEM((4, 4, BLOCKS, 128), f32),
            pltpu.VMEM((4, shard, 128), f32),
            dma((4,)),
            dma((2, 4)),
            dma((2, 4)),
            dma((2,)),
            dma((2 * PARTS, STEPS)),
            dma((2 * PARTS, STEPS)),
            dma((3,)),
            dma((2,)),
            dma((2,)),
            dma((3, 3)),
            dma((3,)),
            dma((11,)),
            dma((6,)),
        ],
        compiler_params=pltpu.CompilerParams(
            collective_id=0, has_side_effects=True, vmem_limit_bytes=60 * 2**20
        ),
        name="step",
    )(inputs, out_cotangent, up_proj, down_proj.T)
    gin, gup, gdn, eup, edn = pl.pallas_call(
        layout,
        out_shape=(
            shape((rows, width), bf16),
            shape((shard, both), f32),
            shape((shard, both), f32),
            shape((shard,), f32),
            shape((2, BLOCKS, 128), f32),
        ),
        in_specs=[anywhere] * 4,
        out_specs=(anywhere,) * 5,
        scratch_shapes=[
            pltpu.VMEM((rows, width), bf16),
            pltpu.VMEM((2, 2, UNITS, 16, 128), f32),
            pltpu.VMEM((4, shard, 128), f32),
            pltpu.VMEM((2, BLOCKS, 128), f32),
            pltpu.VMEM((2, shard, both), f32),
            pltpu.VMEM((shard,), f32),
            dma((5,)),
            dma((5,)),
        ],
        name="layout",
    )(*raw)
    return gin, gup, gdn.T, eup, edn.reshape((both,))


def solution(mesh):
    return jax.shard_map(
        body,
        mesh=mesh,
        in_specs=(
            P(("rep", "fs", "tp"), None),
            P("fs", "tp"),
            P("tp", "fs"),
            P(("rep", "fs", "tp"), None),
        ),
        out_specs=(P(("rep", "fs", "tp"), None), P("fs", "tp"), P("tp", "fs"), P("fs"), P("tp")),
        check_vma=False,
    )
```

```python
import functools

import jax
import jax.numpy as jnp
from jax import lax
from jax.experimental import pallas as pl
from jax.experimental.pallas import tpu as pltpu
from jax.sharding import PartitionSpec as P

MESH = pl.DeviceIdType.MESH
GATHER = (
    (
        (2, 4, 0, 1, 3),
        (0, 3, 1, 2, 4),
        (1, 4, 0, 2, 3),
        (2, 3, 1, 0, 4),
        (4, 0, 2, 3, 1),
        (4, 3, 0, 1, 2),
        (1, 2, 3, 4, 0),
        (3, 1, 4, 0, 2),
    ),
    (
        (0, 4, 1, 3, 2),
        (3, 2, 0, 1, 4),
        (2, 4, 3, 1, 0),
        (1, 3, 2, 0, 4),
        (0, 1, 2, 4, 3),
        (2, 4, 3, 1, 0),
        (2, 1, 4, 0, 3),
        (3, 0, 4, 2, 1),
    ),
)
REDUCE = (
    (
        (3, 4, 2, 0, 1),
        (4, 3, 0, 1, 2),
        (1, 2, 0, 4, 3),
        (2, 1, 0, 4, 3),
        (3, 4, 0, 2, 1),
        (3, 4, 2, 1, 0),
        (2, 1, 0, 3, 4),
        (3, 4, 1, 0, 2),
    ),
    (
        (1, 2, 0, 4, 3),
        (4, 3, 1, 0, 2),
        (1, 2, 4, 3, 0),
        (4, 3, 2, 0, 1),
        (2, 1, 0, 4, 3),
        (4, 3, 0, 2, 1),
        (1, 2, 3, 0, 4),
        (2, 1, 3, 4, 0),
    ),
)
FIRST = (
    0, 10, 20, 40, 70, 30, 50, 60, 100, 110, 120, 130, 140, 170, 150, 160,
    1, 11, 41, 71, 61, 21, 31, 51, 101, 111, 141, 161, 171, 121, 131,
    151, 2, 12, 42, 72, 62, 22, 32, 52, 102, 122, 142, 132, -2, 162, 172,
    152, 112, 3, 13, 43, 63, 73, 53, 23, 33, 103, 143, 123, 173, 133, -3, -1,
    153, 163, 4, 14, 113, 74, 64, 24, 34, 44, 54,
)
THEN = (
    1010, 1011, 1012, 1013, 1100, 1101, 1102, 100, 110, 1103, 120, 130, 1000, 140, 160, 1001,
    170, 150, 101, 1002, 111, 121, 1003, 131, 141, 1201, 0, 161, 10, 171, 102, 1200,
    122, 20, 151, 40, 1301, 50, 112, 60, 30, 70, 142, 162, 1300, 132, 11, 172,
    1, 103, 152, 21, 123, 41, 51, 113, 31, 61, 71, 143, 163, 12, 133, 173,
    2, 22, 153, 42, 52, 32, 72, 62, 13, 3, 1400, 23, 43, 1500, 53, 33,
    73, 63, 1401, 1402, 1310, 1311,
)
STEPS = 5
PARTS = 8
SPLIT = 2
SIZE = 2
UNITS = 16
BLOCKS = 8
HALF = (16, 8, 4)
HALVINGS = 3
ROOM = 68
SPAN = 240.0
SHIFT = 120.0


def encode(value, scale):
    code = jnp.exp2(jnp.abs(value) * (SPAN / scale) - SHIFT)
    return jnp.where(value < 0.0, -code, code).astype(jnp.bfloat16)


def decode(code, scale):
    code = code.astype(jnp.float32)
    size = (jnp.log2(jnp.abs(code)) + SHIFT) * (scale * (1.0 / SPAN))
    return jnp.where(code < 0.0, -size, size)


def scale_of(top):
    return (top * 1.01 + 1e-35).astype(jnp.bfloat16)


def bits_of(fs):
    z, y, x = fs // 16, (fs // 4) % 4, fs % 4
    return (z, (y % 2 + y // 2) % 2, y // 2, (x % 2 + x // 2) % 2, x // 2)


def partners_of(fs):
    z, y, x = fs // 16, (fs // 4) % 4, fs % 4
    return (
        fs + 16 - 32 * z,
        fs + 4 - 8 * (y % 2),
        fs + 12 - 8 * y,
        fs + 1 - 2 * (x % 2),
        fs + 3 - 2 * x,
    )


def remote(src, dst, send, recv, device):
    return pltpu.make_async_remote_copy(
        src_ref=src, dst_ref=dst, send_sem=send, recv_sem=recv, device_id=device, device_id_type=MESH
    )


def contract(left, right, left_dim, right_dim):
    return lax.dot_general(
        left, right, (((left_dim,), (right_dim,)), ((), ())), preferred_element_type=jnp.float32
    )


def kernel(
    factor,
    x_ref,
    c_ref,
    u_ref,
    d_ref,
    gin_ref,
    grad_ref,
    eup_ref,
    edn_ref,
    tok,
    tokt,
    wg,
    wn,
    pre,
    act,
    gpre,
    gbuf,
    sbuf,
    rbuf,
    part_in,
    pair_out,
    pair_in,
    twin_out,
    twin_in,
    outs,
    gin,
    ebuf,
    eup,
    load_s,
    tok_r,
    fwd_r,
    sib_r,
    g_r,
    r_r,
    rep_r,
    pi_r,
    li_r,
    e_r,
    eu_r,
    sent,
    out_s,
):
    rep, fs, tp = lax.axis_index("rep"), lax.axis_index("fs"), lax.axis_index("tp")
    mine = bits_of(fs)
    near = [{"fs": other} for other in partners_of(fs)]
    sibling = {"tp": 1 - tp}
    pair = {"rep": 1 - rep, "fs": partners_of(fs)[0]}
    twin = {"rep": 1 - rep}
    cross = {"rep": 1 - rep, "tp": 1 - tp}
    z, y, x = fs // 16, (fs // 4) % 4, fs % 4
    far_x = {"fs": fs + (x + 2) % 4 - x}
    far_y = {"fs": fs + 4 * ((y + 2) % 4 - y)}
    rows, width = x_ref.shape
    shard = u_ref.shape[0]
    hidden = u_ref.shape[1] // 2
    base = rep * hidden
    weights = (u_ref, d_ref)
    tokens = (x_ref, c_ref)
    pieces = 2
    chunk = rows // pieces
    cuts = (2, 4)
    half_rows = 2 * rows
    bw = 256
    blocks = hidden // bw
    all_parts = range(PARTS)
    f32, bf16 = jnp.float32, jnp.bfloat16

    flip = [(bit, 1 - bit) for bit in mine]
    tables = {}

    def slot(order, s):
        if order not in tables:
            place = {d: 2**k for k, d in enumerate(order)}
            high, low = [], []
            for v in range(8):
                bits = bits_of(4 * v)
                high.append(sum(flip[d][bits[d]] * place[d] for d in (0, 1, 2)))
            for v in range(4):
                bits = bits_of(v)
                low.append(sum(flip[d][bits[d]] * place[d] for d in (3, 4)))
            tables[order] = high, low
        high, low = tables[order]
        return high[s // 4] + low[s % 4]

    def home(m, p):
        return (m * PARTS + p) * 32 * SIZE

    def place_of(m, p):
        return (m * PARTS + p) * 32

    barrier = pltpu.get_barrier_semaphore()
    for device in near + [sibling, pair, twin, cross, far_x, far_y]:
        pl.semaphore_signal(barrier, inc=1, device_id=device, device_id_type=MESH)

    for m in range(2):
        pltpu.make_async_copy(tokens[m], tok.at[m, pl.ds(0, rows)], load_s.at[m]).start()
        for p in all_parts:
            columns = pl.ds(pl.multiple_of(base + p * 128, 128), 128)
            pltpu.make_async_copy(weights[m].at[:, columns], wg.at[place_of(m, p)], load_s.at[2 + m]).start()

    def wait_bytes(ref, sem):
        pltpu.make_async_copy(ref, ref, sem).wait()

    for m in range(2):
        wait_bytes(tok.at[m, pl.ds(0, rows)], load_s.at[m])
        wait_bytes(wg.at[pl.ds(0, PARTS)], load_s.at[2 + m])

    pl.semaphore_wait(barrier, STEPS + 6)

    def start(copy):
        copy.start()
        return copy

    def token_copy(m, q):
        return remote(
            tok.at[m, pl.ds(q * (rows // cuts[m]), rows // cuts[m])],
            tok.at[m, pl.ds(2 * rows + q * (rows // cuts[m]), rows // cuts[m])],
            sent.at[0],
            tok_r.at[m, q],
            pair,
        )

    def forward_copy(m, q):
        return remote(
            tok.at[m, pl.ds(2 * rows + q * (rows // cuts[m]), rows // cuts[m])],
            tok.at[m, pl.ds(3 * rows + q * (rows // cuts[m]), rows // cuts[m])],
            sent.at[1],
            fwd_r.at[m, q],
            sibling,
        )

    def sibling_copy(m):
        return remote(tok.at[m, pl.ds(0, rows)], tok.at[m, pl.ds(rows, rows)], sent.at[2], sib_r.at[m], sibling)

    def gather_copy(m, p, k):
        n = 2**k
        return remote(
            wg.at[pl.ds(place_of(m, p), n)],
            wg.at[pl.ds(place_of(m, p) + n, n)],
            sent.at[3 + m],
            g_r.at[m * PARTS + p, k],
            near[GATHER[m][p][k]],
        )

    def forward(m, q):
        token_copy(m, q).wait_recv()
        start(forward_copy(m, q))

    def transpose(m, g):
        tokt[m, :, g * rows : (g + 1) * rows] = tok[m, g * rows : (g + 1) * rows].T

    def unpack(m, p):
        for s in range(32):
            wn[m, s * shard : (s + 1) * shard, p * 128 : (p + 1) * 128] = wg[
                place_of(m, p) + slot(GATHER[m][p], s)
            ]

    def part_cols(j):
        return slice(j * bw, (j + 1) * bw)

    def forward_block(j):
        for h in range(2):
            part = slice(h * half_rows, (h + 1) * half_rows)
            kept = jnp.maximum(
                jnp.dot(tok[0, part], wn[0, :, part_cols(j)], preferred_element_type=f32), 0.0
            )
            pre[part, part_cols(j)] = kept
            act[part, part_cols(j)] = (kept * kept).astype(bf16)

    def back_block(j):
        for p in (2 * j, 2 * j + 1):
            gather_copy(1, p, STEPS - 1).wait_recv()
            unpack(1, p)
        for h in range(2):
            part = slice(h * half_rows, (h + 1) * half_rows)
            value = jnp.dot(tok[1, part], wn[1, :, part_cols(j)], preferred_element_type=f32)
            gpre[part, part_cols(j)] = (2.0 * pre[part, part_cols(j)] * value).astype(bf16)

    def room(m, p, k):
        before = sum(1 + HALF[i] * SIZE for i in range(k))
        return (m * PARTS + p) * ROOM + before

    def reduce_copy(m, p, k):
        place = pl.ds(room(m, p, k), 1 + HALF[k] * SIZE)
        return remote(
            sbuf.at[place],
            rbuf.at[place],
            sent.at[5],
            r_r.at[m * PARTS + p, k],
            near[REDUCE[m][p][STEPS - 1 - k]],
        )

    def direct_room(m, p, i):
        return room(m, p, HALVINGS) + (i - 1) * (1 + SIZE)

    def direct_copy(m, p, i):
        order = REDUCE[m][p]
        far = far_x if 3 in order[:2] else far_y
        place = pl.ds(direct_room(m, p, i), 1 + SIZE)
        return remote(
            sbuf.at[place],
            rbuf.at[place],
            sent.at[5],
            r_r.at[m * PARTS + p, HALVINGS + i - 1],
            (None, near[order[0]], near[order[1]], far)[i],
        )

    def chunks(count, size):
        step = min(count, 4) * size
        return count * size // step, step

    def highest(m, p, k):
        n = SIZE
        loops, step = chunks(HALF[k], n)
        at = home(m, p) + HALF[k] * n

        def some(i, top):
            return jnp.maximum(top, jnp.max(jnp.abs(gbuf[pl.ds(at + i * step, step)]), axis=0))

        return lax.fori_loop(0, loops, some, jnp.zeros((16, 128), f32))

    def send_sums(m, p, k, top):
        n = SIZE
        loops, step = chunks(HALF[k], n)
        at, to = home(m, p) + HALF[k] * n, room(m, p, k)
        coded = scale_of(top)
        sbuf[to] = coded
        scale = coded.astype(f32)

        def some(i, carry):
            sbuf[pl.ds(to + 1 + i * step, step)] = encode(gbuf[pl.ds(at + i * step, step)], scale)
            return carry

        lax.fori_loop(0, loops, some, 0)
        start(reduce_copy(m, p, k))

    def begin(m, p):
        send_sums(m, p, 0, highest(m, p, 0))

    def add_sums(m, p, k, first, count):
        n = SIZE
        loops, step = chunks(count, n)
        at, got = home(m, p) + first * n, room(m, p, k) + 1 + first * n
        scale = rbuf[room(m, p, k)].astype(f32)

        def some(i, top):
            place = pl.ds(at + i * step, step)
            value = gbuf[place] + decode(rbuf[pl.ds(got + i * step, step)], scale)
            gbuf[place] = value
            return jnp.maximum(top, jnp.max(jnp.abs(value), axis=0))

        return lax.fori_loop(0, loops, some, jnp.zeros((16, 128), f32))

    def reduce_step(m, p, k):
        reduce_copy(m, p, k).wait_recv()
        if k == HALVINGS - 1:
            scale = rbuf[room(m, p, k)].astype(f32)
            for i in (3, 2, 1, 0):
                at = home(m, p) + i * SIZE
                got = room(m, p, k) + 1 + i * SIZE
                value = gbuf[pl.ds(at, SIZE)] + decode(rbuf[pl.ds(got, SIZE)], scale)
                if i == 0:
                    gbuf[pl.ds(at, SIZE)] = value
                    continue
                coded = scale_of(jnp.max(jnp.abs(value), axis=0))
                to = direct_room(m, p, i)
                sbuf[to] = coded
                sbuf[pl.ds(to + 1, SIZE)] = encode(value, coded.astype(f32))
                start(direct_copy(m, p, i))
            return
        n = HALF[k + 1]
        top = add_sums(m, p, k, n, n)
        send_sums(m, p, k + 1, top)
        add_sums(m, p, k, 0, n)

    def weight_grad(m, right, j):
        tall = width // SPLIT
        for i in range(SPLIT):
            out = jnp.dot(
                tokt[m, i * tall : (i + 1) * tall, :], right[:, part_cols(j)], preferred_element_type=f32
            )
            for t in range(tall // shard):
                for e in range(2):
                    p = 2 * j + e
                    at = home(m, p) + slot(REDUCE[m][p], i * (tall // shard) + t) * SIZE
                    value = out[t * shard : (t + 1) * shard, e * 128 : (e + 1) * 128]
                    gbuf[pl.ds(at, SIZE)] = value.reshape(SIZE, 16, 128)
        begin(m, 2 * j)
        begin(m, 2 * j + 1)

    def share_copy(i):
        return remote(
            pre.at[pl.ds((1 + 2 * i) * rows, rows)], part_in.at[i], sent.at[6], pi_r.at[i], sibling
        )

    def pair_copy(q):
        return remote(pair_out.at[q], pair_in.at[q], sent.at[7], li_r.at[q], pair)

    for m in range(2):
        for p in all_parts:
            start(gather_copy(m, p, 0))
        for q in range(cuts[m]):
            start(token_copy(m, q))
    for m in range(2):
        start(sibling_copy(m))

    unpacked = []
    for a in FIRST:
        if a == -1:
            for m in range(2):
                transpose(m, 0)
                sibling_copy(m).wait_recv()
                transpose(m, 1)
        elif a < 0:
            forward((-2 - a) // 2, (-2 - a) % 2)
        else:
            m, p, k = a // 100, a // 10 % 10, a % 10
            gather_copy(m, p, k).wait_recv()
            if k < STEPS - 1:
                start(gather_copy(m, p, k + 1))
                continue
            unpack(m, p)
            if not unpacked:
                for q in range(pieces):
                    forward_copy(0, q).wait_recv()
                transpose(0, 2)
                transpose(0, 3)
            unpacked.append(p)
            if p ^ 1 in unpacked:
                forward_block(p // 2)

    for q in range(cuts[1]):
        forward(1, q)
    transpose(1, 2)
    for q in range(cuts[1]):
        forward_copy(1, q).wait_recv()
    transpose(1, 3)

    order = [a // 10 % 10 for a in THEN if a < 100 and a % 10 == HALVINGS]
    groups = (tuple(all_parts), tuple(order[:6]), tuple(order[6:]))
    spots = (0, 17, 30)

    def twin_copy(g):
        place = pl.ds(spots[g], 1 + len(groups[g]) * SIZE)
        return remote(twin_out.at[place], twin_in.at[place], sent.at[10], rep_r.at[g], twin)

    def twin_send(g):
        m = 1 if g == 0 else 0
        top = jnp.zeros((16, 128), f32)
        for p in groups[g]:
            for i in range(SIZE):
                top = jnp.maximum(top, jnp.abs(outs[m, rep, p * SIZE + i]))
        coded = scale_of(top)
        twin_out[spots[g]] = coded
        scale = coded.astype(f32)
        for n, p in enumerate(groups[g]):
            code = encode(outs[m, rep, pl.ds(p * SIZE, SIZE)], scale)
            twin_out[pl.ds(spots[g] + 1 + n * SIZE, SIZE)] = code
        start(twin_copy(g))
        for n, p in enumerate(groups[g]):
            code = twin_out[pl.ds(spots[g] + 1 + n * SIZE, SIZE)]
            outs[m, rep, pl.ds(p * SIZE, SIZE)] = decode(code, scale)

    def twin_receive(g):
        m = 1 if g == 0 else 0
        twin_copy(g).wait_recv()
        scale = twin_in[spots[g]].astype(f32)
        for n, p in enumerate(groups[g]):
            code = twin_in[pl.ds(spots[g] + 1 + n * SIZE, SIZE)]
            outs[m, 1 - rep, pl.ds(p * SIZE, SIZE)] = decode(code, scale)

    def finish(m, p):
        value = gbuf[pl.ds(home(m, p), SIZE)]
        for i in (1, 2, 3):
            direct_copy(m, p, i).wait_recv()
            to = direct_room(m, p, i)
            value = value + decode(rbuf[pl.ds(to + 1, SIZE)], rbuf[to].astype(f32))
        value = value * factor
        outs[m, rep, pl.ds(p * SIZE, SIZE)] = value
        return value

    def output(i, src, dst):
        copy = pltpu.make_async_copy(src, dst, out_s.at[i])
        copy.start()
        return copy

    rounds = ((near[3], near[4], far_x), (near[1], near[2], far_y), (near[0], twin, pair))

    def energy_copy(k, i):
        return remote(ebuf.at[k, 0], ebuf.at[k, 1 + i], sent.at[8], e_r.at[k, i], rounds[k][i])

    def energy_begin(k):
        for i in range(3):
            start(energy_copy(k, i))

    def energy_step(k):
        for i in range(3):
            energy_copy(k, i).wait_recv()
        ebuf[k + 1, 0] = (ebuf[k, 0] + ebuf[k, 1]) + (ebuf[k, 2] + ebuf[k, 3])
        energy_begin(k + 1)

    squares = [jnp.zeros((16, 128), f32), jnp.zeros((16, 128), f32)]
    left = [PARTS, PARTS]
    outputs = []
    row_copies = []

    def arrived(m, p, k):
        if k < HALVINGS:
            reduce_step(m, p, k)
            return
        value = finish(m, p)
        left[m] -= 1
        if m == 1:
            total = value[0] * value[0] + value[1] * value[1]
            ebuf[0, 0, p : p + 1, :] = jnp.sum(total, axis=0, keepdims=True)
            if left[m] == 0:
                energy_begin(0)
                twin_send(0)
            return
        for row in range(2):
            squares[row] = squares[row] + value[row] * value[row]
        if left[m] == 2:
            twin_send(1)
        if left[m] == 0:
            twin_send(2)
            for row in range(2):
                eup[0, row * 16 : row * 16 + 16] = squares[row]
            for i, device in enumerate((sibling, twin, cross)):
                row_copies.append(start(remote(eup.at[0], eup.at[1 + i], sent.at[9], eu_r.at[i], device)))

    def inputs_grad(i):
        part = slice(i * half_rows, (i + 1) * half_rows)
        for n in range(width // bw):
            pre[part, n * bw : (n + 1) * bw] = contract(
                gpre[part, :], wn[0, n * bw : (n + 1) * bw, :], 1, 1
            )
        start(share_copy(i))

    def share_arrived(i):
        share_copy(i).wait_recv()
        if i == 0:
            pre[0:rows] = pre[0:rows] + part_in[0]
            return
        for q in range(pieces):
            s = slice(q * chunk, (q + 1) * chunk)
            value = pre[2 * rows + q * chunk : 2 * rows + (q + 1) * chunk] + part_in[1, s]
            coded = scale_of(jnp.max(jnp.abs(value), axis=0, keepdims=True))
            pair_out[q, 0:16] = jnp.broadcast_to(coded, (16, width))
            pair_out[q, 16 : 16 + chunk] = encode(value, coded.astype(f32))
            start(pair_copy(q))

    def pair_arrived(q):
        pair_copy(q).wait_recv()
        s = slice(q * chunk, (q + 1) * chunk)
        scale = pair_in[q, 0:16].astype(f32)[0:1]
        gin[s] = (pre[s] + decode(pair_in[q, 16 : 16 + chunk], scale)).astype(bf16)
        if q == pieces - 1:
            outputs.append(output(0, gin, gin_ref))

    def energy_end():
        for i in range(3):
            energy_copy(2, i).wait_recv()
        ebuf[3, 0] = (ebuf[2, 0] + ebuf[2, 1]) * (1.0 / width)
        ebuf[3, 1] = (ebuf[2, 2] + ebuf[2, 3]) * (1.0 / width)
        outputs.append(output(2, ebuf.at[3, 0], edn_ref.at[rep]))
        outputs.append(output(3, ebuf.at[3, 1], edn_ref.at[1 - rep]))

    def twins_arrived(m):
        for g in (0,) if m == 1 else (1, 2):
            twin_receive(g)
        outputs.append(output(4 if m == 0 else 1, outs.at[m], grad_ref.at[m]))

    def run(a):
        if a < 200:
            arrived(a // 100, a // 10 % 10, a % 10)
        elif a < 1100:
            m, j = (a - 1000) // 10, a % 10
            weight_grad(m, (gpre, act)[m], j)
        elif a < 1200:
            back_block(a - 1100)
        elif a < 1300:
            inputs_grad(a - 1200)
        elif a < 1310:
            share_arrived(a - 1300)
        elif a < 1400:
            pair_arrived(a - 1310)
        elif a < 1402:
            energy_step(a - 1400)
        elif a == 1402:
            energy_end()
        else:
            twins_arrived(1)

    for a in THEN[:-3]:
        run(a)
    twins_arrived(0)
    for a in THEN[-3:]:
        run(a)
    for copy in row_copies:
        copy.wait_recv()
    outputs.append(output(5, eup, eup_ref))
    wait_bytes(tok.at[:, pl.ds(0, rows)], sent.at[0])
    wait_bytes(tok.at[:, pl.ds(0, rows)], sent.at[1])
    wait_bytes(tok.at[:, pl.ds(0, rows)], sent.at[2])
    for m in range(2):
        wait_bytes(wg.at[pl.ds(0, 31 * PARTS)], sent.at[3 + m])
    wait_bytes(sbuf, sent.at[5])
    wait_bytes(part_in, sent.at[6])
    wait_bytes(pair_out, sent.at[7])
    wait_bytes(ebuf.at[pl.ds(0, 3), pl.ds(0, 3)], sent.at[8])
    wait_bytes(eup.at[pl.ds(0, 3)], sent.at[9])
    wait_bytes(twin_out, sent.at[10])
    for copy in outputs:
        copy.wait()


def layout(
    gin_ref, grad_ref, eup_ref, edn_ref, gin_out, gup_out, gdn_out, eup_out, edn_out,
    gin, grad, eup, edn, both, row, in_s, out_s,
):
    pairs = ((gin_ref, gin), (grad_ref.at[1], grad.at[1]), (grad_ref.at[0], grad.at[0]), (eup_ref, eup), (edn_ref, edn))
    loads = [pltpu.make_async_copy(a, b, in_s.at[i]) for i, (a, b) in enumerate(pairs)]
    for copy in loads:
        copy.start()
    stores = []

    def store(i, src, dst):
        copy = pltpu.make_async_copy(src, dst, out_s.at[i])
        copy.start()
        stores.append(copy)

    half = gup_out.shape[1] // 2
    loads[3].wait()
    total = (eup[0] + eup[1]) + (eup[2] + eup[3])
    row[...] = jnp.sum(total.T, axis=0) * (1.0 / (4 * half))
    loads[4].wait()
    store(3, row, eup_out)
    store(4, edn, edn_out)
    loads[0].wait()
    store(0, gin, gin_out)
    for m, load, out in ((1, 1, gdn_out), (0, 2, gup_out)):
        loads[load].wait()
        for r in range(2):
            for u in range(UNITS):
                block, top = divmod(u, 2)
                left = r * half + block * 128
                both[m, top * 16 : top * 16 + 16, left : left + 128] = grad[m, r, u]
        store(load, both.at[m], out)
    for copy in stores:
        copy.wait()


def body(inputs, up_proj, down_proj, out_cotangent):
    rows, width = inputs.shape
    shard, both = up_proj.shape
    hidden = both // 2
    factor = float(rows * lax.axis_size("rep") * lax.axis_size("fs") * lax.axis_size("tp")) ** (-0.5)
    f32, bf16 = jnp.float32, jnp.bfloat16
    shape = jax.ShapeDtypeStruct
    dma = pltpu.SemaphoreType.DMA
    messages = 2 * PARTS * ROOM
    anywhere = pl.BlockSpec(memory_space=pl.ANY)
    raw = pl.pallas_call(
        functools.partial(kernel, factor),
        out_shape=(
            shape((rows, width), bf16),
            shape((2, 2, UNITS, 16, 128), f32),
            shape((4, shard, 128), f32),
            shape((2, BLOCKS, 128), f32),
        ),
        in_specs=[anywhere] * 4,
        out_specs=(anywhere,) * 4,
        scratch_shapes=[
            pltpu.VMEM((2, 4 * rows, width), bf16),
            pltpu.VMEM((2, width, 4 * rows), bf16),
            pltpu.VMEM((2 * PARTS * 32, shard, 128), bf16),
            pltpu.VMEM((2, width, hidden), bf16),
            pltpu.VMEM((4 * rows, max(hidden, width)), f32),
            pltpu.VMEM((4 * rows, hidden), bf16),
            pltpu.VMEM((4 * rows, hidden), bf16),
            pltpu.VMEM((2 * 32 * UNITS, 16, 128), f32),
            pltpu.VMEM((messages, 16, 128), bf16),
            pltpu.VMEM((messages, 16, 128), bf16),
            pltpu.VMEM((2, rows, width), f32),
            pltpu.VMEM((2, 16 + rows // 2, width), bf16),
            pltpu.VMEM((2, 16 + rows // 2, width), bf16),
            pltpu.VMEM((35, 16, 128), bf16),
            pltpu.VMEM((35, 16, 128), bf16),
            pltpu.VMEM((2, 2, UNITS, 16, 128), f32),
            pltpu.VMEM((rows, width), bf16),
            pltpu.VMEM((4, 4, BLOCKS, 128), f32),
            pltpu.VMEM((4, shard, 128), f32),
            dma((4,)),
            dma((2, 4)),
            dma((2, 4)),
            dma((2,)),
            dma((2 * PARTS, STEPS)),
            dma((2 * PARTS, 6)),
            dma((3,)),
            dma((2,)),
            dma((2,)),
            dma((3, 3)),
            dma((3,)),
            dma((11,)),
            dma((6,)),
        ],
        compiler_params=pltpu.CompilerParams(
            collective_id=0, has_side_effects=True, vmem_limit_bytes=60 * 2**20
        ),
        name="step",
    )(inputs, out_cotangent, up_proj, down_proj.T)
    gin, gup, gdn, eup, edn = pl.pallas_call(
        layout,
        out_shape=(
            shape((rows, width), bf16),
            shape((shard, both), f32),
            shape((shard, both), f32),
            shape((shard,), f32),
            shape((2, BLOCKS, 128), f32),
        ),
        in_specs=[anywhere] * 4,
        out_specs=(anywhere,) * 5,
        scratch_shapes=[
            pltpu.VMEM((rows, width), bf16),
            pltpu.VMEM((2, 2, UNITS, 16, 128), f32),
            pltpu.VMEM((4, shard, 128), f32),
            pltpu.VMEM((2, BLOCKS, 128), f32),
            pltpu.VMEM((2, shard, both), f32),
            pltpu.VMEM((shard,), f32),
            dma((5,)),
            dma((5,)),
        ],
        name="layout",
    )(*raw)
    return gin, gup, gdn.T, eup, edn.reshape((both,))


def solution(mesh):
    return jax.shard_map(
        body,
        mesh=mesh,
        in_specs=(
            P(("rep", "fs", "tp"), None),
            P("fs", "tp"),
            P("tp", "fs"),
            P(("rep", "fs", "tp"), None),
        ),
        out_specs=(P(("rep", "fs", "tp"), None), P("fs", "tp"), P("tp", "fs"), P("fs"), P("tp")),
        check_vma=False,
    )
```

```python
import functools

import jax
import jax.numpy as jnp
from jax import lax
from jax.experimental import pallas as pl
from jax.experimental.pallas import tpu as pltpu
from jax.sharding import PartitionSpec as P

MESH = pl.DeviceIdType.MESH
GATHER = (
    (
        (2, 4, 0, 1, 3),
        (0, 3, 1, 2, 4),
        (1, 4, 0, 2, 3),
        (2, 3, 1, 0, 4),
        (4, 0, 2, 3, 1),
        (4, 3, 0, 1, 2),
        (1, 2, 3, 4, 0),
        (3, 1, 4, 0, 2),
    ),
    (
        (0, 4, 1, 3, 2),
        (3, 2, 0, 1, 4),
        (2, 4, 3, 1, 0),
        (1, 3, 2, 0, 4),
        (0, 1, 2, 4, 3),
        (2, 4, 3, 1, 0),
        (2, 1, 4, 0, 3),
        (3, 0, 4, 2, 1),
    ),
)
REDUCE = (
    (
        (3, 4, 2, 0, 1),
        (4, 3, 0, 1, 2),
        (1, 2, 0, 4, 3),
        (2, 1, 0, 4, 3),
        (3, 4, 0, 2, 1),
        (3, 4, 2, 1, 0),
        (2, 1, 0, 3, 4),
        (3, 4, 1, 0, 2),
    ),
    (
        (1, 2, 0, 4, 3),
        (4, 3, 1, 0, 2),
        (1, 2, 4, 3, 0),
        (4, 3, 2, 0, 1),
        (2, 1, 0, 4, 3),
        (4, 3, 0, 2, 1),
        (1, 2, 3, 0, 4),
        (2, 1, 3, 4, 0),
    ),
)
FIRST = (
    0, 10, 20, 40, 70, 30, 50, 60, 100, 110, 120, 130, 140, 170, 150, 160,
    1, 11, 41, 71, 61, 21, 31, 51, 101, 111, 141, 161, 171, 121, 131,
    151, 2, 12, 42, 72, 62, 22, 32, 52, 102, 122, 142, 132, -2, 162, 172,
    152, 112, 3, 13, 43, 63, 73, 53, 23, 33, 103, 143, 123, 173, 133, -3, -1,
    153, 163, 4, 14, 113, 74, 64, 24, 34, 44, 54,
)
THEN = (
    1010, 1011, 1012, 1013, 1100, 1101, 1102, 100, 110, 1103, 120, 130, 1000, 140, 160, 1001,
    170, 150, 101, 1002, 111, 121, 1003, 131, 141, 1201, 0, 161, 10, 171, 102, 1200,
    122, 20, 151, 40, 1301, 50, 112, 60, 30, 70, 142, 162, 1300, 132, 11, 172,
    1, 103, 152, 21, 123, 41, 51, 113, 31, 61, 71, 143, 163, 12, 133, 173,
    2, 22, 153, 42, 52, 32, 72, 62, 13, 3, 1400, 23, 43, 1500, 53, 33,
    73, 63, 1401, 1402, 1310, 1311,
)
STEPS = 5
PARTS = 8
SPLIT = 2
SIZE = 2
UNITS = 16
BLOCKS = 8
HALF = (16, 8, 4)
HALVINGS = 3
ROOM = 68
SPAN = 240.0
SHIFT = 120.0


def encode(value, scale):
    code = jnp.exp2(jnp.abs(value) * (SPAN / scale) - SHIFT)
    return jnp.where(value < 0.0, -code, code).astype(jnp.bfloat16)


def decode(code, scale):
    code = code.astype(jnp.float32)
    size = (jnp.log2(jnp.abs(code)) + SHIFT) * (scale * (1.0 / SPAN))
    return jnp.where(code < 0.0, -size, size)


def scale_of(top):
    return (top * 1.01 + 1e-35).astype(jnp.bfloat16)


def bits_of(fs):
    z, y, x = fs // 16, (fs // 4) % 4, fs % 4
    return (z, (y % 2 + y // 2) % 2, y // 2, (x % 2 + x // 2) % 2, x // 2)


def partners_of(fs):
    z, y, x = fs // 16, (fs // 4) % 4, fs % 4
    return (
        fs + 16 - 32 * z,
        fs + 4 - 8 * (y % 2),
        fs + 12 - 8 * y,
        fs + 1 - 2 * (x % 2),
        fs + 3 - 2 * x,
    )


def remote(src, dst, send, recv, device):
    return pltpu.make_async_remote_copy(
        src_ref=src, dst_ref=dst, send_sem=send, recv_sem=recv, device_id=device, device_id_type=MESH
    )


def contract(left, right, left_dim, right_dim):
    return lax.dot_general(
        left, right, (((left_dim,), (right_dim,)), ((), ())), preferred_element_type=jnp.float32
    )


def kernel(
    factor,
    x_ref,
    c_ref,
    u_ref,
    d_ref,
    gin_ref,
    grad_ref,
    eup_ref,
    edn_ref,
    tok,
    tokt,
    wg,
    wn,
    pre,
    act,
    gpre,
    gbuf,
    sbuf,
    rbuf,
    part_in,
    pair_out,
    pair_in,
    twin_out,
    twin_in,
    outs,
    gin,
    ebuf,
    eup,
    load_s,
    tok_r,
    fwd_r,
    sib_r,
    g_r,
    r_r,
    rep_r,
    pi_r,
    li_r,
    e_r,
    eu_r,
    sent,
    out_s,
):
    rep, fs, tp = lax.axis_index("rep"), lax.axis_index("fs"), lax.axis_index("tp")
    mine = bits_of(fs)
    near = [{"fs": other} for other in partners_of(fs)]
    sibling = {"tp": 1 - tp}
    pair = {"rep": 1 - rep, "fs": partners_of(fs)[0]}
    twin = {"rep": 1 - rep}
    cross = {"rep": 1 - rep, "tp": 1 - tp}
    z, y, x = fs // 16, (fs // 4) % 4, fs % 4
    far_x = {"fs": fs + (x + 2) % 4 - x}
    far_y = {"fs": fs + 4 * ((y + 2) % 4 - y)}
    rows, width = x_ref.shape
    shard = u_ref.shape[0]
    hidden = u_ref.shape[1] // 2
    base = rep * hidden
    weights = (u_ref, d_ref)
    tokens = (x_ref, c_ref)
    pieces = 2
    chunk = rows // pieces
    cuts = (2, 4)
    half_rows = 2 * rows
    bw = 256
    blocks = hidden // bw
    all_parts = range(PARTS)
    f32, bf16 = jnp.float32, jnp.bfloat16

    flip = [(bit, 1 - bit) for bit in mine]
    tables = {}

    def slot(order, s):
        if order not in tables:
            place = {d: 2**k for k, d in enumerate(order)}
            high, low = [], []
            for v in range(8):
                bits = bits_of(4 * v)
                high.append(sum(flip[d][bits[d]] * place[d] for d in (0, 1, 2)))
            for v in range(4):
                bits = bits_of(v)
                low.append(sum(flip[d][bits[d]] * place[d] for d in (3, 4)))
            tables[order] = high, low
        high, low = tables[order]
        return high[s // 4] + low[s % 4]

    def home(m, p):
        return (m * PARTS + p) * 32 * SIZE

    def place_of(m, p):
        return (m * PARTS + p) * 32

    barrier = pltpu.get_barrier_semaphore()
    for device in near + [sibling, pair, twin, cross, far_x, far_y]:
        pl.semaphore_signal(barrier, inc=1, device_id=device, device_id_type=MESH)

    for m in range(2):
        pltpu.make_async_copy(tokens[m], tok.at[m, pl.ds(0, rows)], load_s.at[m]).start()
        for p in all_parts:
            columns = pl.ds(pl.multiple_of(base + p * 128, 128), 128)
            pltpu.make_async_copy(weights[m].at[:, columns], wg.at[place_of(m, p)], load_s.at[2 + m]).start()

    def wait_bytes(ref, sem):
        pltpu.make_async_copy(ref, ref, sem).wait()

    for m in range(2):
        wait_bytes(tok.at[m, pl.ds(0, rows)], load_s.at[m])
        wait_bytes(wg.at[pl.ds(0, PARTS)], load_s.at[2 + m])

    pl.semaphore_wait(barrier, STEPS + 6)

    def start(copy):
        copy.start()
        return copy

    def token_copy(m, q):
        return remote(
            tok.at[m, pl.ds(q * (rows // cuts[m]), rows // cuts[m])],
            tok.at[m, pl.ds(2 * rows + q * (rows // cuts[m]), rows // cuts[m])],
            sent.at[0],
            tok_r.at[m, q],
            pair,
        )

    def forward_copy(m, q):
        return remote(
            tok.at[m, pl.ds(2 * rows + q * (rows // cuts[m]), rows // cuts[m])],
            tok.at[m, pl.ds(3 * rows + q * (rows // cuts[m]), rows // cuts[m])],
            sent.at[1],
            fwd_r.at[m, q],
            sibling,
        )

    def sibling_copy(m):
        return remote(tok.at[m, pl.ds(0, rows)], tok.at[m, pl.ds(rows, rows)], sent.at[2], sib_r.at[m], sibling)

    def gather_copy(m, p, k):
        n = 2**k
        return remote(
            wg.at[pl.ds(place_of(m, p), n)],
            wg.at[pl.ds(place_of(m, p) + n, n)],
            sent.at[3 + m],
            g_r.at[m * PARTS + p, k],
            near[GATHER[m][p][k]],
        )

    def forward(m, q):
        token_copy(m, q).wait_recv()
        start(forward_copy(m, q))

    def transpose(m, g):
        tokt[m, :, g * rows : (g + 1) * rows] = tok[m, g * rows : (g + 1) * rows].T

    def unpack(m, p):
        for s in range(32):
            wn[m, s * shard : (s + 1) * shard, p * 128 : (p + 1) * 128] = wg[
                place_of(m, p) + slot(GATHER[m][p], s)
            ]

    def part_cols(j):
        return slice(j * bw, (j + 1) * bw)

    def forward_block(j):
        for h in range(2):
            part = slice(h * half_rows, (h + 1) * half_rows)
            kept = jnp.maximum(
                jnp.dot(tok[0, part], wn[0, :, part_cols(j)], preferred_element_type=f32), 0.0
            )
            pre[part, part_cols(j)] = kept
            act[part, part_cols(j)] = (kept * kept).astype(bf16)

    def back_block(j):
        for p in (2 * j, 2 * j + 1):
            gather_copy(1, p, STEPS - 1).wait_recv()
            unpack(1, p)
        for h in range(2):
            part = slice(h * half_rows, (h + 1) * half_rows)
            value = jnp.dot(tok[1, part], wn[1, :, part_cols(j)], preferred_element_type=f32)
            gpre[part, part_cols(j)] = (2.0 * pre[part, part_cols(j)] * value).astype(bf16)

    def room(m, p, k):
        before = sum(1 + HALF[i] * SIZE for i in range(k))
        return (m * PARTS + p) * ROOM + before

    def reduce_copy(m, p, k):
        place = pl.ds(room(m, p, k), 1 + HALF[k] * SIZE)
        return remote(
            sbuf.at[place],
            rbuf.at[place],
            sent.at[5],
            r_r.at[m * PARTS + p, k],
            near[REDUCE[m][p][STEPS - 1 - k]],
        )

    def direct_room(m, p, i):
        return room(m, p, HALVINGS) + (i - 1) * (1 + SIZE)

    def direct_copy(m, p, i):
        order = REDUCE[m][p]
        far = far_x if 3 in order[:2] else far_y
        place = pl.ds(direct_room(m, p, i), 1 + SIZE)
        return remote(
            sbuf.at[place],
            rbuf.at[place],
            sent.at[5],
            r_r.at[m * PARTS + p, HALVINGS],
            (None, near[order[0]], near[order[1]], far)[i],
        )

    def chunks(count, size):
        step = min(count, 8) * size
        return count * size // step, step

    def highest(m, p, k):
        n = SIZE
        loops, step = chunks(HALF[k], n)
        at = home(m, p) + HALF[k] * n

        def some(i, top):
            return jnp.maximum(top, jnp.max(jnp.abs(gbuf[pl.ds(at + i * step, step)]), axis=0))

        return lax.fori_loop(0, loops, some, jnp.zeros((16, 128), f32))

    def send_sums(m, p, k, top):
        n = SIZE
        loops, step = chunks(HALF[k], n)
        at, to = home(m, p) + HALF[k] * n, room(m, p, k)
        coded = scale_of(top)
        sbuf[to] = coded
        scale = coded.astype(f32)

        def some(i, carry):
            sbuf[pl.ds(to + 1 + i * step, step)] = encode(gbuf[pl.ds(at + i * step, step)], scale)
            return carry

        lax.fori_loop(0, loops, some, 0)
        start(reduce_copy(m, p, k))

    def begin(m, p):
        send_sums(m, p, 0, highest(m, p, 0))

    def add_sums(m, p, k, first, count):
        n = SIZE
        loops, step = chunks(count, n)
        at, got = home(m, p) + first * n, room(m, p, k) + 1 + first * n
        scale = rbuf[room(m, p, k)].astype(f32)

        def some(i, top):
            place = pl.ds(at + i * step, step)
            value = gbuf[place] + decode(rbuf[pl.ds(got + i * step, step)], scale)
            gbuf[place] = value
            return jnp.maximum(top, jnp.max(jnp.abs(value), axis=0))

        return lax.fori_loop(0, loops, some, jnp.zeros((16, 128), f32))

    def reduce_step(m, p, k):
        reduce_copy(m, p, k).wait_recv()
        if k == HALVINGS - 1:
            scale = rbuf[room(m, p, k)].astype(f32)
            for i in (3, 2, 1, 0):
                at = home(m, p) + i * SIZE
                got = room(m, p, k) + 1 + i * SIZE
                value = gbuf[pl.ds(at, SIZE)] + decode(rbuf[pl.ds(got, SIZE)], scale)
                if i == 0:
                    gbuf[pl.ds(at, SIZE)] = value
                    continue
                coded = scale_of(jnp.max(jnp.abs(value), axis=0))
                to = direct_room(m, p, i)
                sbuf[to] = coded
                sbuf[pl.ds(to + 1, SIZE)] = encode(value, coded.astype(f32))
                start(direct_copy(m, p, i))
            return
        n = HALF[k + 1]
        top = add_sums(m, p, k, n, n)
        send_sums(m, p, k + 1, top)
        add_sums(m, p, k, 0, n)

    def weight_grad(m, right, j):
        tall = width // SPLIT
        for i in range(SPLIT):
            out = jnp.dot(
                tokt[m, i * tall : (i + 1) * tall, :], right[:, part_cols(j)], preferred_element_type=f32
            )
            for t in range(tall // shard):
                for e in range(2):
                    p = 2 * j + e
                    at = home(m, p) + slot(REDUCE[m][p], i * (tall // shard) + t) * SIZE
                    value = out[t * shard : (t + 1) * shard, e * 128 : (e + 1) * 128]
                    gbuf[pl.ds(at, SIZE)] = value.reshape(SIZE, 16, 128)
        begin(m, 2 * j)
        begin(m, 2 * j + 1)

    def share_copy(i):
        return remote(
            pre.at[pl.ds((1 + 2 * i) * rows, rows)], part_in.at[i], sent.at[6], pi_r.at[i], sibling
        )

    def pair_copy(q):
        return remote(pair_out.at[q], pair_in.at[q], sent.at[7], li_r.at[q], pair)

    for m in range(2):
        for p in all_parts:
            start(gather_copy(m, p, 0))
        for q in range(cuts[m]):
            start(token_copy(m, q))
    for m in range(2):
        start(sibling_copy(m))

    unpacked = []
    for a in FIRST:
        if a == -1:
            for m in range(2):
                transpose(m, 0)
                sibling_copy(m).wait_recv()
                transpose(m, 1)
        elif a < 0:
            forward((-2 - a) // 2, (-2 - a) % 2)
        else:
            m, p, k = a // 100, a // 10 % 10, a % 10
            gather_copy(m, p, k).wait_recv()
            if k < STEPS - 1:
                start(gather_copy(m, p, k + 1))
                continue
            unpack(m, p)
            if not unpacked:
                for q in range(pieces):
                    forward_copy(0, q).wait_recv()
                transpose(0, 2)
                transpose(0, 3)
            unpacked.append(p)
            if p ^ 1 in unpacked:
                forward_block(p // 2)

    for q in range(cuts[1]):
        forward(1, q)
    transpose(1, 2)
    for q in range(cuts[1]):
        forward_copy(1, q).wait_recv()
    transpose(1, 3)

    order = [a // 10 % 10 for a in THEN if a < 100 and a % 10 == HALVINGS]
    groups = (tuple(all_parts), tuple(order[:6]), tuple(order[6:]))
    spots = (0, 17, 30)

    def twin_copy(g):
        place = pl.ds(spots[g], 1 + len(groups[g]) * SIZE)
        return remote(twin_out.at[place], twin_in.at[place], sent.at[10], rep_r.at[g], twin)

    def twin_send(g):
        m = 1 if g == 0 else 0
        top = jnp.zeros((16, 128), f32)
        for p in groups[g]:
            for i in range(SIZE):
                top = jnp.maximum(top, jnp.abs(outs[m, rep, p * SIZE + i]))
        coded = scale_of(top)
        twin_out[spots[g]] = coded
        scale = coded.astype(f32)
        for n, p in enumerate(groups[g]):
            code = encode(outs[m, rep, pl.ds(p * SIZE, SIZE)], scale)
            twin_out[pl.ds(spots[g] + 1 + n * SIZE, SIZE)] = code
        start(twin_copy(g))
        for n, p in enumerate(groups[g]):
            code = twin_out[pl.ds(spots[g] + 1 + n * SIZE, SIZE)]
            outs[m, rep, pl.ds(p * SIZE, SIZE)] = decode(code, scale)

    def twin_receive(g):
        m = 1 if g == 0 else 0
        twin_copy(g).wait_recv()
        scale = twin_in[spots[g]].astype(f32)
        for n, p in enumerate(groups[g]):
            code = twin_in[pl.ds(spots[g] + 1 + n * SIZE, SIZE)]
            outs[m, 1 - rep, pl.ds(p * SIZE, SIZE)] = decode(code, scale)

    def finish(m, p):
        value = gbuf[pl.ds(home(m, p), SIZE)]
        wait_bytes(rbuf.at[pl.ds(direct_room(m, p, 1), 3 * (1 + SIZE))], r_r.at[m * PARTS + p, HALVINGS])
        for i in (1, 2, 3):
            to = direct_room(m, p, i)
            value = value + decode(rbuf[pl.ds(to + 1, SIZE)], rbuf[to].astype(f32))
        value = value * factor
        outs[m, rep, pl.ds(p * SIZE, SIZE)] = value
        return value

    def output(i, src, dst):
        copy = pltpu.make_async_copy(src, dst, out_s.at[i])
        copy.start()
        return copy

    rounds = ((near[3], near[4], far_x), (near[1], near[2], far_y), (near[0], twin, pair))

    def energy_copy(k, i):
        return remote(ebuf.at[k, 0], ebuf.at[k, 1 + i], sent.at[8], e_r.at[k], rounds[k][i])

    def energy_begin(k):
        for i in range(3):
            start(energy_copy(k, i))

    def energy_step(k):
        wait_bytes(ebuf.at[k, pl.ds(1, 3)], e_r.at[k])
        ebuf[k + 1, 0] = (ebuf[k, 0] + ebuf[k, 1]) + (ebuf[k, 2] + ebuf[k, 3])
        energy_begin(k + 1)

    squares = [jnp.zeros((16, 128), f32), jnp.zeros((16, 128), f32)]
    left = [PARTS, PARTS]
    outputs = []
    row_copies = []

    def arrived(m, p, k):
        if k < HALVINGS:
            reduce_step(m, p, k)
            return
        value = finish(m, p)
        left[m] -= 1
        if m == 1:
            total = value[0] * value[0] + value[1] * value[1]
            ebuf[0, 0, p : p + 1, :] = jnp.sum(total, axis=0, keepdims=True)
            if left[m] == 0:
                energy_begin(0)
                twin_send(0)
            return
        for row in range(2):
            squares[row] = squares[row] + value[row] * value[row]
        if left[m] == 2:
            twin_send(1)
        if left[m] == 0:
            twin_send(2)
            for row in range(2):
                eup[0, row * 16 : row * 16 + 16] = squares[row]
            for i, device in enumerate((sibling, twin, cross)):
                row_copies.append(start(remote(eup.at[0], eup.at[1 + i], sent.at[9], eu_r.at[0], device)))

    def inputs_grad(i):
        part = slice(i * half_rows, (i + 1) * half_rows)
        for n in range(width // bw):
            pre[part, n * bw : (n + 1) * bw] = contract(
                gpre[part, :], wn[0, n * bw : (n + 1) * bw, :], 1, 1
            )
        start(share_copy(i))

    def share_arrived(i):
        share_copy(i).wait_recv()
        if i == 0:
            pre[0:rows] = pre[0:rows] + part_in[0]
            return
        for q in range(pieces):
            s = slice(q * chunk, (q + 1) * chunk)
            value = pre[2 * rows + q * chunk : 2 * rows + (q + 1) * chunk] + part_in[1, s]
            coded = scale_of(jnp.max(jnp.abs(value), axis=0, keepdims=True))
            pair_out[q, 0:16] = jnp.broadcast_to(coded, (16, width))
            pair_out[q, 16 : 16 + chunk] = encode(value, coded.astype(f32))
            start(pair_copy(q))

    def pair_arrived(q):
        pair_copy(q).wait_recv()
        s = slice(q * chunk, (q + 1) * chunk)
        scale = pair_in[q, 0:16].astype(f32)[0:1]
        gin[s] = (pre[s] + decode(pair_in[q, 16 : 16 + chunk], scale)).astype(bf16)
        if q == pieces - 1:
            outputs.append(output(0, gin, gin_ref))

    def energy_end():
        wait_bytes(ebuf.at[2, pl.ds(1, 3)], e_r.at[2])
        ebuf[3, 0] = (ebuf[2, 0] + ebuf[2, 1]) * (1.0 / width)
        ebuf[3, 1] = (ebuf[2, 2] + ebuf[2, 3]) * (1.0 / width)
        outputs.append(output(2, ebuf.at[3, 0], edn_ref.at[rep]))
        outputs.append(output(3, ebuf.at[3, 1], edn_ref.at[1 - rep]))

    def twins_arrived(m):
        for g in (0,) if m == 1 else (1, 2):
            twin_receive(g)
        outputs.append(output(4 if m == 0 else 1, outs.at[m], grad_ref.at[m]))

    def run(a):
        if a < 200:
            arrived(a // 100, a // 10 % 10, a % 10)
        elif a < 1100:
            m, j = (a - 1000) // 10, a % 10
            weight_grad(m, (gpre, act)[m], j)
        elif a < 1200:
            back_block(a - 1100)
        elif a < 1300:
            inputs_grad(a - 1200)
        elif a < 1310:
            share_arrived(a - 1300)
        elif a < 1400:
            pair_arrived(a - 1310)
        elif a < 1402:
            energy_step(a - 1400)
        elif a == 1402:
            energy_end()
        else:
            twins_arrived(1)

    for a in THEN[:-3]:
        run(a)
    twins_arrived(0)
    for a in THEN[-3:]:
        run(a)
    wait_bytes(eup.at[pl.ds(1, 3)], eu_r.at[0])
    outputs.append(output(5, eup, eup_ref))
    wait_bytes(tok.at[:, pl.ds(0, rows)], sent.at[0])
    wait_bytes(tok.at[:, pl.ds(0, rows)], sent.at[1])
    wait_bytes(tok.at[:, pl.ds(0, rows)], sent.at[2])
    for m in range(2):
        wait_bytes(wg.at[pl.ds(0, 31 * PARTS)], sent.at[3 + m])
    wait_bytes(sbuf, sent.at[5])
    wait_bytes(part_in, sent.at[6])
    wait_bytes(pair_out, sent.at[7])
    wait_bytes(ebuf.at[pl.ds(0, 3), pl.ds(0, 3)], sent.at[8])
    wait_bytes(eup.at[pl.ds(0, 3)], sent.at[9])
    wait_bytes(twin_out, sent.at[10])
    for copy in outputs:
        copy.wait()


def layout(
    gin_ref, grad_ref, eup_ref, edn_ref, gin_out, gup_out, gdn_out, eup_out, edn_out,
    gin, grad, eup, edn, both, row, in_s, out_s,
):
    pairs = ((gin_ref, gin), (grad_ref.at[1], grad.at[1]), (grad_ref.at[0], grad.at[0]), (eup_ref, eup), (edn_ref, edn))
    loads = [pltpu.make_async_copy(a, b, in_s.at[i]) for i, (a, b) in enumerate(pairs)]
    for copy in loads:
        copy.start()
    stores = []

    def store(i, src, dst):
        copy = pltpu.make_async_copy(src, dst, out_s.at[i])
        copy.start()
        stores.append(copy)

    half = gup_out.shape[1] // 2
    loads[3].wait()
    total = (eup[0] + eup[1]) + (eup[2] + eup[3])
    row[...] = jnp.sum(total.T, axis=0) * (1.0 / (4 * half))
    loads[4].wait()
    store(3, row, eup_out)
    store(4, edn, edn_out)
    loads[0].wait()
    store(0, gin, gin_out)
    for m, load, out in ((1, 1, gdn_out), (0, 2, gup_out)):
        loads[load].wait()
        for r in range(2):
            for u in range(UNITS):
                block, top = divmod(u, 2)
                left = r * half + block * 128
                both[m, top * 16 : top * 16 + 16, left : left + 128] = grad[m, r, u]
        store(load, both.at[m], out)
    for copy in stores:
        copy.wait()


def body(inputs, up_proj, down_proj, out_cotangent):
    rows, width = inputs.shape
    shard, both = up_proj.shape
    hidden = both // 2
    factor = float(rows * lax.axis_size("rep") * lax.axis_size("fs") * lax.axis_size("tp")) ** (-0.5)
    f32, bf16 = jnp.float32, jnp.bfloat16
    shape = jax.ShapeDtypeStruct
    dma = pltpu.SemaphoreType.DMA
    messages = 2 * PARTS * ROOM
    anywhere = pl.BlockSpec(memory_space=pl.ANY)
    raw = pl.pallas_call(
        functools.partial(kernel, factor),
        out_shape=(
            shape((rows, width), bf16),
            shape((2, 2, UNITS, 16, 128), f32),
            shape((4, shard, 128), f32),
            shape((2, BLOCKS, 128), f32),
        ),
        in_specs=[anywhere] * 4,
        out_specs=(anywhere,) * 4,
        scratch_shapes=[
            pltpu.VMEM((2, 4 * rows, width), bf16),
            pltpu.VMEM((2, width, 4 * rows), bf16),
            pltpu.VMEM((2 * PARTS * 32, shard, 128), bf16),
            pltpu.VMEM((2, width, hidden), bf16),
            pltpu.VMEM((4 * rows, max(hidden, width)), f32),
            pltpu.VMEM((4 * rows, hidden), bf16),
            pltpu.VMEM((4 * rows, hidden), bf16),
            pltpu.VMEM((2 * 32 * UNITS, 16, 128), f32),
            pltpu.VMEM((messages, 16, 128), bf16),
            pltpu.VMEM((messages, 16, 128), bf16),
            pltpu.VMEM((2, rows, width), f32),
            pltpu.VMEM((2, 16 + rows // 2, width), bf16),
            pltpu.VMEM((2, 16 + rows // 2, width), bf16),
            pltpu.VMEM((35, 16, 128), bf16),
            pltpu.VMEM((35, 16, 128), bf16),
            pltpu.VMEM((2, 2, UNITS, 16, 128), f32),
            pltpu.VMEM((rows, width), bf16),
            pltpu.VMEM((4, 4, BLOCKS, 128), f32),
            pltpu.VMEM((4, shard, 128), f32),
            dma((4,)),
            dma((2, 4)),
            dma((2, 4)),
            dma((2,)),
            dma((2 * PARTS, STEPS)),
            dma((2 * PARTS, HALVINGS + 1)),
            dma((3,)),
            dma((2,)),
            dma((2,)),
            dma((3,)),
            dma((1,)),
            dma((11,)),
            dma((6,)),
        ],
        compiler_params=pltpu.CompilerParams(
            collective_id=0, has_side_effects=True, vmem_limit_bytes=60 * 2**20
        ),
        name="step",
    )(inputs, out_cotangent, up_proj, down_proj.T)
    gin, gup, gdn, eup, edn = pl.pallas_call(
        layout,
        out_shape=(
            shape((rows, width), bf16),
            shape((shard, both), f32),
            shape((shard, both), f32),
            shape((shard,), f32),
            shape((2, BLOCKS, 128), f32),
        ),
        in_specs=[anywhere] * 4,
        out_specs=(anywhere,) * 5,
        scratch_shapes=[
            pltpu.VMEM((rows, width), bf16),
            pltpu.VMEM((2, 2, UNITS, 16, 128), f32),
            pltpu.VMEM((4, shard, 128), f32),
            pltpu.VMEM((2, BLOCKS, 128), f32),
            pltpu.VMEM((2, shard, both), f32),
            pltpu.VMEM((shard,), f32),
            dma((5,)),
            dma((5,)),
        ],
        name="layout",
    )(*raw)
    return gin, gup, gdn.T, eup, edn.reshape((both,))


def solution(mesh):
    return jax.shard_map(
        body,
        mesh=mesh,
        in_specs=(
            P(("rep", "fs", "tp"), None),
            P("fs", "tp"),
            P("tp", "fs"),
            P(("rep", "fs", "tp"), None),
        ),
        out_specs=(P(("rep", "fs", "tp"), None), P("fs", "tp"), P("tp", "fs"), P("fs"), P("tp")),
        check_vma=False,
    )
```

```python
import functools

import jax
import jax.numpy as jnp
from jax import lax
from jax.experimental import pallas as pl
from jax.experimental.pallas import tpu as pltpu
from jax.sharding import PartitionSpec as P

MESH = pl.DeviceIdType.MESH
GATHER = (
    (
        (2, 4, 0, 1, 3),
        (0, 3, 1, 2, 4),
        (1, 4, 0, 2, 3),
        (2, 3, 1, 0, 4),
        (4, 0, 2, 3, 1),
        (4, 3, 0, 1, 2),
        (1, 2, 3, 4, 0),
        (3, 1, 4, 0, 2),
    ),
    (
        (0, 4, 1, 3, 2),
        (3, 2, 0, 1, 4),
        (2, 4, 3, 1, 0),
        (1, 3, 2, 0, 4),
        (0, 1, 2, 4, 3),
        (2, 4, 3, 1, 0),
        (2, 1, 4, 0, 3),
        (3, 0, 4, 2, 1),
    ),
)
REDUCE = (
    (
        (3, 4, 2, 0, 1),
        (4, 3, 0, 1, 2),
        (1, 2, 0, 4, 3),
        (2, 1, 0, 4, 3),
        (3, 4, 0, 2, 1),
        (3, 4, 2, 1, 0),
        (2, 1, 0, 3, 4),
        (3, 4, 1, 0, 2),
    ),
    (
        (1, 2, 0, 4, 3),
        (4, 3, 1, 0, 2),
        (1, 2, 4, 3, 0),
        (4, 3, 2, 0, 1),
        (2, 1, 0, 4, 3),
        (4, 3, 0, 2, 1),
        (1, 2, 3, 0, 4),
        (2, 1, 3, 4, 0),
    ),
)
FIRST = (
    0, 10, 20, 40, 70, 30, 50, 60, 100, 110, 120, 130, 140, 170, 150, 160,
    1, 11, 41, 71, 61, 21, 31, 51, 101, 111, 141, 161, 171, 121, 131,
    151, 2, 12, 42, 72, 62, 22, 32, 52, 102, 122, 142, 132, -2, 162, 172,
    152, 112, 3, 13, 43, 63, 73, 53, 23, 33, 103, 143, 123, 173, 133, -3, -1,
    153, 163, 4, 14, 113, 74, 64, 24, 34, 44, 54,
)
THEN = (
    1010, 1011, 1012, 1013, 1100, 1101, 1102, 100, 110, 1103, 120, 130, 1000, 140, 160, 1001,
    170, 150, 101, 1002, 111, 121, 1003, 131, 141, 1201, 0, 161, 10, 171, 102, 1200,
    122, 20, 151, 40, 1301, 50, 112, 60, 30, 70, 142, 162, 1300, 132, 11, 172,
    1, 103, 152, 21, 123, 41, 51, 113, 31, 61, 71, 143, 163, 12, 133, 173,
    2, 22, 153, 42, 52, 32, 72, 62, 13, 3, 1400, 23, 43, 1500, 53, 33,
    73, 63, 1401, 1402, 1310, 1311,
)
STEPS = 5
PARTS = 8
SPLIT = 2
SIZE = 2
UNITS = 16
BLOCKS = 8
HALF = (16, 8, 4)
HALVINGS = 3
ROOM = 68
SPAN = 240.0
SHIFT = 120.0


def encode(value, scale):
    code = jnp.exp2(jnp.abs(value) * (SPAN / scale) - SHIFT)
    return jnp.where(value < 0.0, -code, code).astype(jnp.bfloat16)


def decode(code, scale):
    code = code.astype(jnp.float32)
    size = (jnp.log2(jnp.abs(code)) + SHIFT) * (scale * (1.0 / SPAN))
    return jnp.where(code < 0.0, -size, size)


def scale_of(top):
    return (top * 1.01 + 1e-35).astype(jnp.bfloat16)


def bits_of(fs):
    z, y, x = fs // 16, (fs // 4) % 4, fs % 4
    return (z, (y % 2 + y // 2) % 2, y // 2, (x % 2 + x // 2) % 2, x // 2)


def partners_of(fs):
    z, y, x = fs // 16, (fs // 4) % 4, fs % 4
    return (
        fs + 16 - 32 * z,
        fs + 4 - 8 * (y % 2),
        fs + 12 - 8 * y,
        fs + 1 - 2 * (x % 2),
        fs + 3 - 2 * x,
    )


def remote(src, dst, send, recv, device):
    return pltpu.make_async_remote_copy(
        src_ref=src, dst_ref=dst, send_sem=send, recv_sem=recv, device_id=device, device_id_type=MESH
    )


def contract(left, right, left_dim, right_dim):
    return lax.dot_general(
        left, right, (((left_dim,), (right_dim,)), ((), ())), preferred_element_type=jnp.float32
    )


def kernel(
    factor,
    x_ref,
    c_ref,
    u_ref,
    d_ref,
    gin,
    outs,
    eup_ref,
    edn_ref,
    tok,
    tokt,
    wg,
    wn,
    pre,
    act,
    gpre,
    gbuf,
    sbuf,
    rbuf,
    part_in,
    pair_out,
    pair_in,
    twin_out,
    twin_in,
    ebuf,
    eup,
    load_s,
    tok_r,
    fwd_r,
    sib_r,
    g_r,
    r_r,
    rep_r,
    pi_r,
    li_r,
    e_r,
    eu_r,
    sent,
):
    rep, fs, tp = lax.axis_index("rep"), lax.axis_index("fs"), lax.axis_index("tp")
    mine = bits_of(fs)
    near = [{"fs": other} for other in partners_of(fs)]
    sibling = {"tp": 1 - tp}
    pair = {"rep": 1 - rep, "fs": partners_of(fs)[0]}
    twin = {"rep": 1 - rep}
    cross = {"rep": 1 - rep, "tp": 1 - tp}
    z, y, x = fs // 16, (fs // 4) % 4, fs % 4
    far_x = {"fs": fs + (x + 2) % 4 - x}
    far_y = {"fs": fs + 4 * ((y + 2) % 4 - y)}
    rows, width = x_ref.shape
    shard = u_ref.shape[0]
    hidden = u_ref.shape[1] // 2
    base = rep * hidden
    weights = (u_ref, d_ref)
    tokens = (x_ref, c_ref)
    pieces = 2
    chunk = rows // pieces
    cuts = (2, 4)
    half_rows = 2 * rows
    bw = 256
    blocks = hidden // bw
    all_parts = range(PARTS)
    f32, bf16 = jnp.float32, jnp.bfloat16

    flip = [(bit, 1 - bit) for bit in mine]
    tables = {}

    def slot(order, s):
        if order not in tables:
            place = {d: 2**k for k, d in enumerate(order)}
            high, low = [], []
            for v in range(8):
                bits = bits_of(4 * v)
                high.append(sum(flip[d][bits[d]] * place[d] for d in (0, 1, 2)))
            for v in range(4):
                bits = bits_of(v)
                low.append(sum(flip[d][bits[d]] * place[d] for d in (3, 4)))
            tables[order] = high, low
        high, low = tables[order]
        return high[s // 4] + low[s % 4]

    def home(m, p):
        return (m * PARTS + p) * 32 * SIZE

    def place_of(m, p):
        return (m * PARTS + p) * 32

    barrier = pltpu.get_barrier_semaphore()
    for device in near + [sibling, pair, twin, cross, far_x, far_y]:
        pl.semaphore_signal(barrier, inc=1, device_id=device, device_id_type=MESH)

    for m in range(2):
        pltpu.make_async_copy(tokens[m], tok.at[m, pl.ds(0, rows)], load_s.at[m]).start()
        for p in all_parts:
            columns = pl.ds(pl.multiple_of(base + p * 128, 128), 128)
            pltpu.make_async_copy(weights[m].at[:, columns], wg.at[place_of(m, p)], load_s.at[2 + m]).start()

    def wait_bytes(ref, sem):
        pltpu.make_async_copy(ref, ref, sem).wait()

    for m in range(2):
        wait_bytes(tok.at[m, pl.ds(0, rows)], load_s.at[m])
        wait_bytes(wg.at[pl.ds(0, PARTS)], load_s.at[2 + m])

    pl.semaphore_wait(barrier, STEPS + 6)

    def start(copy):
        copy.start()
        return copy

    def token_copy(m, q):
        return remote(
            tok.at[m, pl.ds(q * (rows // cuts[m]), rows // cuts[m])],
            tok.at[m, pl.ds(2 * rows + q * (rows // cuts[m]), rows // cuts[m])],
            sent.at[0],
            tok_r.at[m, q],
            pair,
        )

    def forward_copy(m, q):
        return remote(
            tok.at[m, pl.ds(2 * rows + q * (rows // cuts[m]), rows // cuts[m])],
            tok.at[m, pl.ds(3 * rows + q * (rows // cuts[m]), rows // cuts[m])],
            sent.at[1],
            fwd_r.at[m, q],
            sibling,
        )

    def sibling_copy(m):
        return remote(tok.at[m, pl.ds(0, rows)], tok.at[m, pl.ds(rows, rows)], sent.at[2], sib_r.at[m], sibling)

    def gather_copy(m, p, k):
        n = 2**k
        return remote(
            wg.at[pl.ds(place_of(m, p), n)],
            wg.at[pl.ds(place_of(m, p) + n, n)],
            sent.at[3 + m],
            g_r.at[m * PARTS + p, k],
            near[GATHER[m][p][k]],
        )

    def forward(m, q):
        token_copy(m, q).wait_recv()
        start(forward_copy(m, q))

    def transpose(m, g):
        tokt[m, :, g * rows : (g + 1) * rows] = tok[m, g * rows : (g + 1) * rows].T

    def unpack(m, p):
        for s in range(32):
            wn[m, s * shard : (s + 1) * shard, p * 128 : (p + 1) * 128] = wg[
                place_of(m, p) + slot(GATHER[m][p], s)
            ]

    def part_cols(j):
        return slice(j * bw, (j + 1) * bw)

    def forward_block(j):
        for h in range(2):
            part = slice(h * half_rows, (h + 1) * half_rows)
            kept = jnp.maximum(
                jnp.dot(tok[0, part], wn[0, :, part_cols(j)], preferred_element_type=f32), 0.0
            )
            pre[part, part_cols(j)] = kept
            act[part, part_cols(j)] = (kept * kept).astype(bf16)

    def back_block(j):
        for p in (2 * j, 2 * j + 1):
            gather_copy(1, p, STEPS - 1).wait_recv()
            unpack(1, p)
        for h in range(2):
            part = slice(h * half_rows, (h + 1) * half_rows)
            value = jnp.dot(tok[1, part], wn[1, :, part_cols(j)], preferred_element_type=f32)
            gpre[part, part_cols(j)] = (2.0 * pre[part, part_cols(j)] * value).astype(bf16)

    def room(m, p, k):
        before = sum(1 + HALF[i] * SIZE for i in range(k))
        return (m * PARTS + p) * ROOM + before

    def reduce_copy(m, p, k):
        place = pl.ds(room(m, p, k), 1 + HALF[k] * SIZE)
        return remote(
            sbuf.at[place],
            rbuf.at[place],
            sent.at[5],
            r_r.at[m * PARTS + p, k],
            near[REDUCE[m][p][STEPS - 1 - k]],
        )

    def direct_room(m, p, i):
        return room(m, p, HALVINGS) + (i - 1) * (1 + SIZE)

    def direct_copy(m, p, i):
        order = REDUCE[m][p]
        far = far_x if 3 in order[:2] else far_y
        place = pl.ds(direct_room(m, p, i), 1 + SIZE)
        return remote(
            sbuf.at[place],
            rbuf.at[place],
            sent.at[5],
            r_r.at[m * PARTS + p, HALVINGS],
            (None, near[order[0]], near[order[1]], far)[i],
        )

    def chunks(count, size):
        step = min(count, 8) * size
        return count * size // step, step

    def highest(m, p, k):
        n = SIZE
        loops, step = chunks(HALF[k], n)
        at = home(m, p) + HALF[k] * n

        def some(i, top):
            return jnp.maximum(top, jnp.max(jnp.abs(gbuf[pl.ds(at + i * step, step)]), axis=0))

        return lax.fori_loop(0, loops, some, jnp.zeros((16, 128), f32))

    def send_sums(m, p, k, top):
        n = SIZE
        loops, step = chunks(HALF[k], n)
        at, to = home(m, p) + HALF[k] * n, room(m, p, k)
        coded = scale_of(top)
        sbuf[to] = coded
        scale = coded.astype(f32)

        def some(i, carry):
            sbuf[pl.ds(to + 1 + i * step, step)] = encode(gbuf[pl.ds(at + i * step, step)], scale)
            return carry

        lax.fori_loop(0, loops, some, 0)
        start(reduce_copy(m, p, k))

    def begin(m, p):
        send_sums(m, p, 0, highest(m, p, 0))

    def add_sums(m, p, k, first, count):
        n = SIZE
        loops, step = chunks(count, n)
        at, got = home(m, p) + first * n, room(m, p, k) + 1 + first * n
        scale = rbuf[room(m, p, k)].astype(f32)

        def some(i, top):
            place = pl.ds(at + i * step, step)
            value = gbuf[place] + decode(rbuf[pl.ds(got + i * step, step)], scale)
            gbuf[place] = value
            return jnp.maximum(top, jnp.max(jnp.abs(value), axis=0))

        return lax.fori_loop(0, loops, some, jnp.zeros((16, 128), f32))

    def reduce_step(m, p, k):
        reduce_copy(m, p, k).wait_recv()
        if k == HALVINGS - 1:
            scale = rbuf[room(m, p, k)].astype(f32)
            for i in (3, 2, 1, 0):
                at = home(m, p) + i * SIZE
                got = room(m, p, k) + 1 + i * SIZE
                value = gbuf[pl.ds(at, SIZE)] + decode(rbuf[pl.ds(got, SIZE)], scale)
                if i == 0:
                    gbuf[pl.ds(at, SIZE)] = value
                    continue
                coded = scale_of(jnp.max(jnp.abs(value), axis=0))
                to = direct_room(m, p, i)
                sbuf[to] = coded
                sbuf[pl.ds(to + 1, SIZE)] = encode(value, coded.astype(f32))
                start(direct_copy(m, p, i))
            return
        n = HALF[k + 1]
        top = add_sums(m, p, k, n, n)
        send_sums(m, p, k + 1, top)
        add_sums(m, p, k, 0, n)

    def weight_grad(m, right, j):
        tall = width // SPLIT
        for i in range(SPLIT):
            out = jnp.dot(
                tokt[m, i * tall : (i + 1) * tall, :], right[:, part_cols(j)], preferred_element_type=f32
            )
            for t in range(tall // shard):
                for e in range(2):
                    p = 2 * j + e
                    at = home(m, p) + slot(REDUCE[m][p], i * (tall // shard) + t) * SIZE
                    value = out[t * shard : (t + 1) * shard, e * 128 : (e + 1) * 128]
                    gbuf[pl.ds(at, SIZE)] = value.reshape(SIZE, 16, 128)
        begin(m, 2 * j)
        begin(m, 2 * j + 1)

    def share_copy(i):
        return remote(
            pre.at[pl.ds((1 + 2 * i) * rows, rows)], part_in.at[i], sent.at[6], pi_r.at[i], sibling
        )

    def pair_copy(q):
        return remote(pair_out.at[q], pair_in.at[q], sent.at[7], li_r.at[q], pair)

    for m in range(2):
        for p in all_parts:
            start(gather_copy(m, p, 0))
        for q in range(cuts[m]):
            start(token_copy(m, q))
    for m in range(2):
        start(sibling_copy(m))

    unpacked = []
    for a in FIRST:
        if a == -1:
            for m in range(2):
                transpose(m, 0)
                sibling_copy(m).wait_recv()
                transpose(m, 1)
        elif a < 0:
            forward((-2 - a) // 2, (-2 - a) % 2)
        else:
            m, p, k = a // 100, a // 10 % 10, a % 10
            gather_copy(m, p, k).wait_recv()
            if k < STEPS - 1:
                start(gather_copy(m, p, k + 1))
                continue
            unpack(m, p)
            if not unpacked:
                for q in range(pieces):
                    forward_copy(0, q).wait_recv()
                transpose(0, 2)
                transpose(0, 3)
            unpacked.append(p)
            if p ^ 1 in unpacked:
                forward_block(p // 2)

    for q in range(cuts[1]):
        forward(1, q)
    transpose(1, 2)
    for q in range(cuts[1]):
        forward_copy(1, q).wait_recv()
    transpose(1, 3)

    order = [a // 10 % 10 for a in THEN if a < 100 and a % 10 == HALVINGS]
    groups = (tuple(all_parts), tuple(order[:6]), tuple(order[6:]))
    spots = (0, 17, 30)

    def twin_copy(g):
        place = pl.ds(spots[g], 1 + len(groups[g]) * SIZE)
        return remote(twin_out.at[place], twin_in.at[place], sent.at[10], rep_r.at[g], twin)

    def twin_send(g):
        m = 1 if g == 0 else 0
        top = jnp.zeros((16, 128), f32)
        for p in groups[g]:
            for i in range(SIZE):
                top = jnp.maximum(top, jnp.abs(outs[m, rep, p * SIZE + i]))
        coded = scale_of(top)
        twin_out[spots[g]] = coded
        scale = coded.astype(f32)
        for n, p in enumerate(groups[g]):
            code = encode(outs[m, rep, pl.ds(p * SIZE, SIZE)], scale)
            twin_out[pl.ds(spots[g] + 1 + n * SIZE, SIZE)] = code
        start(twin_copy(g))
        for n, p in enumerate(groups[g]):
            code = twin_out[pl.ds(spots[g] + 1 + n * SIZE, SIZE)]
            outs[m, rep, pl.ds(p * SIZE, SIZE)] = decode(code, scale)

    def twin_receive(g):
        m = 1 if g == 0 else 0
        twin_copy(g).wait_recv()
        scale = twin_in[spots[g]].astype(f32)
        for n, p in enumerate(groups[g]):
            code = twin_in[pl.ds(spots[g] + 1 + n * SIZE, SIZE)]
            outs[m, 1 - rep, pl.ds(p * SIZE, SIZE)] = decode(code, scale)

    def finish(m, p):
        value = gbuf[pl.ds(home(m, p), SIZE)]
        wait_bytes(rbuf.at[pl.ds(direct_room(m, p, 1), 3 * (1 + SIZE))], r_r.at[m * PARTS + p, HALVINGS])
        for i in (1, 2, 3):
            to = direct_room(m, p, i)
            value = value + decode(rbuf[pl.ds(to + 1, SIZE)], rbuf[to].astype(f32))
        value = value * factor
        outs[m, rep, pl.ds(p * SIZE, SIZE)] = value
        return value

    rounds = ((near[3], near[4], far_x), (near[1], near[2], far_y), (near[0], twin, pair))

    def energy_copy(k, i):
        return remote(ebuf.at[k, 0], ebuf.at[k, 1 + i], sent.at[8], e_r.at[k], rounds[k][i])

    def energy_begin(k):
        for i in range(3):
            start(energy_copy(k, i))

    def energy_step(k):
        wait_bytes(ebuf.at[k, pl.ds(1, 3)], e_r.at[k])
        ebuf[k + 1, 0] = (ebuf[k, 0] + ebuf[k, 1]) + (ebuf[k, 2] + ebuf[k, 3])
        energy_begin(k + 1)

    squares = [jnp.zeros((16, 128), f32), jnp.zeros((16, 128), f32)]
    left = [PARTS, PARTS]
    row_copies = []

    def arrived(m, p, k):
        if k < HALVINGS:
            reduce_step(m, p, k)
            return
        value = finish(m, p)
        left[m] -= 1
        if m == 1:
            total = value[0] * value[0] + value[1] * value[1]
            ebuf[0, 0, p : p + 1, :] = jnp.sum(total, axis=0, keepdims=True)
            if left[m] == 0:
                energy_begin(0)
                twin_send(0)
            return
        for row in range(2):
            squares[row] = squares[row] + value[row] * value[row]
        if left[m] == 2:
            twin_send(1)
        if left[m] == 0:
            twin_send(2)
            for row in range(2):
                eup[0, row * 16 : row * 16 + 16] = squares[row]
            for i, device in enumerate((sibling, twin, cross)):
                row_copies.append(start(remote(eup.at[0], eup.at[1 + i], sent.at[9], eu_r.at[0], device)))

    def inputs_grad(i):
        part = slice(i * half_rows, (i + 1) * half_rows)
        for n in range(width // bw):
            pre[part, n * bw : (n + 1) * bw] = contract(
                gpre[part, :], wn[0, n * bw : (n + 1) * bw, :], 1, 1
            )
        start(share_copy(i))

    def share_arrived(i):
        share_copy(i).wait_recv()
        if i == 0:
            pre[0:rows] = pre[0:rows] + part_in[0]
            return
        for q in range(pieces):
            s = slice(q * chunk, (q + 1) * chunk)
            value = pre[2 * rows + q * chunk : 2 * rows + (q + 1) * chunk] + part_in[1, s]
            coded = scale_of(jnp.max(jnp.abs(value), axis=0, keepdims=True))
            pair_out[q, 0:16] = jnp.broadcast_to(coded, (16, width))
            pair_out[q, 16 : 16 + chunk] = encode(value, coded.astype(f32))
            start(pair_copy(q))

    def pair_arrived(q):
        pair_copy(q).wait_recv()
        s = slice(q * chunk, (q + 1) * chunk)
        scale = pair_in[q, 0:16].astype(f32)[0:1]
        gin[s] = (pre[s] + decode(pair_in[q, 16 : 16 + chunk], scale)).astype(bf16)

    def energy_end():
        wait_bytes(ebuf.at[2, pl.ds(1, 3)], e_r.at[2])
        edn_ref[rep] = (ebuf[2, 0] + ebuf[2, 1]) * (1.0 / width)
        edn_ref[1 - rep] = (ebuf[2, 2] + ebuf[2, 3]) * (1.0 / width)

    def twins_arrived(m):
        for g in (0,) if m == 1 else (1, 2):
            twin_receive(g)

    def run(a):
        if a < 200:
            arrived(a // 100, a // 10 % 10, a % 10)
        elif a < 1100:
            m, j = (a - 1000) // 10, a % 10
            weight_grad(m, (gpre, act)[m], j)
        elif a < 1200:
            back_block(a - 1100)
        elif a < 1300:
            inputs_grad(a - 1200)
        elif a < 1310:
            share_arrived(a - 1300)
        elif a < 1400:
            pair_arrived(a - 1310)
        elif a < 1402:
            energy_step(a - 1400)
        elif a == 1402:
            energy_end()
        else:
            twins_arrived(1)

    for a in THEN[:-3]:
        run(a)
    twins_arrived(0)
    for a in THEN[-3:]:
        run(a)
    wait_bytes(eup.at[pl.ds(1, 3)], eu_r.at[0])
    eup_ref[...] = (eup[0] + eup[1]) + (eup[2] + eup[3])
    wait_bytes(tok.at[:, pl.ds(0, rows)], sent.at[0])
    wait_bytes(tok.at[:, pl.ds(0, rows)], sent.at[1])
    wait_bytes(tok.at[:, pl.ds(0, rows)], sent.at[2])
    for m in range(2):
        wait_bytes(wg.at[pl.ds(0, 31 * PARTS)], sent.at[3 + m])
    wait_bytes(sbuf, sent.at[5])
    wait_bytes(part_in, sent.at[6])
    wait_bytes(pair_out, sent.at[7])
    wait_bytes(ebuf.at[pl.ds(0, 3), pl.ds(0, 3)], sent.at[8])
    wait_bytes(eup.at[pl.ds(0, 3)], sent.at[9])
    wait_bytes(twin_out, sent.at[10])


def layout(gin, grad, eup, edn, gin_out, gup_out, gdn_out, eup_out, edn_out, both, row, out_s):
    stores = []

    def store(i, src, dst):
        copy = pltpu.make_async_copy(src, dst, out_s.at[i])
        copy.start()
        stores.append(copy)

    half = gup_out.shape[1] // 2
    store(0, gin, gin_out)
    store(1, edn, edn_out)
    for m, out in ((1, gdn_out), (0, gup_out)):
        for r in range(2):
            for u in range(UNITS):
                block, top = divmod(u, 2)
                left = r * half + block * 128
                both[m, top * 16 : top * 16 + 16, left : left + 128] = grad[m, r, u]
        store(2 + m, both.at[m], out)
    row[...] = jnp.sum(eup[...].T, axis=0) * (1.0 / (4 * half))
    store(4, row, eup_out)
    for copy in stores:
        copy.wait()


def body(inputs, up_proj, down_proj, out_cotangent):
    rows, width = inputs.shape
    shard, both = up_proj.shape
    hidden = both // 2
    factor = float(rows * lax.axis_size("rep") * lax.axis_size("fs") * lax.axis_size("tp")) ** (-0.5)
    f32, bf16 = jnp.float32, jnp.bfloat16
    shape = jax.ShapeDtypeStruct
    dma = pltpu.SemaphoreType.DMA
    messages = 2 * PARTS * ROOM
    anywhere = pl.BlockSpec(memory_space=pl.ANY)
    vmem = pl.BlockSpec(memory_space=pltpu.VMEM)
    raw = pl.pallas_call(
        functools.partial(kernel, factor),
        out_shape=(
            pltpu.VMEM((rows, width), bf16),
            pltpu.VMEM((2, 2, UNITS, 16, 128), f32),
            pltpu.VMEM((shard, 128), f32),
            pltpu.VMEM((2, BLOCKS, 128), f32),
        ),
        in_specs=[anywhere] * 4,
        out_specs=(vmem,) * 4,
        scratch_shapes=[
            pltpu.VMEM((2, 4 * rows, width), bf16),
            pltpu.VMEM((2, width, 4 * rows), bf16),
            pltpu.VMEM((2 * PARTS * 32, shard, 128), bf16),
            pltpu.VMEM((2, width, hidden), bf16),
            pltpu.VMEM((4 * rows, max(hidden, width)), f32),
            pltpu.VMEM((4 * rows, hidden), bf16),
            pltpu.VMEM((4 * rows, hidden), bf16),
            pltpu.VMEM((2 * 32 * UNITS, 16, 128), f32),
            pltpu.VMEM((messages, 16, 128), bf16),
            pltpu.VMEM((messages, 16, 128), bf16),
            pltpu.VMEM((2, rows, width), f32),
            pltpu.VMEM((2, 16 + rows // 2, width), bf16),
            pltpu.VMEM((2, 16 + rows // 2, width), bf16),
            pltpu.VMEM((35, 16, 128), bf16),
            pltpu.VMEM((35, 16, 128), bf16),
            pltpu.VMEM((4, 4, BLOCKS, 128), f32),
            pltpu.VMEM((4, shard, 128), f32),
            dma((4,)),
            dma((2, 4)),
            dma((2, 4)),
            dma((2,)),
            dma((2 * PARTS, STEPS)),
            dma((2 * PARTS, HALVINGS + 1)),
            dma((3,)),
            dma((2,)),
            dma((2,)),
            dma((3,)),
            dma((1,)),
            dma((11,)),
        ],
        compiler_params=pltpu.CompilerParams(
            collective_id=0, has_side_effects=True, vmem_limit_bytes=60 * 2**20
        ),
        name="step",
    )(inputs, out_cotangent, up_proj, down_proj.T)
    gin, gup, gdn, eup, edn = pl.pallas_call(
        layout,
        out_shape=(
            shape((rows, width), bf16),
            shape((shard, both), f32),
            shape((shard, both), f32),
            shape((shard,), f32),
            shape((2, BLOCKS, 128), f32),
        ),
        in_specs=[vmem] * 4,
        out_specs=(anywhere,) * 5,
        scratch_shapes=[
            pltpu.VMEM((2, shard, both), f32),
            pltpu.VMEM((shard,), f32),
            dma((5,)),
        ],
        compiler_params=pltpu.CompilerParams(vmem_limit_bytes=8 * 2**20),
        name="layout",
    )(*raw)
    return gin, gup, gdn.T, eup, edn.reshape((both,))


def solution(mesh):
    return jax.shard_map(
        body,
        mesh=mesh,
        in_specs=(
            P(("rep", "fs", "tp"), None),
            P("fs", "tp"),
            P("tp", "fs"),
            P(("rep", "fs", "tp"), None),
        ),
        out_specs=(P(("rep", "fs", "tp"), None), P("fs", "tp"), P("tp", "fs"), P("fs"), P("tp")),
        check_vma=False,
    )
```

```python
import functools

import jax
import jax.numpy as jnp
from jax import lax
from jax.experimental import pallas as pl
from jax.experimental.pallas import tpu as pltpu
from jax.sharding import PartitionSpec as P

MESH = pl.DeviceIdType.MESH
GATHER = (
    (
        (2, 4, 0, 1, 3),
        (0, 3, 1, 2, 4),
        (1, 4, 0, 2, 3),
        (2, 3, 1, 0, 4),
        (4, 0, 2, 3, 1),
        (4, 3, 0, 1, 2),
        (1, 2, 3, 4, 0),
        (3, 1, 4, 0, 2),
    ),
    (
        (0, 4, 1, 3, 2),
        (3, 2, 0, 1, 4),
        (2, 4, 3, 1, 0),
        (1, 3, 2, 0, 4),
        (0, 1, 2, 4, 3),
        (2, 4, 3, 1, 0),
        (2, 1, 4, 0, 3),
        (3, 0, 4, 2, 1),
    ),
)
REDUCE = (
    (
        (3, 4, 2, 0, 1),
        (4, 3, 0, 1, 2),
        (1, 2, 0, 4, 3),
        (2, 1, 0, 4, 3),
        (3, 4, 0, 2, 1),
        (3, 4, 2, 1, 0),
        (2, 1, 0, 3, 4),
        (3, 4, 1, 0, 2),
    ),
    (
        (1, 2, 0, 4, 3),
        (4, 3, 1, 0, 2),
        (1, 2, 4, 3, 0),
        (4, 3, 2, 0, 1),
        (2, 1, 0, 4, 3),
        (4, 3, 0, 2, 1),
        (1, 2, 3, 0, 4),
        (2, 1, 3, 4, 0),
    ),
)
FIRST = (
    0, 10, 20, 40, 70, 30, 50, 60, 100, 110, 120, 130, 140, 170, 150, 160,
    1, 11, 41, 71, 61, 21, 31, 51, 101, 111, 141, 161, 171, 121, 131,
    151, 2, 12, 42, 72, 62, 22, 32, 52, 102, 122, 142, 132, -2, 162, 172,
    152, 112, 3, 13, 43, 63, 73, 53, 23, 33, 103, 143, 123, 173, 133, -3, -1,
    153, 163, 4, 14, 113, 74, 64, 24, 34, 44, 54,
)
THEN = (
    1010, 1011, 1012, 1013, 1100, 1101, 1102, 100, 110, 1103, 120, 130, 1000, 140, 160, 1001,
    170, 150, 101, 1002, 111, 121, 1003, 131, 141, 1201, 0, 161, 10, 171, 102, 1200,
    122, 20, 151, 40, 1301, 50, 112, 60, 30, 70, 142, 162, 1300, 132, 11, 172,
    1, 103, 152, 21, 123, 41, 51, 113, 31, 61, 71, 143, 163, 12, 133, 173,
    2, 22, 153, 42, 52, 32, 72, 62, 13, 3, 1400, 23, 43, 1500, 53, 33,
    73, 63, 1401, 1310, 1311, 1402,
)
STEPS = 5
PARTS = 8
SPLIT = 2
SIZE = 2
UNITS = 16
BLOCKS = 8
HALF = (16, 8, 4)
HALVINGS = 3
ROOM = 68
SPAN = 240.0
SHIFT = 120.0


def encode(value, scale):
    code = jnp.exp2(jnp.abs(value) * (SPAN / scale) - SHIFT)
    return jnp.where(value < 0.0, -code, code).astype(jnp.bfloat16)


def decode(code, scale):
    code = code.astype(jnp.float32)
    size = (jnp.log2(jnp.abs(code)) + SHIFT) * (scale * (1.0 / SPAN))
    return jnp.where(code < 0.0, -size, size)


def scale_of(top):
    return (top * 1.01 + 1e-35).astype(jnp.bfloat16)


def bits_of(fs):
    z, y, x = fs // 16, (fs // 4) % 4, fs % 4
    return (z, (y % 2 + y // 2) % 2, y // 2, (x % 2 + x // 2) % 2, x // 2)


def partners_of(fs):
    z, y, x = fs // 16, (fs // 4) % 4, fs % 4
    return (
        fs + 16 - 32 * z,
        fs + 4 - 8 * (y % 2),
        fs + 12 - 8 * y,
        fs + 1 - 2 * (x % 2),
        fs + 3 - 2 * x,
    )


def remote(src, dst, send, recv, device):
    return pltpu.make_async_remote_copy(
        src_ref=src, dst_ref=dst, send_sem=send, recv_sem=recv, device_id=device, device_id_type=MESH
    )


def contract(left, right, left_dim, right_dim):
    return lax.dot_general(
        left, right, (((left_dim,), (right_dim,)), ((), ())), preferred_element_type=jnp.float32
    )


def kernel(
    factor,
    x_ref,
    c_ref,
    u_ref,
    d_ref,
    gin,
    outs,
    eup_ref,
    edn_ref,
    tok,
    tokt,
    wg,
    wn,
    pre,
    act,
    gpre,
    gbuf,
    sbuf,
    rbuf,
    part_in,
    pair_out,
    pair_in,
    twin_out,
    twin_in,
    ebuf,
    eup,
    load_s,
    tok_r,
    fwd_r,
    sib_r,
    g_r,
    r_r,
    rep_r,
    pi_r,
    li_r,
    e_r,
    eu_r,
    sent,
):
    rep, fs, tp = lax.axis_index("rep"), lax.axis_index("fs"), lax.axis_index("tp")
    mine = bits_of(fs)
    near = [{"fs": other} for other in partners_of(fs)]
    sibling = {"tp": 1 - tp}
    pair = {"rep": 1 - rep, "fs": partners_of(fs)[0]}
    twin = {"rep": 1 - rep}
    cross = {"rep": 1 - rep, "tp": 1 - tp}
    z, y, x = fs // 16, (fs // 4) % 4, fs % 4
    far_x = {"fs": fs + (x + 2) % 4 - x}
    far_y = {"fs": fs + 4 * ((y + 2) % 4 - y)}
    rows, width = x_ref.shape
    shard = u_ref.shape[0]
    hidden = u_ref.shape[1] // 2
    base = rep * hidden
    weights = (u_ref, d_ref)
    tokens = (x_ref, c_ref)
    pieces = 2
    chunk = rows // pieces
    cuts = (2, 4)
    half_rows = 2 * rows
    bw = 256
    blocks = hidden // bw
    all_parts = range(PARTS)
    f32, bf16 = jnp.float32, jnp.bfloat16

    flip = [(bit, 1 - bit) for bit in mine]
    tables = {}

    def slot(order, s):
        if order not in tables:
            place = {d: 2**k for k, d in enumerate(order)}
            high, low = [], []
            for v in range(8):
                bits = bits_of(4 * v)
                high.append(sum(flip[d][bits[d]] * place[d] for d in (0, 1, 2)))
            for v in range(4):
                bits = bits_of(v)
                low.append(sum(flip[d][bits[d]] * place[d] for d in (3, 4)))
            tables[order] = high, low
        high, low = tables[order]
        return high[s // 4] + low[s % 4]

    def home(m, p):
        return (m * PARTS + p) * 32 * SIZE

    def place_of(m, p):
        return (m * PARTS + p) * 32

    barrier = pltpu.get_barrier_semaphore()
    for device in near + [sibling, pair, twin, cross, far_x, far_y]:
        pl.semaphore_signal(barrier, inc=1, device_id=device, device_id_type=MESH)

    for m in range(2):
        pltpu.make_async_copy(tokens[m], tok.at[m, pl.ds(0, rows)], load_s.at[m]).start()
        for p in all_parts:
            columns = pl.ds(pl.multiple_of(base + p * 128, 128), 128)
            pltpu.make_async_copy(weights[m].at[:, columns], wg.at[place_of(m, p)], load_s.at[2 + m]).start()

    def wait_bytes(ref, sem):
        pltpu.make_async_copy(ref, ref, sem).wait()

    for m in range(2):
        wait_bytes(tok.at[m, pl.ds(0, rows)], load_s.at[m])
        wait_bytes(wg.at[pl.ds(0, PARTS)], load_s.at[2 + m])

    pl.semaphore_wait(barrier, STEPS + 6)

    def start(copy):
        copy.start()
        return copy

    def token_copy(m, q):
        return remote(
            tok.at[m, pl.ds(q * (rows // cuts[m]), rows // cuts[m])],
            tok.at[m, pl.ds(2 * rows + q * (rows // cuts[m]), rows // cuts[m])],
            sent.at[0],
            tok_r.at[m, q],
            pair,
        )

    def forward_copy(m, q):
        return remote(
            tok.at[m, pl.ds(2 * rows + q * (rows // cuts[m]), rows // cuts[m])],
            tok.at[m, pl.ds(3 * rows + q * (rows // cuts[m]), rows // cuts[m])],
            sent.at[1],
            fwd_r.at[m, q],
            sibling,
        )

    def sibling_copy(m):
        return remote(tok.at[m, pl.ds(0, rows)], tok.at[m, pl.ds(rows, rows)], sent.at[2], sib_r.at[m], sibling)

    def gather_copy(m, p, k):
        n = 2**k
        return remote(
            wg.at[pl.ds(place_of(m, p), n)],
            wg.at[pl.ds(place_of(m, p) + n, n)],
            sent.at[3 + m],
            g_r.at[m * PARTS + p, k],
            near[GATHER[m][p][k]],
        )

    def forward(m, q):
        token_copy(m, q).wait_recv()
        start(forward_copy(m, q))

    def transpose(m, g):
        tokt[m, :, g * rows : (g + 1) * rows] = tok[m, g * rows : (g + 1) * rows].T

    def unpack(m, p):
        for s in range(32):
            wn[m, s * shard : (s + 1) * shard, p * 128 : (p + 1) * 128] = wg[
                place_of(m, p) + slot(GATHER[m][p], s)
            ]

    def part_cols(j):
        return slice(j * bw, (j + 1) * bw)

    def forward_block(j):
        for h in range(2):
            part = slice(h * half_rows, (h + 1) * half_rows)
            kept = jnp.maximum(
                jnp.dot(tok[0, part], wn[0, :, part_cols(j)], preferred_element_type=f32), 0.0
            )
            pre[part, part_cols(j)] = kept
            act[part, part_cols(j)] = (kept * kept).astype(bf16)

    def back_block(j):
        for p in (2 * j, 2 * j + 1):
            gather_copy(1, p, STEPS - 1).wait_recv()
            unpack(1, p)
        for h in range(2):
            part = slice(h * half_rows, (h + 1) * half_rows)
            value = jnp.dot(tok[1, part], wn[1, :, part_cols(j)], preferred_element_type=f32)
            gpre[part, part_cols(j)] = (2.0 * pre[part, part_cols(j)] * value).astype(bf16)

    def room(m, p, k):
        before = sum(1 + HALF[i] * SIZE for i in range(k))
        return (m * PARTS + p) * ROOM + before

    def reduce_copy(m, p, k):
        place = pl.ds(room(m, p, k), 1 + HALF[k] * SIZE)
        return remote(
            sbuf.at[place],
            rbuf.at[place],
            sent.at[5],
            r_r.at[m * PARTS + p, k],
            near[REDUCE[m][p][STEPS - 1 - k]],
        )

    def direct_room(m, p, i):
        return room(m, p, HALVINGS) + (i - 1) * (1 + SIZE)

    def direct_copy(m, p, i):
        order = REDUCE[m][p]
        far = far_x if 3 in order[:2] else far_y
        place = pl.ds(direct_room(m, p, i), 1 + SIZE)
        return remote(
            sbuf.at[place],
            rbuf.at[place],
            sent.at[5],
            r_r.at[m * PARTS + p, HALVINGS],
            (None, near[order[0]], near[order[1]], far)[i],
        )

    def chunks(count, size):
        step = min(count, 8) * size
        return count * size // step, step

    def highest(m, p, k):
        n = SIZE
        loops, step = chunks(HALF[k], n)
        at = home(m, p) + HALF[k] * n

        def some(i, top):
            return jnp.maximum(top, jnp.max(jnp.abs(gbuf[pl.ds(at + i * step, step)]), axis=0))

        return lax.fori_loop(0, loops, some, jnp.zeros((16, 128), f32))

    def send_sums(m, p, k, top):
        n = SIZE
        loops, step = chunks(HALF[k], n)
        at, to = home(m, p) + HALF[k] * n, room(m, p, k)
        coded = scale_of(top)
        sbuf[to] = coded
        scale = coded.astype(f32)

        def some(i, carry):
            sbuf[pl.ds(to + 1 + i * step, step)] = encode(gbuf[pl.ds(at + i * step, step)], scale)
            return carry

        lax.fori_loop(0, loops, some, 0)
        start(reduce_copy(m, p, k))

    def begin(m, p):
        send_sums(m, p, 0, highest(m, p, 0))

    def add_sums(m, p, k, first, count):
        n = SIZE
        loops, step = chunks(count, n)
        at, got = home(m, p) + first * n, room(m, p, k) + 1 + first * n
        scale = rbuf[room(m, p, k)].astype(f32)

        def some(i, top):
            place = pl.ds(at + i * step, step)
            value = gbuf[place] + decode(rbuf[pl.ds(got + i * step, step)], scale)
            gbuf[place] = value
            return jnp.maximum(top, jnp.max(jnp.abs(value), axis=0))

        return lax.fori_loop(0, loops, some, jnp.zeros((16, 128), f32))

    def reduce_step(m, p, k):
        reduce_copy(m, p, k).wait_recv()
        if k == HALVINGS - 1:
            scale = rbuf[room(m, p, k)].astype(f32)
            for i in (3, 2, 1, 0):
                at = home(m, p) + i * SIZE
                got = room(m, p, k) + 1 + i * SIZE
                value = gbuf[pl.ds(at, SIZE)] + decode(rbuf[pl.ds(got, SIZE)], scale)
                if i == 0:
                    gbuf[pl.ds(at, SIZE)] = value
                    continue
                coded = scale_of(jnp.max(jnp.abs(value), axis=0))
                to = direct_room(m, p, i)
                sbuf[to] = coded
                sbuf[pl.ds(to + 1, SIZE)] = encode(value, coded.astype(f32))
                start(direct_copy(m, p, i))
            return
        n = HALF[k + 1]
        top = add_sums(m, p, k, n, n)
        send_sums(m, p, k + 1, top)
        add_sums(m, p, k, 0, n)

    def weight_grad(m, right, j):
        tall = width // SPLIT
        for i in range(SPLIT):
            out = jnp.dot(
                tokt[m, i * tall : (i + 1) * tall, :], right[:, part_cols(j)], preferred_element_type=f32
            )
            for t in range(tall // shard):
                for e in range(2):
                    p = 2 * j + e
                    at = home(m, p) + slot(REDUCE[m][p], i * (tall // shard) + t) * SIZE
                    value = out[t * shard : (t + 1) * shard, e * 128 : (e + 1) * 128]
                    gbuf[pl.ds(at, SIZE)] = value.reshape(SIZE, 16, 128)
        begin(m, 2 * j)
        begin(m, 2 * j + 1)

    def share_copy(i):
        return remote(
            pre.at[pl.ds((1 + 2 * i) * rows, rows)], part_in.at[i], sent.at[6], pi_r.at[i], sibling
        )

    def pair_copy(q):
        return remote(pair_out.at[q], pair_in.at[q], sent.at[7], li_r.at[q], pair)

    for m in range(2):
        for p in all_parts:
            start(gather_copy(m, p, 0))
        for q in range(cuts[m]):
            start(token_copy(m, q))
    for m in range(2):
        start(sibling_copy(m))

    unpacked = []
    for a in FIRST:
        if a == -1:
            for m in range(2):
                transpose(m, 0)
                sibling_copy(m).wait_recv()
                transpose(m, 1)
        elif a < 0:
            forward((-2 - a) // 2, (-2 - a) % 2)
        else:
            m, p, k = a // 100, a // 10 % 10, a % 10
            gather_copy(m, p, k).wait_recv()
            if k < STEPS - 1:
                start(gather_copy(m, p, k + 1))
                continue
            unpack(m, p)
            if not unpacked:
                for q in range(pieces):
                    forward_copy(0, q).wait_recv()
                transpose(0, 2)
                transpose(0, 3)
            unpacked.append(p)
            if p ^ 1 in unpacked:
                forward_block(p // 2)

    for q in range(cuts[1]):
        forward(1, q)
    transpose(1, 2)
    for q in range(cuts[1]):
        forward_copy(1, q).wait_recv()
    transpose(1, 3)

    order = [a // 10 % 10 for a in THEN if a < 100 and a % 10 == HALVINGS]
    groups = (tuple(all_parts), tuple(order[:6]), tuple(order[6:]))
    spots = (0, 17, 30)

    def twin_copy(g):
        place = pl.ds(spots[g], 1 + len(groups[g]) * SIZE)
        return remote(twin_out.at[place], twin_in.at[place], sent.at[10], rep_r.at[g], twin)

    def twin_send(g):
        m = 1 if g == 0 else 0
        top = jnp.zeros((16, 128), f32)
        for p in groups[g]:
            for i in range(SIZE):
                top = jnp.maximum(top, jnp.abs(outs[m, rep, p * SIZE + i]))
        coded = scale_of(top)
        twin_out[spots[g]] = coded
        scale = coded.astype(f32)
        for n, p in enumerate(groups[g]):
            code = encode(outs[m, rep, pl.ds(p * SIZE, SIZE)], scale)
            twin_out[pl.ds(spots[g] + 1 + n * SIZE, SIZE)] = code
        start(twin_copy(g))
        for n, p in enumerate(groups[g]):
            code = twin_out[pl.ds(spots[g] + 1 + n * SIZE, SIZE)]
            outs[m, rep, pl.ds(p * SIZE, SIZE)] = decode(code, scale)

    def twin_receive(g):
        m = 1 if g == 0 else 0
        twin_copy(g).wait_recv()
        scale = twin_in[spots[g]].astype(f32)
        for n, p in enumerate(groups[g]):
            code = twin_in[pl.ds(spots[g] + 1 + n * SIZE, SIZE)]
            outs[m, 1 - rep, pl.ds(p * SIZE, SIZE)] = decode(code, scale)

    def finish(m, p):
        value = gbuf[pl.ds(home(m, p), SIZE)]
        wait_bytes(rbuf.at[pl.ds(direct_room(m, p, 1), 3 * (1 + SIZE))], r_r.at[m * PARTS + p, HALVINGS])
        for i in (1, 2, 3):
            to = direct_room(m, p, i)
            value = value + decode(rbuf[pl.ds(to + 1, SIZE)], rbuf[to].astype(f32))
        value = value * factor
        outs[m, rep, pl.ds(p * SIZE, SIZE)] = value
        return value

    rounds = ((near[0], twin, pair), (near[3], near[4], far_x), (near[1], near[2], far_y))

    def energy_copy(k, i):
        n = 1 if k == 0 else 2
        return remote(
            ebuf.at[k, 0, pl.ds(0, n)],
            ebuf.at[k, 1 + i, pl.ds(0, n)],
            sent.at[11 if k == 0 else 8],
            e_r.at[k],
            rounds[k][i],
        )

    def energy_begin(k):
        for i in range(3):
            start(energy_copy(k, i))

    def energy_step(k):
        if k == 0:
            wait_bytes(ebuf.at[0, pl.ds(1, 3), 0], e_r.at[0])
            ebuf[1, 0, 0] = ebuf[0, 0, 0] + ebuf[0, 1, 0]
            ebuf[1, 0, 1] = ebuf[0, 2, 0] + ebuf[0, 3, 0]
        else:
            wait_bytes(ebuf.at[k, pl.ds(1, 3)], e_r.at[k])
            ebuf[k + 1, 0] = (ebuf[k, 0] + ebuf[k, 1]) + (ebuf[k, 2] + ebuf[k, 3])
        energy_begin(k + 1)

    squares = [jnp.zeros((16, 128), f32), jnp.zeros((16, 128), f32)]
    left = [PARTS, PARTS]
    row_copies = []

    def arrived(m, p, k):
        if k < HALVINGS:
            reduce_step(m, p, k)
            return
        value = finish(m, p)
        left[m] -= 1
        if m == 1:
            total = value[0] * value[0] + value[1] * value[1]
            ebuf[0, 0, 0, p : p + 1, :] = jnp.sum(total, axis=0, keepdims=True)
            if left[m] == 0:
                energy_begin(0)
                twin_send(0)
            return
        for row in range(2):
            squares[row] = squares[row] + value[row] * value[row]
        if left[m] == 2:
            twin_send(1)
        if left[m] == 0:
            twin_send(2)
            for row in range(2):
                eup[0, row * 16 : row * 16 + 16] = squares[row]
            for i, device in enumerate((sibling, twin, cross)):
                row_copies.append(start(remote(eup.at[0], eup.at[1 + i], sent.at[9], eu_r.at[0], device)))

    def inputs_grad(i):
        part = slice(i * half_rows, (i + 1) * half_rows)
        for n in range(width // bw):
            pre[part, n * bw : (n + 1) * bw] = contract(
                gpre[part, :], wn[0, n * bw : (n + 1) * bw, :], 1, 1
            )
        start(share_copy(i))

    def share_arrived(i):
        share_copy(i).wait_recv()
        if i == 0:
            pre[0:rows] = pre[0:rows] + part_in[0]
            return
        for q in range(pieces):
            s = slice(q * chunk, (q + 1) * chunk)
            value = pre[2 * rows + q * chunk : 2 * rows + (q + 1) * chunk] + part_in[1, s]
            coded = scale_of(jnp.max(jnp.abs(value), axis=0, keepdims=True))
            pair_out[q, 0:16] = jnp.broadcast_to(coded, (16, width))
            pair_out[q, 16 : 16 + chunk] = encode(value, coded.astype(f32))
            start(pair_copy(q))

    def pair_arrived(q):
        pair_copy(q).wait_recv()
        s = slice(q * chunk, (q + 1) * chunk)
        scale = pair_in[q, 0:16].astype(f32)[0:1]
        gin[s] = (pre[s] + decode(pair_in[q, 16 : 16 + chunk], scale)).astype(bf16)

    def energy_end():
        wait_bytes(ebuf.at[2, pl.ds(1, 3)], e_r.at[2])
        total = (ebuf[2, 0] + ebuf[2, 1]) + (ebuf[2, 2] + ebuf[2, 3])
        edn_ref[rep] = total[0] * (1.0 / width)
        edn_ref[1 - rep] = total[1] * (1.0 / width)

    def twins_arrived(m):
        for g in (0,) if m == 1 else (1, 2):
            twin_receive(g)

    def run(a):
        if a < 200:
            arrived(a // 100, a // 10 % 10, a % 10)
        elif a < 1100:
            m, j = (a - 1000) // 10, a % 10
            weight_grad(m, (gpre, act)[m], j)
        elif a < 1200:
            back_block(a - 1100)
        elif a < 1300:
            inputs_grad(a - 1200)
        elif a < 1310:
            share_arrived(a - 1300)
        elif a < 1400:
            pair_arrived(a - 1310)
        elif a < 1402:
            energy_step(a - 1400)
        elif a == 1402:
            energy_end()
        else:
            twins_arrived(1)

    for a in THEN[:-1]:
        run(a)
    twins_arrived(0)
    for a in THEN[-1:]:
        run(a)
    wait_bytes(eup.at[pl.ds(1, 3)], eu_r.at[0])
    eup_ref[...] = (eup[0] + eup[1]) + (eup[2] + eup[3])
    wait_bytes(tok.at[:, pl.ds(0, rows)], sent.at[0])
    wait_bytes(tok.at[:, pl.ds(0, rows)], sent.at[1])
    wait_bytes(tok.at[:, pl.ds(0, rows)], sent.at[2])
    for m in range(2):
        wait_bytes(wg.at[pl.ds(0, 31 * PARTS)], sent.at[3 + m])
    wait_bytes(sbuf, sent.at[5])
    wait_bytes(part_in, sent.at[6])
    wait_bytes(pair_out, sent.at[7])
    wait_bytes(ebuf.at[0, pl.ds(0, 3), 0], sent.at[11])
    wait_bytes(ebuf.at[pl.ds(1, 2), pl.ds(0, 3)], sent.at[8])
    wait_bytes(eup.at[pl.ds(0, 3)], sent.at[9])
    wait_bytes(twin_out, sent.at[10])


def layout(gin, grad, eup, edn, gin_out, gup_out, gdn_out, eup_out, edn_out, both, row, out_s):
    stores = []

    def store(i, src, dst):
        copy = pltpu.make_async_copy(src, dst, out_s.at[i])
        copy.start()
        stores.append(copy)

    half = gup_out.shape[1] // 2
    store(0, gin, gin_out)
    store(1, edn, edn_out)
    for m, out in ((1, gdn_out), (0, gup_out)):
        for r in range(2):
            for u in range(UNITS):
                block, top = divmod(u, 2)
                left = r * half + block * 128
                both[m, top * 16 : top * 16 + 16, left : left + 128] = grad[m, r, u]
        store(2 + m, both.at[m], out)
    row[...] = jnp.sum(eup[...].T, axis=0) * (1.0 / (4 * half))
    store(4, row, eup_out)
    for copy in stores:
        copy.wait()


def body(inputs, up_proj, down_proj, out_cotangent):
    rows, width = inputs.shape
    shard, both = up_proj.shape
    hidden = both // 2
    factor = float(rows * lax.axis_size("rep") * lax.axis_size("fs") * lax.axis_size("tp")) ** (-0.5)
    f32, bf16 = jnp.float32, jnp.bfloat16
    shape = jax.ShapeDtypeStruct
    dma = pltpu.SemaphoreType.DMA
    messages = 2 * PARTS * ROOM
    anywhere = pl.BlockSpec(memory_space=pl.ANY)
    vmem = pl.BlockSpec(memory_space=pltpu.VMEM)
    raw = pl.pallas_call(
        functools.partial(kernel, factor),
        out_shape=(
            pltpu.VMEM((rows, width), bf16),
            pltpu.VMEM((2, 2, UNITS, 16, 128), f32),
            pltpu.VMEM((shard, 128), f32),
            pltpu.VMEM((2, BLOCKS, 128), f32),
        ),
        in_specs=[anywhere] * 4,
        out_specs=(vmem,) * 4,
        scratch_shapes=[
            pltpu.VMEM((2, 4 * rows, width), bf16),
            pltpu.VMEM((2, width, 4 * rows), bf16),
            pltpu.VMEM((2 * PARTS * 32, shard, 128), bf16),
            pltpu.VMEM((2, width, hidden), bf16),
            pltpu.VMEM((4 * rows, max(hidden, width)), f32),
            pltpu.VMEM((4 * rows, hidden), bf16),
            pltpu.VMEM((4 * rows, hidden), bf16),
            pltpu.VMEM((2 * 32 * UNITS, 16, 128), f32),
            pltpu.VMEM((messages, 16, 128), bf16),
            pltpu.VMEM((messages, 16, 128), bf16),
            pltpu.VMEM((2, rows, width), f32),
            pltpu.VMEM((2, 16 + rows // 2, width), bf16),
            pltpu.VMEM((2, 16 + rows // 2, width), bf16),
            pltpu.VMEM((35, 16, 128), bf16),
            pltpu.VMEM((35, 16, 128), bf16),
            pltpu.VMEM((3, 4, 2, BLOCKS, 128), f32),
            pltpu.VMEM((4, shard, 128), f32),
            dma((4,)),
            dma((2, 4)),
            dma((2, 4)),
            dma((2,)),
            dma((2 * PARTS, STEPS)),
            dma((2 * PARTS, HALVINGS + 1)),
            dma((3,)),
            dma((2,)),
            dma((2,)),
            dma((3,)),
            dma((1,)),
            dma((12,)),
        ],
        compiler_params=pltpu.CompilerParams(
            collective_id=0, has_side_effects=True, vmem_limit_bytes=60 * 2**20
        ),
        name="step",
    )(inputs, out_cotangent, up_proj, down_proj.T)
    gin, gup, gdn, eup, edn = pl.pallas_call(
        layout,
        out_shape=(
            shape((rows, width), bf16),
            shape((shard, both), f32),
            shape((shard, both), f32),
            shape((shard,), f32),
            shape((2, BLOCKS, 128), f32),
        ),
        in_specs=[vmem] * 4,
        out_specs=(anywhere,) * 5,
        scratch_shapes=[
            pltpu.VMEM((2, shard, both), f32),
            pltpu.VMEM((shard,), f32),
            dma((5,)),
        ],
        compiler_params=pltpu.CompilerParams(vmem_limit_bytes=8 * 2**20),
        name="layout",
    )(*raw)
    return gin, gup, gdn.T, eup, edn.reshape((both,))


def solution(mesh):
    return jax.shard_map(
        body,
        mesh=mesh,
        in_specs=(
            P(("rep", "fs", "tp"), None),
            P("fs", "tp"),
            P("tp", "fs"),
            P(("rep", "fs", "tp"), None),
        ),
        out_specs=(P(("rep", "fs", "tp"), None), P("fs", "tp"), P("tp", "fs"), P("fs"), P("tp")),
        check_vma=False,
    )
```

```python
import functools

import jax
import jax.numpy as jnp
from jax import lax
from jax.experimental import pallas as pl
from jax.experimental.pallas import tpu as pltpu
from jax.sharding import PartitionSpec as P

MESH = pl.DeviceIdType.MESH
GATHER = (
    (
        (2, 4, 0, 1, 3),
        (0, 3, 1, 2, 4),
        (1, 4, 0, 2, 3),
        (2, 3, 1, 0, 4),
        (4, 0, 2, 3, 1),
        (4, 3, 0, 1, 2),
        (1, 2, 3, 4, 0),
        (3, 1, 4, 0, 2),
    ),
    (
        (0, 4, 1, 3, 2),
        (3, 2, 0, 1, 4),
        (2, 4, 3, 1, 0),
        (1, 3, 2, 0, 4),
        (0, 1, 2, 4, 3),
        (2, 4, 3, 1, 0),
        (2, 1, 4, 0, 3),
        (3, 0, 4, 2, 1),
    ),
)
REDUCE = (
    (
        (3, 4, 2, 0, 1),
        (4, 3, 0, 1, 2),
        (1, 2, 0, 4, 3),
        (2, 1, 0, 4, 3),
        (3, 4, 0, 2, 1),
        (3, 4, 2, 1, 0),
        (2, 1, 0, 3, 4),
        (3, 4, 1, 0, 2),
    ),
    (
        (1, 2, 0, 4, 3),
        (4, 3, 1, 0, 2),
        (1, 2, 4, 3, 0),
        (4, 3, 2, 0, 1),
        (2, 1, 0, 4, 3),
        (4, 3, 0, 2, 1),
        (1, 2, 3, 0, 4),
        (2, 1, 3, 4, 0),
    ),
)
FIRST = (
    0, 10, 20, 40, 70, 30, 50, 60, 100, 110, 120, 130, 140, 170, 150, 160,
    1, 11, 41, 71, 61, 21, 31, 51, 101, 111, 141, 161, 171, 121, 131,
    151, 2, 12, 42, 72, 62, 22, 32, 52, 102, 122, 142, 132, -2, 162, 172,
    152, 112, 3, 13, 43, 63, 73, 53, 23, 33, 103, 143, 123, 173, 133, -3, -1,
    153, 163, 4, 14, 113, 74, 64, 24, 34, 44, 54,
)
THEN = (
    1010, 1011, 1012, 1013, 1100, 1101, 1102, 100, 110, 1103, 120, 130, 1000, 140, 160, 1001,
    170, 150, 101, 1002, 111, 121, 1003, 131, 141, 1201, 0, 161, 10, 171, 102, 1200,
    122, 20, 151, 40, 1301, 50, 112, 60, 30, 70, 142, 162, 1300, 132, 11, 172,
    1, 103, 152, 21, 123, 41, 51, 113, 31, 61, 71, 143, 163, 12, 133, 173,
    2, 22, 153, 42, 52, 32, 72, 62, 13, 3, 1400, 23, 43, 53, 33, 73,
    63, 1401, 1500, 1310, 1311, 1402,
)
STEPS = 5
PARTS = 8
SPLIT = 2
SIZE = 2
UNITS = 16
BLOCKS = 8
HALF = (16, 8, 4)
HALVINGS = 3
ROOM = 68
SPAN = 240.0
SHIFT = 120.0


def encode(value, scale):
    code = jnp.exp2(jnp.abs(value) * (SPAN / scale) - SHIFT)
    return jnp.where(value < 0.0, -code, code).astype(jnp.bfloat16)


def decode(code, scale):
    code = code.astype(jnp.float32)
    size = (jnp.log2(jnp.abs(code)) + SHIFT) * (scale * (1.0 / SPAN))
    return jnp.where(code < 0.0, -size, size)


def scale_of(top):
    return (top * 1.01 + 1e-35).astype(jnp.bfloat16)


def bits_of(fs):
    z, y, x = fs // 16, (fs // 4) % 4, fs % 4
    return (z, (y % 2 + y // 2) % 2, y // 2, (x % 2 + x // 2) % 2, x // 2)


def partners_of(fs):
    z, y, x = fs // 16, (fs // 4) % 4, fs % 4
    return (
        fs + 16 - 32 * z,
        fs + 4 - 8 * (y % 2),
        fs + 12 - 8 * y,
        fs + 1 - 2 * (x % 2),
        fs + 3 - 2 * x,
    )


def remote(src, dst, send, recv, device):
    return pltpu.make_async_remote_copy(
        src_ref=src, dst_ref=dst, send_sem=send, recv_sem=recv, device_id=device, device_id_type=MESH
    )


def contract(left, right, left_dim, right_dim):
    return lax.dot_general(
        left, right, (((left_dim,), (right_dim,)), ((), ())), preferred_element_type=jnp.float32
    )


def kernel(
    factor,
    x_ref,
    c_ref,
    u_ref,
    d_ref,
    gin,
    outs,
    eup_ref,
    edn_ref,
    tok,
    tokt,
    wg,
    wn,
    pre,
    act,
    gpre,
    gbuf,
    sbuf,
    rbuf,
    part_in,
    pair_out,
    pair_in,
    twin_out,
    twin_in,
    ebuf,
    eup,
    load_s,
    tok_r,
    fwd_r,
    sib_r,
    g_r,
    r_r,
    rep_r,
    pi_r,
    li_r,
    e_r,
    eu_r,
    sent,
):
    rep, fs, tp = lax.axis_index("rep"), lax.axis_index("fs"), lax.axis_index("tp")
    mine = bits_of(fs)
    near = [{"fs": other} for other in partners_of(fs)]
    sibling = {"tp": 1 - tp}
    pair = {"rep": 1 - rep, "fs": partners_of(fs)[0]}
    twin = {"rep": 1 - rep}
    cross = {"rep": 1 - rep, "tp": 1 - tp}
    z, y, x = fs // 16, (fs // 4) % 4, fs % 4
    far_x = {"fs": fs + (x + 2) % 4 - x}
    far_y = {"fs": fs + 4 * ((y + 2) % 4 - y)}
    rows, width = x_ref.shape
    shard = u_ref.shape[0]
    hidden = u_ref.shape[1] // 2
    base = rep * hidden
    weights = (u_ref, d_ref)
    tokens = (x_ref, c_ref)
    pieces = 2
    chunk = rows // pieces
    cuts = (2, 4)
    half_rows = 2 * rows
    bw = 256
    blocks = hidden // bw
    all_parts = range(PARTS)
    f32, bf16 = jnp.float32, jnp.bfloat16

    flip = [(bit, 1 - bit) for bit in mine]
    tables = {}

    def slot(order, s):
        if order not in tables:
            place = {d: 2**k for k, d in enumerate(order)}
            high, low = [], []
            for v in range(8):
                bits = bits_of(4 * v)
                high.append(sum(flip[d][bits[d]] * place[d] for d in (0, 1, 2)))
            for v in range(4):
                bits = bits_of(v)
                low.append(sum(flip[d][bits[d]] * place[d] for d in (3, 4)))
            tables[order] = high, low
        high, low = tables[order]
        return high[s // 4] + low[s % 4]

    def home(m, p):
        return (m * PARTS + p) * 32 * SIZE

    def place_of(m, p):
        return (m * PARTS + p) * 32

    barrier = pltpu.get_barrier_semaphore()
    for device in near + [sibling, pair, twin, cross, far_x, far_y]:
        pl.semaphore_signal(barrier, inc=1, device_id=device, device_id_type=MESH)

    for m in range(2):
        pltpu.make_async_copy(tokens[m], tok.at[m, pl.ds(0, rows)], load_s.at[m]).start()
        for p in all_parts:
            columns = pl.ds(pl.multiple_of(base + p * 128, 128), 128)
            pltpu.make_async_copy(weights[m].at[:, columns], wg.at[place_of(m, p)], load_s.at[2 + m]).start()

    def wait_bytes(ref, sem):
        pltpu.make_async_copy(ref, ref, sem).wait()

    for m in range(2):
        wait_bytes(tok.at[m, pl.ds(0, rows)], load_s.at[m])
        wait_bytes(wg.at[pl.ds(0, PARTS)], load_s.at[2 + m])

    pl.semaphore_wait(barrier, STEPS + 6)

    def start(copy):
        copy.start()
        return copy

    def token_copy(m, q):
        return remote(
            tok.at[m, pl.ds(q * (rows // cuts[m]), rows // cuts[m])],
            tok.at[m, pl.ds(2 * rows + q * (rows // cuts[m]), rows // cuts[m])],
            sent.at[0],
            tok_r.at[m, q],
            pair,
        )

    def forward_copy(m, q):
        return remote(
            tok.at[m, pl.ds(2 * rows + q * (rows // cuts[m]), rows // cuts[m])],
            tok.at[m, pl.ds(3 * rows + q * (rows // cuts[m]), rows // cuts[m])],
            sent.at[1],
            fwd_r.at[m, q],
            sibling,
        )

    def sibling_copy(m):
        return remote(tok.at[m, pl.ds(0, rows)], tok.at[m, pl.ds(rows, rows)], sent.at[2], sib_r.at[m], sibling)

    def gather_copy(m, p, k):
        n = 2**k
        return remote(
            wg.at[pl.ds(place_of(m, p), n)],
            wg.at[pl.ds(place_of(m, p) + n, n)],
            sent.at[3 + m],
            g_r.at[m * PARTS + p, k],
            near[GATHER[m][p][k]],
        )

    def forward(m, q):
        token_copy(m, q).wait_recv()
        start(forward_copy(m, q))

    def transpose(m, g):
        tokt[m, :, g * rows : (g + 1) * rows] = tok[m, g * rows : (g + 1) * rows].T

    def unpack(m, p):
        for s in range(32):
            wn[m, s * shard : (s + 1) * shard, p * 128 : (p + 1) * 128] = wg[
                place_of(m, p) + slot(GATHER[m][p], s)
            ]

    def part_cols(j):
        return slice(j * bw, (j + 1) * bw)

    def forward_block(j):
        for h in range(2):
            part = slice(h * half_rows, (h + 1) * half_rows)
            kept = jnp.maximum(
                jnp.dot(tok[0, part], wn[0, :, part_cols(j)], preferred_element_type=f32), 0.0
            )
            pre[part, part_cols(j)] = kept
            act[part, part_cols(j)] = (kept * kept).astype(bf16)

    def back_block(j):
        for p in (2 * j, 2 * j + 1):
            gather_copy(1, p, STEPS - 1).wait_recv()
            unpack(1, p)
        for h in range(2):
            part = slice(h * half_rows, (h + 1) * half_rows)
            value = jnp.dot(tok[1, part], wn[1, :, part_cols(j)], preferred_element_type=f32)
            gpre[part, part_cols(j)] = (2.0 * pre[part, part_cols(j)] * value).astype(bf16)

    def room(m, p, k):
        before = sum(1 + HALF[i] * SIZE for i in range(k))
        return (m * PARTS + p) * ROOM + before

    def reduce_copy(m, p, k):
        place = pl.ds(room(m, p, k), 1 + HALF[k] * SIZE)
        return remote(
            sbuf.at[place],
            rbuf.at[place],
            sent.at[5],
            r_r.at[m * PARTS + p, k],
            near[REDUCE[m][p][STEPS - 1 - k]],
        )

    def direct_room(m, p, i):
        return room(m, p, HALVINGS) + (i - 1) * (1 + SIZE)

    def direct_copy(m, p, i):
        order = REDUCE[m][p]
        far = far_x if 3 in order[:2] else far_y
        place = pl.ds(direct_room(m, p, i), 1 + SIZE)
        return remote(
            sbuf.at[place],
            rbuf.at[place],
            sent.at[5],
            r_r.at[m * PARTS + p, HALVINGS],
            (None, near[order[0]], near[order[1]], far)[i],
        )

    def chunks(count, size):
        step = min(count, 8) * size
        return count * size // step, step

    def highest(m, p, k):
        n = SIZE
        loops, step = chunks(HALF[k], n)
        at = home(m, p) + HALF[k] * n

        def some(i, top):
            return jnp.maximum(top, jnp.max(jnp.abs(gbuf[pl.ds(at + i * step, step)]), axis=0))

        return lax.fori_loop(0, loops, some, jnp.zeros((16, 128), f32))

    def send_sums(m, p, k, top):
        n = SIZE
        loops, step = chunks(HALF[k], n)
        at, to = home(m, p) + HALF[k] * n, room(m, p, k)
        coded = scale_of(top)
        sbuf[to] = coded
        scale = coded.astype(f32)

        def some(i, carry):
            sbuf[pl.ds(to + 1 + i * step, step)] = encode(gbuf[pl.ds(at + i * step, step)], scale)
            return carry

        lax.fori_loop(0, loops, some, 0)
        start(reduce_copy(m, p, k))

    def begin(m, p):
        send_sums(m, p, 0, highest(m, p, 0))

    def add_sums(m, p, k, first, count):
        n = SIZE
        loops, step = chunks(count, n)
        at, got = home(m, p) + first * n, room(m, p, k) + 1 + first * n
        scale = rbuf[room(m, p, k)].astype(f32)

        def some(i, top):
            place = pl.ds(at + i * step, step)
            value = gbuf[place] + decode(rbuf[pl.ds(got + i * step, step)], scale)
            gbuf[place] = value
            return jnp.maximum(top, jnp.max(jnp.abs(value), axis=0))

        return lax.fori_loop(0, loops, some, jnp.zeros((16, 128), f32))

    def reduce_step(m, p, k):
        reduce_copy(m, p, k).wait_recv()
        if k == HALVINGS - 1:
            scale = rbuf[room(m, p, k)].astype(f32)
            for i in (3, 2, 1, 0):
                at = home(m, p) + i * SIZE
                got = room(m, p, k) + 1 + i * SIZE
                value = gbuf[pl.ds(at, SIZE)] + decode(rbuf[pl.ds(got, SIZE)], scale)
                if i == 0:
                    gbuf[pl.ds(at, SIZE)] = value
                    continue
                coded = scale_of(jnp.max(jnp.abs(value), axis=0))
                to = direct_room(m, p, i)
                sbuf[to] = coded
                sbuf[pl.ds(to + 1, SIZE)] = encode(value, coded.astype(f32))
                start(direct_copy(m, p, i))
            return
        n = HALF[k + 1]
        top = add_sums(m, p, k, n, n)
        send_sums(m, p, k + 1, top)
        add_sums(m, p, k, 0, n)

    def weight_grad(m, right, j):
        tall = width // SPLIT
        for i in range(SPLIT):
            out = jnp.dot(
                tokt[m, i * tall : (i + 1) * tall, :], right[:, part_cols(j)], preferred_element_type=f32
            )
            for t in range(tall // shard):
                for e in range(2):
                    p = 2 * j + e
                    at = home(m, p) + slot(REDUCE[m][p], i * (tall // shard) + t) * SIZE
                    value = out[t * shard : (t + 1) * shard, e * 128 : (e + 1) * 128]
                    gbuf[pl.ds(at, SIZE)] = value.reshape(SIZE, 16, 128)
        begin(m, 2 * j)
        begin(m, 2 * j + 1)

    def share_copy(i):
        return remote(
            pre.at[pl.ds((1 + 2 * i) * rows, rows)], part_in.at[i], sent.at[6], pi_r.at[i], sibling
        )

    def pair_copy(q):
        return remote(pair_out.at[q], pair_in.at[q], sent.at[7], li_r.at[q], pair)

    for m in range(2):
        for p in all_parts:
            start(gather_copy(m, p, 0))
        for q in range(cuts[m]):
            start(token_copy(m, q))
    for m in range(2):
        start(sibling_copy(m))

    unpacked = []
    for a in FIRST:
        if a == -1:
            for m in range(2):
                transpose(m, 0)
                sibling_copy(m).wait_recv()
                transpose(m, 1)
        elif a < 0:
            forward((-2 - a) // 2, (-2 - a) % 2)
        else:
            m, p, k = a // 100, a // 10 % 10, a % 10
            gather_copy(m, p, k).wait_recv()
            if k < STEPS - 1:
                start(gather_copy(m, p, k + 1))
                continue
            unpack(m, p)
            if not unpacked:
                for q in range(pieces):
                    forward_copy(0, q).wait_recv()
                transpose(0, 2)
                transpose(0, 3)
            unpacked.append(p)
            if p ^ 1 in unpacked:
                forward_block(p // 2)

    for q in range(cuts[1]):
        forward(1, q)
    transpose(1, 2)
    for q in range(cuts[1]):
        forward_copy(1, q).wait_recv()
    transpose(1, 3)

    order = [a // 10 % 10 for a in THEN if a < 100 and a % 10 == HALVINGS]
    groups = (tuple(all_parts), tuple(order[:6]), tuple(order[6:]))
    spots = (0, 17, 30)

    def twin_copy(g):
        place = pl.ds(spots[g], 1 + len(groups[g]) * SIZE)
        return remote(twin_out.at[place], twin_in.at[place], sent.at[10], rep_r.at[g], twin)

    def twin_send(g):
        m = 1 if g == 0 else 0
        top = jnp.zeros((16, 128), f32)
        for p in groups[g]:
            for i in range(SIZE):
                top = jnp.maximum(top, jnp.abs(outs[m, rep, p * SIZE + i]))
        coded = scale_of(top)
        twin_out[spots[g]] = coded
        scale = coded.astype(f32)
        for n, p in enumerate(groups[g]):
            code = encode(outs[m, rep, pl.ds(p * SIZE, SIZE)], scale)
            twin_out[pl.ds(spots[g] + 1 + n * SIZE, SIZE)] = code
        start(twin_copy(g))
        for n, p in enumerate(groups[g]):
            code = twin_out[pl.ds(spots[g] + 1 + n * SIZE, SIZE)]
            outs[m, rep, pl.ds(p * SIZE, SIZE)] = decode(code, scale)

    def twin_receive(g):
        m = 1 if g == 0 else 0
        twin_copy(g).wait_recv()
        scale = twin_in[spots[g]].astype(f32)
        for n, p in enumerate(groups[g]):
            code = twin_in[pl.ds(spots[g] + 1 + n * SIZE, SIZE)]
            outs[m, 1 - rep, pl.ds(p * SIZE, SIZE)] = decode(code, scale)

    def finish(m, p):
        value = gbuf[pl.ds(home(m, p), SIZE)]
        wait_bytes(rbuf.at[pl.ds(direct_room(m, p, 1), 3 * (1 + SIZE))], r_r.at[m * PARTS + p, HALVINGS])
        for i in (1, 2, 3):
            to = direct_room(m, p, i)
            value = value + decode(rbuf[pl.ds(to + 1, SIZE)], rbuf[to].astype(f32))
        value = value * factor
        outs[m, rep, pl.ds(p * SIZE, SIZE)] = value
        return value

    rounds = ((near[3], near[4], far_x), (near[1], near[2], far_y), (near[0], twin, pair))

    def energy_copy(k, i):
        return remote(ebuf.at[k, 0], ebuf.at[k, 1 + i], sent.at[8], e_r.at[k], rounds[k][i])

    def energy_begin(k):
        for i in range(3):
            start(energy_copy(k, i))

    def energy_step(k):
        wait_bytes(ebuf.at[k, pl.ds(1, 3)], e_r.at[k])
        ebuf[k + 1, 0] = (ebuf[k, 0] + ebuf[k, 1]) + (ebuf[k, 2] + ebuf[k, 3])
        energy_begin(k + 1)

    squares = [jnp.zeros((16, 128), f32), jnp.zeros((16, 128), f32)]
    left = [PARTS, PARTS]
    row_copies = []

    def arrived(m, p, k):
        if k < HALVINGS:
            reduce_step(m, p, k)
            return
        value = finish(m, p)
        left[m] -= 1
        if m == 1:
            total = value[0] * value[0] + value[1] * value[1]
            ebuf[0, 0, p : p + 1, :] = jnp.sum(total, axis=0, keepdims=True)
            if left[m] == 0:
                energy_begin(0)
                twin_send(0)
            return
        for row in range(2):
            squares[row] = squares[row] + value[row] * value[row]
        if left[m] == 2:
            twin_send(1)
        if left[m] == 0:
            twin_send(2)
            for row in range(2):
                eup[0, row * 16 : row * 16 + 16] = squares[row]
            for i, device in enumerate((sibling, twin, cross)):
                row_copies.append(start(remote(eup.at[0], eup.at[1 + i], sent.at[9], eu_r.at[0], device)))

    def inputs_grad(i):
        part = slice(i * half_rows, (i + 1) * half_rows)
        for n in range(width // bw):
            pre[part, n * bw : (n + 1) * bw] = contract(
                gpre[part, :], wn[0, n * bw : (n + 1) * bw, :], 1, 1
            )
        start(share_copy(i))

    def share_arrived(i):
        share_copy(i).wait_recv()
        if i == 0:
            pre[0:rows] = pre[0:rows] + part_in[0]
            return
        for q in range(pieces):
            s = slice(q * chunk, (q + 1) * chunk)
            value = pre[2 * rows + q * chunk : 2 * rows + (q + 1) * chunk] + part_in[1, s]
            coded = scale_of(jnp.max(jnp.abs(value), axis=0, keepdims=True))
            pair_out[q, 0:16] = jnp.broadcast_to(coded, (16, width))
            pair_out[q, 16 : 16 + chunk] = encode(value, coded.astype(f32))
            start(pair_copy(q))

    def pair_arrived(q):
        pair_copy(q).wait_recv()
        s = slice(q * chunk, (q + 1) * chunk)
        scale = pair_in[q, 0:16].astype(f32)[0:1]
        gin[s] = (pre[s] + decode(pair_in[q, 16 : 16 + chunk], scale)).astype(bf16)

    def energy_end():
        wait_bytes(ebuf.at[2, pl.ds(1, 3)], e_r.at[2])
        edn_ref[rep] = (ebuf[2, 0] + ebuf[2, 1]) * (1.0 / width)
        edn_ref[1 - rep] = (ebuf[2, 2] + ebuf[2, 3]) * (1.0 / width)

    def twins_arrived(m):
        for g in (0,) if m == 1 else (1, 2):
            twin_receive(g)

    def run(a):
        if a < 200:
            arrived(a // 100, a // 10 % 10, a % 10)
        elif a < 1100:
            m, j = (a - 1000) // 10, a % 10
            weight_grad(m, (gpre, act)[m], j)
        elif a < 1200:
            back_block(a - 1100)
        elif a < 1300:
            inputs_grad(a - 1200)
        elif a < 1310:
            share_arrived(a - 1300)
        elif a < 1400:
            pair_arrived(a - 1310)
        elif a < 1402:
            energy_step(a - 1400)
        elif a == 1402:
            energy_end()
        else:
            twins_arrived(1)

    for a in THEN[:-1]:
        run(a)
    twins_arrived(0)
    for a in THEN[-1:]:
        run(a)
    wait_bytes(eup.at[pl.ds(1, 3)], eu_r.at[0])
    eup_ref[...] = (eup[0] + eup[1]) + (eup[2] + eup[3])
    wait_bytes(tok.at[:, pl.ds(0, rows)], sent.at[0])
    wait_bytes(tok.at[:, pl.ds(0, rows)], sent.at[1])
    wait_bytes(tok.at[:, pl.ds(0, rows)], sent.at[2])
    for m in range(2):
        wait_bytes(wg.at[pl.ds(0, 31 * PARTS)], sent.at[3 + m])
    wait_bytes(sbuf, sent.at[5])
    wait_bytes(part_in, sent.at[6])
    wait_bytes(pair_out, sent.at[7])
    wait_bytes(ebuf.at[pl.ds(0, 3), pl.ds(0, 3)], sent.at[8])
    wait_bytes(eup.at[pl.ds(0, 3)], sent.at[9])
    wait_bytes(twin_out, sent.at[10])


def layout(gin, grad, eup, edn, gin_out, gup_out, gdn_out, eup_out, edn_out, both, row, out_s):
    stores = []

    def store(i, src, dst):
        copy = pltpu.make_async_copy(src, dst, out_s.at[i])
        copy.start()
        stores.append(copy)

    half = gup_out.shape[1] // 2
    store(0, gin, gin_out)
    store(1, edn, edn_out)
    for m, out in ((1, gdn_out), (0, gup_out)):
        for r in range(2):
            for u in range(UNITS):
                block, top = divmod(u, 2)
                left = r * half + block * 128
                both[m, top * 16 : top * 16 + 16, left : left + 128] = grad[m, r, u]
        store(2 + m, both.at[m], out)
    row[...] = jnp.sum(eup[...].T, axis=0) * (1.0 / (4 * half))
    store(4, row, eup_out)
    for copy in stores:
        copy.wait()


def body(inputs, up_proj, down_proj, out_cotangent):
    rows, width = inputs.shape
    shard, both = up_proj.shape
    hidden = both // 2
    factor = float(rows * lax.axis_size("rep") * lax.axis_size("fs") * lax.axis_size("tp")) ** (-0.5)
    f32, bf16 = jnp.float32, jnp.bfloat16
    shape = jax.ShapeDtypeStruct
    dma = pltpu.SemaphoreType.DMA
    messages = 2 * PARTS * ROOM
    anywhere = pl.BlockSpec(memory_space=pl.ANY)
    vmem = pl.BlockSpec(memory_space=pltpu.VMEM)
    raw = pl.pallas_call(
        functools.partial(kernel, factor),
        out_shape=(
            pltpu.VMEM((rows, width), bf16),
            pltpu.VMEM((2, 2, UNITS, 16, 128), f32),
            pltpu.VMEM((shard, 128), f32),
            pltpu.VMEM((2, BLOCKS, 128), f32),
        ),
        in_specs=[anywhere] * 4,
        out_specs=(vmem,) * 4,
        scratch_shapes=[
            pltpu.VMEM((2, 4 * rows, width), bf16),
            pltpu.VMEM((2, width, 4 * rows), bf16),
            pltpu.VMEM((2 * PARTS * 32, shard, 128), bf16),
            pltpu.VMEM((2, width, hidden), bf16),
            pltpu.VMEM((4 * rows, max(hidden, width)), f32),
            pltpu.VMEM((4 * rows, hidden), bf16),
            pltpu.VMEM((4 * rows, hidden), bf16),
            pltpu.VMEM((2 * 32 * UNITS, 16, 128), f32),
            pltpu.VMEM((messages, 16, 128), bf16),
            pltpu.VMEM((messages, 16, 128), bf16),
            pltpu.VMEM((2, rows, width), f32),
            pltpu.VMEM((2, 16 + rows // 2, width), bf16),
            pltpu.VMEM((2, 16 + rows // 2, width), bf16),
            pltpu.VMEM((35, 16, 128), bf16),
            pltpu.VMEM((35, 16, 128), bf16),
            pltpu.VMEM((4, 4, BLOCKS, 128), f32),
            pltpu.VMEM((4, shard, 128), f32),
            dma((4,)),
            dma((2, 4)),
            dma((2, 4)),
            dma((2,)),
            dma((2 * PARTS, STEPS)),
            dma((2 * PARTS, HALVINGS + 1)),
            dma((3,)),
            dma((2,)),
            dma((2,)),
            dma((3,)),
            dma((1,)),
            dma((11,)),
        ],
        compiler_params=pltpu.CompilerParams(
            collective_id=0, has_side_effects=True, vmem_limit_bytes=60 * 2**20
        ),
        name="step",
    )(inputs, out_cotangent, up_proj, down_proj.T)
    gin, gup, gdn, eup, edn = pl.pallas_call(
        layout,
        out_shape=(
            shape((rows, width), bf16),
            shape((shard, both), f32),
            shape((shard, both), f32),
            shape((shard,), f32),
            shape((2, BLOCKS, 128), f32),
        ),
        in_specs=[vmem] * 4,
        out_specs=(anywhere,) * 5,
        scratch_shapes=[
            pltpu.VMEM((2, shard, both), f32),
            pltpu.VMEM((shard,), f32),
            dma((5,)),
        ],
        compiler_params=pltpu.CompilerParams(vmem_limit_bytes=8 * 2**20),
        name="layout",
    )(*raw)
    return gin, gup, gdn.T, eup, edn.reshape((both,))


def solution(mesh):
    return jax.shard_map(
        body,
        mesh=mesh,
        in_specs=(
            P(("rep", "fs", "tp"), None),
            P("fs", "tp"),
            P("tp", "fs"),
            P(("rep", "fs", "tp"), None),
        ),
        out_specs=(P(("rep", "fs", "tp"), None), P("fs", "tp"), P("tp", "fs"), P("fs"), P("tp")),
        check_vma=False,
    )
```
